128 devices in a mesh: fs: 16 (over z, y), tp: 8 (over x, core).
Axes of the slice: x: 4, y: 4, z: 4, core: 2. Of those that a mesh axis runs over, the one named last changes fastest.
Arguments:
- tokens: bfloat16 [16384, 2048], P(('fs', 'tp')), may hold values from -6 to 6
- norm_gain: float32 [2048], replicated, may hold values from 0.1 to 1.9
- up_weight: float32 [2048, 8192], P('fs', 'tp'), may hold values from -0.125 to 0.125
- down_weight: float32 [8192, 2048], P('tp', 'fs'), may hold values from -0.0625 to 0.0625
Outputs:
- mlp_out: bfloat16 [16384, 2048], P(('fs', 'tp'))
The draws below stay inside these ranges and needn't reach their ends.
All inputs are finite; a program needn't handle non-finite values.
Results may differ from the reference program's by a relative error of at most 0.0017.
Values may be sent and summed in bfloat16 or wider, within the bound.
A program may use at most 64 MiB of HBM per device.

```python
import jax
import jax.numpy as jnp
from jax import lax

D = 2048
FF = 8192
TOKENS = 16384


def levels(rng, shape, pieces, least, largest):
    level = 1.0
    for axis_at, shards_of in pieces:
        steps = jax.random.uniform(jax.random.fold_in(jax.random.fold_in(rng, 6), axis_at), (shards_of,), jnp.float32, least / len(pieces), largest / len(pieces))
        level = level * jnp.repeat(jnp.exp(steps), shape[axis_at] // shards_of).reshape((-1,) + (1,) * (len(shape) - 1 - axis_at))
    return level


def noise(rng, extent, width, bound, cuts=(), held_as=jnp.bfloat16):
    entries = jax.random.normal(rng, extent, jnp.float32) * width
    if len(cuts) > 0:
        entries = levels(rng, extent, cuts, -0.22, 0.18) * entries
    return jnp.clip(entries, min=-bound, max=bound).astype(held_as)


def setup_inputs(seed: int = 0) -> dict:
    streams_of = jax.random.split(jax.random.key(seed), 5)
    return {
        "tokens": noise(streams_of[0], (TOKENS, D), 1.0, 6.0, ((0, 128),)),
        "norm_gain": jnp.clip(1.0 + 0.18 * jax.random.normal(streams_of[1], (D,), jnp.float32), 0.1, 1.9),
        "up_weight": noise(streams_of[2], (D, FF), D ** -0.5, 0.125, ((0, 16), (1, 8)), jnp.float32),
        "down_weight": noise(streams_of[3], (FF, D), FF ** -0.5, 0.0625, ((0, 8), (1, 16)), jnp.float32),
    }


epsilon = 1e-06

def reference(tokens, norm_gain, up_weight, down_weight):
    up_low = up_weight.astype(jnp.bfloat16)
    down_low = down_weight.astype(jnp.bfloat16)
    block_rows = min(TOKENS, 1024)
    blocks = tokens.reshape(TOKENS // block_rows, block_rows, D)

    def one_block(rows):
        values = rows.astype(jnp.float32)
        scale = lax.rsqrt(lax.optimization_barrier(jnp.mean(values * values, axis=-1, keepdims=True)) + epsilon)
        normed = (values * scale * norm_gain).astype(jnp.bfloat16)
        pre = jnp.dot(normed, up_low, preferred_element_type=jnp.float32)
        hidden = jnp.square(jax.nn.relu(pre)).astype(jnp.bfloat16)
        return jnp.dot(hidden, down_low, preferred_element_type=jnp.float32).astype(jnp.bfloat16)
    return lax.map(one_block, blocks).reshape(TOKENS, D)
```

```python
import jax
import jax.numpy as jnp
from jax import lax
from jax.experimental import pallas as pl
from jax.experimental.pallas import tpu as pltpu
from jax.sharding import PartitionSpec as P

epsilon = 1e-06
MESH = pl.DeviceIdType.MESH
SIDE = 4
OFFSETS = (0, -1, 1, 2)
BF = jnp.bfloat16
F32 = jnp.float32

ORDER = (
    (0, 0),
    (0, -1), (0, 1), (-1, 0), (1, 0),
    (-1, -1), (-1, 1), (1, -1), (1, 1),
    (2, 0), (0, 2),
    (-1, 2), (2, -1), (1, 2), (2, 1),
    (2, 2),
)


def kernel(
    tokens_ref, gain_ref, up_ref, down_ref, out_ref,
    tok, upw, dnw, pre, hid, part, first, last,
    up_recv, dn_recv, up_pair, dn_pair, tok_recv, first_recv, last_recv,
    up_send, dn_send, up_pair_send, dn_pair_send, tok_send, rs_send,
):
    rows, width = tokens_ref.shape
    half = up_ref.shape[1] // 2
    depth = up_ref.shape[0]
    blocks = SIDE * SIDE
    fs = lax.axis_index("fs")
    tp = lax.axis_index("tp")
    z, y, x, core = fs // SIDE, fs % SIDE, tp // 2, tp % 2

    def near(at, by):
        return (at + (by + SIDE)) % SIDE

    def device(dz=0, dy=0, dx=0):
        return {"fs": near(z, dz) * SIDE + near(y, dy), "tp": near(x, dx) * 2 + core}

    partner = {"fs": fs, "tp": x * 2 + (1 - core)}

    def copy(src, dst, send_sem, recv_sem, to):
        return pltpu.make_async_remote_copy(
            src_ref=src, dst_ref=dst, send_sem=send_sem, recv_sem=recv_sem,
            device_id=to, device_id_type=MESH,
        )

    barrier = pltpu.get_barrier_semaphore()
    peers = [device(dz=1), device(dz=-1), device(dy=1), device(dy=-1), device(dx=1), device(dx=-1), partner]
    for peer in peers:
        pl.semaphore_signal(barrier, inc=1, device_id=peer, device_id_type=MESH)

    def up_at(h, dz, dy, q, n):
        zs, ys = near(z, dz), near(y, dy)
        block = zs * SIDE + ys if h == 0 else ys * SIDE + zs
        row = h * blocks * depth + block * depth + q * (depth // 2)
        return upw.at[pl.ds(pl.multiple_of(row, depth // 2), n * (depth // 2)), :]

    def dn_at(h, dz, dy, q, n):
        block = near(z, dz) * SIDE + near(y, dy)
        row = block * 4 * half + h * half + q * (half // 2)
        return dnw.at[pl.ds(pl.multiple_of(row, half // 2), n * (half // 2)), :]

    class Gather:
        def __init__(self, at, recv, send):
            self.at, self.recv, self.send = at, recv, send

        def piece(self, h, df, ds, q=0, n=2):
            return self.at(h, ds, df, q, n) if h == 0 else self.at(h, df, ds, q, n)

        def peer(self, h, axis, by):
            along_y = (h == 0) == (axis == 0)
            return device(dy=by) if along_y else device(dz=by)

        def post(self, h, stage, slot, df, ds, q=0, n=2):
            ref = self.piece(h, df, ds, q, n)
            by = 1 if slot % 2 == 0 else -1
            copy(ref, ref, self.send, self.recv.at[h, stage, slot], self.peer(h, min(stage, 1), by)).start()

        def wait(self, h, stage, slot, df, ds, q=0, n=2):
            ref = self.piece(h, df, ds, q, n)
            copy(ref, ref, self.send, self.recv.at[h, stage, slot], self.peer(h, 0, 1)).wait_recv()

        def start(self):
            for h in (0, 1):
                for slot in (0, 1):
                    self.post(h, 0, slot, 0, 0)
            for h in (0, 1):
                for slot in (0, 1):
                    self.post(h, 1, slot, 0, 0)

        def second(self, h, j):
            for slot in (0, 1):
                self.post(h, 1 + j, slot, OFFSETS[j], 0)

        def first_axis(self):
            for h in (0, 1):
                self.wait(h, 0, 0, -1, 0)
                self.post(h, 0, 2, -1, 0, 0, 1)
                self.wait(h, 0, 1, 1, 0)
                self.post(h, 0, 3, 1, 0, 1, 1)
            for j in (1, 2):
                for h in (0, 1):
                    self.second(h, j)

        def far_first(self):
            for h in (0, 1):
                self.wait(h, 0, 2, 2, 0, 0, 1)
                self.wait(h, 0, 3, 2, 0, 1, 1)
                self.second(h, 3)

        def relay(self, j):
            for h in (0, 1):
                self.wait(h, 1 + j, 0, OFFSETS[j], -1)
                self.post(h, 1 + j, 2, OFFSETS[j], -1, 0, 1)
                self.wait(h, 1 + j, 1, OFFSETS[j], 1)
                self.post(h, 1 + j, 3, OFFSETS[j], 1, 1, 1)

        def far_second(self, j):
            for h in (0, 1):
                self.wait(h, 1 + j, 2, OFFSETS[j], 2, 0, 1)
                self.wait(h, 1 + j, 3, OFFSETS[j], 2, 1, 1)

    up = Gather(up_at, up_recv, up_send)
    dn = Gather(dn_at, dn_recv, dn_send)

    for h in (0, 1):
        block = fs if h == 0 else y * SIDE + z
        row = pl.multiple_of(h * blocks * depth + block * depth, depth)
        upw[pl.ds(row, depth), :] = up_ref[:, h * half:(h + 1) * half].astype(BF)
    pl.semaphore_wait(barrier, len(peers))
    up.start()

    values = tokens_ref[...].astype(F32)
    scale = lax.rsqrt(jnp.mean(values * values, axis=-1, keepdims=True) + epsilon)
    tok[pl.ds(pl.multiple_of(x * rows, rows), rows), :] = (values * scale * gain_ref[...]).astype(BF)

    def tok_at(dx, q, n=1):
        row = near(x, dx) * rows + q * (rows // 2)
        return tok.at[pl.ds(pl.multiple_of(row, rows // 2), n * (rows // 2)), :]

    def tok_post(slot, dx, q, by):
        copy(tok_at(dx, q), tok_at(dx, q), tok_send, tok_recv.at[slot], device(dx=by)).start()

    def tok_wait(slot, dx, q):
        copy(tok_at(dx, q), tok_at(dx, q), tok_send, tok_recv.at[slot], device(dx=1)).wait_recv()

    tok_post(0, 0, 0, 1)
    tok_post(3, 0, 1, -1)
    tok_post(1, 0, 1, 1)
    tok_post(2, 0, 0, -1)

    own = pl.multiple_of(fs * 4 * half, 4 * half)
    dnw[pl.ds(own, 2 * half), :] = down_ref[...].astype(BF)

    def dn_block(b, to_partner):
        block = near(z, ORDER[b][0]) * SIDE + near(y, ORDER[b][1])
        row = block * 4 * half + (2 * half if to_partner else 0)
        return dnw.at[pl.ds(pl.multiple_of(row, 2 * half), 2 * half), :]

    def dn_share(b):
        copy(dn_block(b, False), dn_block(b, True), dn_pair_send, dn_pair.at[b], partner).start()

    def up_plane(h, p, to_partner):
        plane = near(z if h == 0 else y, OFFSETS[p])
        row = (h + (2 if to_partner else 0)) * blocks * depth + plane * SIDE * depth
        return upw.at[pl.ds(pl.multiple_of(row, SIDE * depth), SIDE * depth), :]

    def up_share(p):
        for h in (0, 1):
            copy(up_plane(h, p, False), up_plane(h, p, True), up_pair_send, up_pair.at[h, p], partner).start()

    def up_shared(p):
        for h in (0, 1):
            ref = up_plane(h, p, True)
            copy(ref, ref, up_pair_send, up_pair.at[h, p], partner).wait_recv()

    dn_share(0)

    up.first_axis()
    tok_wait(0, -1, 0)
    tok_post(4, -1, 0, 1)
    tok_wait(3, 1, 1)
    tok_post(5, 1, 1, -1)
    up.relay(0)
    up.far_first()
    up_share(0)
    up.relay(1)
    up.relay(2)
    up.relay(3)
    up_share(1)
    up_share(2)
    dn.start()
    tok_wait(1, -1, 1)
    tok_wait(2, 1, 0)
    tok_wait(4, 2, 0)
    tok_wait(5, 2, 1)

    def columns_of(h, p):
        plane = near(z if h == 0 else y, OFFSETS[p])
        if h == 0:
            return tok[:, pl.ds(pl.multiple_of(plane * SIDE * depth, SIDE * depth), SIDE * depth)]
        return jnp.concatenate(
            [tok[:, pl.ds(pl.multiple_of((a * SIDE + plane) * depth, depth), depth)] for a in range(SIDE)], axis=1
        )

    def dot(a, b):
        return jnp.dot(a, b, preferred_element_type=F32)

    tile = 256

    def early(h, other):
        for n in range(half // tile):
            cols = slice(n * tile, (n + 1) * tile)
            total = sum(dot(columns_of(h, p), up_plane(h, p, other)[:, cols]) for p in (0, 1, 2))
            at = (2 * other + h) * half + n * tile
            pre[:, at:at + tile] = total

    def late(h, other):
        for n in range(half // tile):
            cols = slice(n * tile, (n + 1) * tile)
            at = (2 * other + h) * half + n * tile
            total = pre[:, at:at + tile] + dot(columns_of(h, 3), up_plane(h, 3, other)[:, cols])
            hid[:, at:at + tile] = jnp.square(jnp.maximum(total, 0.0)).astype(BF)

    for h in (0, 1):
        early(h, 0)
    for p in (0, 1, 2):
        up_shared(p)
    for h in (0, 1):
        early(h, 1)
    for j in range(4):
        up.far_second(j)
    up_share(3)
    for h in (0, 1):
        late(h, 0)
    up_shared(3)
    for h in (0, 1):
        late(h, 1)

    def part_at(b, dx, q=0, n=2):
        row = b * SIDE * rows + near(x, dx) * rows + q * (rows // 2)
        return part.at[pl.ds(pl.multiple_of(row, rows // 2), n * (rows // 2)), :]

    def project(b):
        if b:
            ref = dn_block(b, True)
            copy(ref, ref, dn_pair_send, dn_pair.at[b], partner).wait_recv()
        else:
            ref = dn_block(0, True)
            copy(ref, ref, dn_pair_send, dn_pair.at[0], partner).wait_recv()
        block = near(z, ORDER[b][0]) * SIDE + near(y, ORDER[b][1])
        piece = dnw[pl.ds(pl.multiple_of(block * 4 * half, 4 * half), 4 * half), :]
        part[b * SIDE * rows:(b + 1) * SIDE * rows, :] = dot(hid[...], piece)
        copy(part_at(b, 2, 0, 1), first.at[0, b], rs_send, first_recv.at[0, b], device(dx=1)).start()
        copy(part_at(b, 2, 1, 1), first.at[1, b], rs_send, first_recv.at[1, b], device(dx=-1)).start()

    def pass_on(b):
        for side, by in ((0, 1), (1, -1)):
            copy(first.at[side, b], first.at[side, b], rs_send, first_recv.at[side, b], device(dx=by)).wait_recv()
            ref = part_at(b, by, side, 1)
            ref[...] = ref[...] + first[side, b]
            copy(part_at(b, by), last.at[side, b], rs_send, last_recv.at[side, b], device(dx=by)).start()

    def finish(b):
        for side, by in ((0, 1), (1, -1)):
            copy(last.at[side, b], last.at[side, b], rs_send, last_recv.at[side, b], device(dx=by)).wait_recv()
        total = part_at(b, 0)[...] + last[0, b] + last[1, b]
        block = near(z, ORDER[b][0]) * SIDE + near(y, ORDER[b][1])
        out_ref[:, pl.ds(pl.multiple_of(block * rows, rows), rows)] = total.astype(BF)

    def step(b):
        if b < blocks:
            project(b)
        if 0 <= b - 2 < blocks:
            pass_on(b - 2)
        if 0 <= b - 4 < blocks:
            finish(b - 4)

    step(0)
    dn.first_axis()
    dn.relay(0)
    for b in (1, 2, 3, 4):
        dn_share(b)
    dn.far_first()
    step(1)
    dn.relay(1)
    step(2)
    dn.relay(2)
    for b in (5, 6, 7, 8):
        dn_share(b)
    dn.far_second(0)
    for b in (9, 10):
        dn_share(b)
    step(3)
    dn.relay(3)
    step(4)
    step(5)
    step(6)
    dn.far_second(1)
    dn.far_second(2)
    for b in (11, 12, 13, 14):
        dn_share(b)
    step(7)
    dn.far_second(3)
    dn_share(15)
    for b in range(8, blocks + 4):
        step(b)

    def drained(ref, sem):
        pltpu.make_async_copy(ref, ref, sem).wait()

    drained(upw.at[pl.ds(0, 15 * 4 * depth // 2), :], up_send)
    drained(dnw.at[pl.ds(0, 15 * 4 * half // 2), :], dn_send)
    drained(upw.at[pl.ds(0, 2 * blocks * depth), :], up_pair_send)
    drained(dnw.at[pl.ds(0, blocks * 2 * half), :], dn_pair_send)
    drained(tok.at[pl.ds(0, 3 * rows), :], tok_send)
    drained(part.at[pl.ds(0, blocks * 3 * rows), :], rs_send)


def shards(tokens, norm_gain, up_weight, down_weight):
    rows, width = tokens.shape
    depth, inner = up_weight.shape
    blocks = SIDE * SIDE
    vmem = pl.BlockSpec(memory_space=pltpu.VMEM)
    dma = pltpu.SemaphoreType.DMA
    return pl.pallas_call(
        kernel,
        out_shape=jax.ShapeDtypeStruct((rows, width), BF),
        in_specs=[vmem] * 4,
        out_specs=vmem,
        scratch_shapes=[
            pltpu.VMEM((SIDE * rows, width), BF),
            pltpu.VMEM((4 * blocks * depth, inner // 2), BF),
            pltpu.VMEM((blocks * 2 * inner, rows), BF),
            pltpu.VMEM((SIDE * rows, 2 * inner), F32),
            pltpu.VMEM((SIDE * rows, 2 * inner), BF),
            pltpu.VMEM((blocks * SIDE * rows, rows), F32),
            pltpu.VMEM((2, blocks, rows // 2, rows), F32),
            pltpu.VMEM((2, blocks, rows, rows), F32),
            dma((2, 5, 4)), dma((2, 5, 4)), dma((2, 4)), dma((blocks,)), dma((6,)), dma((2, blocks)), dma((2, blocks)),
            dma, dma, dma, dma, dma, dma,
        ],
        compiler_params=pltpu.CompilerParams(
            collective_id=0, has_side_effects=True, vmem_limit_bytes=60 * 1024 * 1024
        ),
    )(tokens, norm_gain.reshape(1, width), up_weight, down_weight)


def solution(mesh):
    placed = (P(("fs", "tp"), None), P(), P("fs", "tp"), P("tp", "fs"))
    return jax.shard_map(
        shards, mesh=mesh, in_specs=placed, out_specs=P(("fs", "tp"), None), check_vma=False
    )
```

```python
import jax
import jax.numpy as jnp
from jax import lax
from jax.experimental import pallas as pl
from jax.experimental.pallas import tpu as pltpu
from jax.sharding import PartitionSpec as P

epsilon = 1e-06
MESH = pl.DeviceIdType.MESH
SIDE = 4
OFFSETS = (0, -1, 1, 2)
BF = jnp.bfloat16
F32 = jnp.float32

ORDER = (
    (0, 0),
    (0, -1), (0, 1), (-1, 0), (1, 0),
    (-1, -1), (-1, 1), (1, -1), (1, 1),
    (2, 0), (0, 2),
    (-1, 2), (2, -1), (1, 2), (2, 1),
    (2, 2),
)


def kernel(
    tokens_hbm, gain_ref, up_hbm, down_hbm, out_hbm,
    tokens_ref, up_ref, down_ref, out_ref, tok, upw, dnw, pre, hid, part, first, last,
    up_recv, dn_recv, up_pair, dn_pair, tok_recv, first_recv, last_recv,
    up_send, dn_send, up_pair_send, dn_pair_send, tok_send, rs_send, load, store,
):
    rows, width = tokens_ref.shape
    half = up_ref.shape[1] // 2
    depth = up_ref.shape[0]
    blocks = SIDE * SIDE
    fs = lax.axis_index("fs")
    tp = lax.axis_index("tp")
    z, y, x, core = fs // SIDE, fs % SIDE, tp // 2, tp % 2

    def near(at, by):
        return (at + (by + SIDE)) % SIDE

    def device(dz=0, dy=0, dx=0):
        return {"fs": near(z, dz) * SIDE + near(y, dy), "tp": near(x, dx) * 2 + core}

    partner = {"fs": fs, "tp": x * 2 + (1 - core)}

    def copy(src, dst, send_sem, recv_sem, to):
        return pltpu.make_async_remote_copy(
            src_ref=src, dst_ref=dst, send_sem=send_sem, recv_sem=recv_sem,
            device_id=to, device_id_type=MESH,
        )

    barrier = pltpu.get_barrier_semaphore()
    peers = [device(dz=1), device(dz=-1), device(dy=1), device(dy=-1), device(dx=1), device(dx=-1), partner]
    for peer in peers:
        pl.semaphore_signal(barrier, inc=1, device_id=peer, device_id_type=MESH)

    loads = [
        pltpu.make_async_copy(src, dst, load.at[i])
        for i, (src, dst) in enumerate(((up_hbm, up_ref), (tokens_hbm, tokens_ref), (down_hbm, down_ref)))
    ]
    for one in loads:
        one.start()

    def up_at(h, dz, dy, q, n):
        zs, ys = near(z, dz), near(y, dy)
        block = zs * SIDE + ys if h == 0 else ys * SIDE + zs
        row = h * blocks * depth + block * depth + q * (depth // 2)
        return upw.at[pl.ds(pl.multiple_of(row, depth // 2), n * (depth // 2)), :]

    def dn_at(h, dz, dy, q, n):
        block = near(z, dz) * SIDE + near(y, dy)
        row = block * 4 * half + h * half + q * (half // 2)
        return dnw.at[pl.ds(pl.multiple_of(row, half // 2), n * (half // 2)), :]

    class Gather:
        def __init__(self, at, recv, send):
            self.at, self.recv, self.send = at, recv, send

        def piece(self, h, df, ds, q=0, n=2):
            return self.at(h, ds, df, q, n) if h == 0 else self.at(h, df, ds, q, n)

        def peer(self, h, axis, by):
            along_y = (h == 0) == (axis == 0)
            return device(dy=by) if along_y else device(dz=by)

        def post(self, h, stage, slot, df, ds, q=0, n=2):
            ref = self.piece(h, df, ds, q, n)
            by = 1 if slot % 2 == 0 else -1
            copy(ref, ref, self.send, self.recv.at[h, stage, slot], self.peer(h, min(stage, 1), by)).start()

        def wait(self, h, stage, slot, df, ds, q=0, n=2):
            ref = self.piece(h, df, ds, q, n)
            copy(ref, ref, self.send, self.recv.at[h, stage, slot], self.peer(h, 0, 1)).wait_recv()

        def start_first(self):
            for h in (0, 1):
                for slot in (0, 1):
                    self.post(h, 0, slot, 0, 0)

        def start_second(self):
            for h in (0, 1):
                for slot in (0, 1):
                    self.post(h, 1, slot, 0, 0)

        def second(self, h, j):
            for slot in (0, 1):
                self.post(h, 1 + j, slot, OFFSETS[j], 0)

        def first_axis(self):
            for h in (0, 1):
                self.wait(h, 0, 0, -1, 0)
                self.post(h, 0, 2, -1, 0, 0, 1)
                self.wait(h, 0, 1, 1, 0)
                self.post(h, 0, 3, 1, 0, 1, 1)
            for j in (1, 2):
                for h in (0, 1):
                    self.second(h, j)

        def far_first(self):
            for h in (0, 1):
                self.wait(h, 0, 2, 2, 0, 0, 1)
                self.wait(h, 0, 3, 2, 0, 1, 1)
                self.second(h, 3)

        def relay(self, j):
            for h in (0, 1):
                self.wait(h, 1 + j, 0, OFFSETS[j], -1)
                self.post(h, 1 + j, 2, OFFSETS[j], -1, 0, 1)
                self.wait(h, 1 + j, 1, OFFSETS[j], 1)
                self.post(h, 1 + j, 3, OFFSETS[j], 1, 1, 1)

        def far_second(self, j):
            for h in (0, 1):
                self.wait(h, 1 + j, 2, OFFSETS[j], 2, 0, 1)
                self.wait(h, 1 + j, 3, OFFSETS[j], 2, 1, 1)

    up = Gather(up_at, up_recv, up_send)
    dn = Gather(dn_at, dn_recv, dn_send)

    loads[0].wait()
    for h in (0, 1):
        block = fs if h == 0 else y * SIDE + z
        row = pl.multiple_of(h * blocks * depth + block * depth, depth)
        upw[pl.ds(row, depth), :] = up_ref[:, h * half:(h + 1) * half].astype(BF)
    pl.semaphore_wait(barrier, len(peers))
    up.start_first()

    loads[1].wait()
    values = tokens_ref[...].astype(F32)
    scale = lax.rsqrt(jnp.mean(values * values, axis=-1, keepdims=True) + epsilon)
    tok[pl.ds(pl.multiple_of(x * rows, rows), rows), :] = (values * scale * gain_ref[...]).astype(BF)

    def tok_at(dx, q, n=1):
        row = near(x, dx) * rows + q * (rows // 2)
        return tok.at[pl.ds(pl.multiple_of(row, rows // 2), n * (rows // 2)), :]

    def tok_post(slot, dx, q, by):
        copy(tok_at(dx, q), tok_at(dx, q), tok_send, tok_recv.at[slot], device(dx=by)).start()

    def tok_wait(slot, dx, q):
        copy(tok_at(dx, q), tok_at(dx, q), tok_send, tok_recv.at[slot], device(dx=1)).wait_recv()

    tok_post(0, 0, 0, 1)
    tok_post(3, 0, 1, -1)
    tok_post(1, 0, 1, 1)
    tok_post(2, 0, 0, -1)
    up.start_second()
    loads[2].wait()

    own = pl.multiple_of(fs * 4 * half, 4 * half)
    dnw[pl.ds(own, 2 * half), :] = down_ref[...].astype(BF)

    def dn_block(b, to_partner):
        block = near(z, ORDER[b][0]) * SIDE + near(y, ORDER[b][1])
        row = block * 4 * half + (2 * half if to_partner else 0)
        return dnw.at[pl.ds(pl.multiple_of(row, 2 * half), 2 * half), :]

    def dn_share(b):
        copy(dn_block(b, False), dn_block(b, True), dn_pair_send, dn_pair.at[b], partner).start()

    def up_plane(h, p, to_partner):
        plane = near(z if h == 0 else y, OFFSETS[p])
        row = (h + (2 if to_partner else 0)) * blocks * depth + plane * SIDE * depth
        return upw.at[pl.ds(pl.multiple_of(row, SIDE * depth), SIDE * depth), :]

    def up_share(j, p):
        for h in (0, 1):
            plane = near(z if h == 0 else y, OFFSETS[p])
            row = (plane * SIDE + near(y if h == 0 else z, OFFSETS[j])) * depth
            mine, theirs = (
                upw.at[pl.ds(pl.multiple_of((h + 2 * side) * blocks * depth + row, depth), depth), :] for side in (0, 1)
            )
            copy(mine, theirs, up_pair_send, up_pair.at[h, p], partner).start()

    def up_shared(p):
        for h in (0, 1):
            ref = up_plane(h, p, True)
            copy(ref, ref, up_pair_send, up_pair.at[h, p], partner).wait_recv()

    up_share(0, 0)
    dn_share(0)

    up.first_axis()
    up_share(1, 0)
    up_share(2, 0)
    up.relay(0)
    up_share(0, 1)
    up_share(0, 2)
    up.far_first()
    up_share(3, 0)
    tok_wait(0, -1, 0)
    tok_post(4, -1, 0, 1)
    tok_wait(3, 1, 1)
    tok_post(5, 1, 1, -1)
    for j in (1, 2, 3):
        up.relay(j)
        up_share(j, 1)
        up_share(j, 2)
    dn.start_first()
    dn.start_second()
    tok_wait(1, -1, 1)
    tok_wait(2, 1, 0)
    tok_wait(4, 2, 0)
    tok_wait(5, 2, 1)

    def columns_of(h, p):
        plane = near(z if h == 0 else y, OFFSETS[p])
        if h == 0:
            return tok[:, pl.ds(pl.multiple_of(plane * SIDE * depth, SIDE * depth), SIDE * depth)]
        return jnp.concatenate(
            [tok[:, pl.ds(pl.multiple_of((a * SIDE + plane) * depth, depth), depth)] for a in range(SIDE)], axis=1
        )

    def dot(a, b):
        return jnp.dot(a, b, preferred_element_type=F32)

    tile = 256

    def early(h, other):
        for n in range(half // tile):
            cols = slice(n * tile, (n + 1) * tile)
            total = sum(dot(columns_of(h, p), up_plane(h, p, other)[:, cols]) for p in (0, 1, 2))
            at = (2 * other + h) * half + n * tile
            pre[:, at:at + tile] = total

    def late(h, other):
        for n in range(half // tile):
            cols = slice(n * tile, (n + 1) * tile)
            at = (2 * other + h) * half + n * tile
            total = pre[:, at:at + tile] + dot(columns_of(h, 3), up_plane(h, 3, other)[:, cols])
            hid[:, at:at + tile] = jnp.square(jnp.maximum(total, 0.0)).astype(BF)

    for h in (0, 1):
        early(h, 0)
    for p in (0, 1, 2):
        up_shared(p)
    for j in (0, 1):
        up.far_second(j)
        up_share(j, 3)
    for h in (0, 1):
        early(h, 1)
    for j in (2, 3):
        up.far_second(j)
        up_share(j, 3)
    for h in (0, 1):
        late(h, 0)
    up_shared(3)
    for h in (0, 1):
        late(h, 1)

    def part_at(b, dx, q=0, n=2):
        row = b * SIDE * rows + near(x, dx) * rows + q * (rows // 2)
        return part.at[pl.ds(pl.multiple_of(row, rows // 2), n * (rows // 2)), :]

    def project(b):
        if b:
            ref = dn_block(b, True)
            copy(ref, ref, dn_pair_send, dn_pair.at[b], partner).wait_recv()
        else:
            ref = dn_block(0, True)
            copy(ref, ref, dn_pair_send, dn_pair.at[0], partner).wait_recv()
        block = near(z, ORDER[b][0]) * SIDE + near(y, ORDER[b][1])
        piece = dnw[pl.ds(pl.multiple_of(block * 4 * half, 4 * half), 4 * half), :]
        part[b * SIDE * rows:(b + 1) * SIDE * rows, :] = dot(hid[...], piece)
        copy(part_at(b, 2, 0, 1), first.at[0, b], rs_send, first_recv.at[0, b], device(dx=1)).start()
        copy(part_at(b, 2, 1, 1), first.at[1, b], rs_send, first_recv.at[1, b], device(dx=-1)).start()

    def pass_on(b):
        for side, by in ((0, 1), (1, -1)):
            copy(first.at[side, b], first.at[side, b], rs_send, first_recv.at[side, b], device(dx=by)).wait_recv()
            ref = part_at(b, by, side, 1)
            ref[...] = ref[...] + first[side, b]
            copy(part_at(b, by), last.at[side, b], rs_send, last_recv.at[side, b], device(dx=by)).start()

    def finish(b):
        for side, by in ((0, 1), (1, -1)):
            copy(last.at[side, b], last.at[side, b], rs_send, last_recv.at[side, b], device(dx=by)).wait_recv()
        total = part_at(b, 0)[...] + last[0, b] + last[1, b]
        block = near(z, ORDER[b][0]) * SIDE + near(y, ORDER[b][1])
        out_ref[b] = total.astype(BF)
        stored(b).start()

    def stored(b):
        block = near(z, ORDER[b][0]) * SIDE + near(y, ORDER[b][1])
        return pltpu.make_async_copy(
            out_ref.at[b], out_hbm.at[:, pl.ds(pl.multiple_of(block * rows, rows), rows)], store.at[b]
        )

    def step(b):
        if b < blocks:
            project(b)
        if 0 <= b - 2 < blocks:
            pass_on(b - 2)
        if 0 <= b - 6 < blocks:
            finish(b - 6)

    step(0)
    dn.first_axis()
    dn.relay(0)
    for b in (1, 2, 3, 4):
        dn_share(b)
    step(1)
    dn.far_first()
    step(2)
    dn.relay(1)
    step(3)
    step(4)
    dn.relay(2)
    for b in (5, 6, 7, 8):
        dn_share(b)
    dn.far_second(0)
    for b in (9, 10):
        dn_share(b)
    step(5)
    step(6)
    dn.relay(3)
    step(7)
    step(8)
    dn.far_second(1)
    dn.far_second(2)
    for b in (11, 12, 13, 14):
        dn_share(b)
    dn.far_second(3)
    dn_share(15)
    for b in range(9, blocks + 6):
        step(b)

    def drained(ref, sem):
        pltpu.make_async_copy(ref, ref, sem).wait()

    drained(upw.at[pl.ds(0, 15 * 4 * depth // 2), :], up_send)
    drained(dnw.at[pl.ds(0, 15 * 4 * half // 2), :], dn_send)
    drained(upw.at[pl.ds(0, 2 * blocks * depth), :], up_pair_send)
    drained(dnw.at[pl.ds(0, blocks * 2 * half), :], dn_pair_send)
    drained(tok.at[pl.ds(0, 3 * rows), :], tok_send)
    drained(part.at[pl.ds(0, blocks * 3 * rows), :], rs_send)
    for b in range(blocks):
        stored(b).wait()


def shards(tokens, norm_gain, up_weight, down_weight):
    rows, width = tokens.shape
    depth, inner = up_weight.shape
    blocks = SIDE * SIDE
    vmem = pl.BlockSpec(memory_space=pltpu.VMEM)
    anywhere = pl.BlockSpec(memory_space=pl.ANY)
    dma = pltpu.SemaphoreType.DMA
    return pl.pallas_call(
        kernel,
        out_shape=jax.ShapeDtypeStruct((rows, width), BF),
        in_specs=[anywhere, vmem, anywhere, anywhere],
        out_specs=anywhere,
        scratch_shapes=[
            pltpu.VMEM(tokens.shape, BF),
            pltpu.VMEM(up_weight.shape, F32),
            pltpu.VMEM(down_weight.shape, F32),
            pltpu.VMEM((blocks, rows, rows), BF),
            pltpu.VMEM((SIDE * rows, width), BF),
            pltpu.VMEM((4 * blocks * depth, inner // 2), BF),
            pltpu.VMEM((blocks * 2 * inner, rows), BF),
            pltpu.VMEM((SIDE * rows, 2 * inner), F32),
            pltpu.VMEM((SIDE * rows, 2 * inner), BF),
            pltpu.VMEM((blocks * SIDE * rows, rows), F32),
            pltpu.VMEM((2, blocks, rows // 2, rows), F32),
            pltpu.VMEM((2, blocks, rows, rows), F32),
            dma((2, 5, 4)), dma((2, 5, 4)), dma((2, 4)), dma((blocks,)), dma((6,)), dma((2, blocks)), dma((2, blocks)),
            dma, dma, dma, dma, dma, dma, dma((3,)), dma((blocks,)),
        ],
        compiler_params=pltpu.CompilerParams(
            collective_id=0, has_side_effects=True, vmem_limit_bytes=60 * 1024 * 1024
        ),
    )(tokens, norm_gain.reshape(1, width), up_weight, down_weight)


def solution(mesh):
    placed = (P(("fs", "tp"), None), P(), P("fs", "tp"), P("tp", "fs"))
    return jax.shard_map(
        shards, mesh=mesh, in_specs=placed, out_specs=P(("fs", "tp"), None), check_vma=False
    )
```

```python
import jax
import jax.numpy as jnp
from jax import lax
from jax.experimental import pallas as pl
from jax.experimental.pallas import tpu as pltpu
from jax.sharding import PartitionSpec as P

epsilon = 1e-06
MESH = pl.DeviceIdType.MESH
SIDE = 4
OFFSETS = (0, -1, 1, 2)
BF = jnp.bfloat16
F32 = jnp.float32

ORDER = (
    (0, 0),
    (0, -1), (0, 1), (-1, 0), (1, 0),
    (-1, -1), (-1, 1), (1, -1), (1, 1),
    (2, 0), (0, 2),
    (-1, 2), (2, -1), (1, 2), (2, 1),
    (2, 2),
)


GROUPS = ((0,), (1, 2), (3, 4), (5, 6), (7, 8), (9, 10), (11, 12), (13, 14), (15,))


def unit_of(groups, largest):
    top = jnp.maximum(jnp.max(jnp.abs(groups), axis=0), 1e-20)
    return top * (1.0 / largest), largest / top


def code_pairs(values):
    groups = values.reshape(-1, 8, values.shape[1])
    unit, inverse = unit_of(groups, 2047.0)
    levels = jnp.round(groups * inverse)
    n = groups.shape[0] // 2
    words = levels[:n] * 4096.0 + (levels[n:] + 2048.0)
    return jnp.concatenate([words, unit[None]], axis=0).reshape(-1, values.shape[1])


def decode_pairs(coded):
    groups = coded.reshape(-1, 8, coded.shape[1])
    words, unit = groups[:-1], groups[-1]
    high = jnp.floor(words * (1.0 / 4096.0))
    low = words - high * 4096.0 - 2048.0
    return (jnp.concatenate([high, low], axis=0) * unit).reshape(-1, coded.shape[1])


def code_triples(values):
    groups = values.reshape(-1, 8, values.shape[1])
    unit, inverse = unit_of(groups, 32767.0)
    n = groups.shape[0] // 3
    a, b, c = (jnp.round(groups[i * n:(i + 1) * n] * inverse) for i in range(3))
    high = jnp.floor(c * (1.0 / 256.0))
    low = c - high * 256.0
    return jnp.concatenate(
        [a * 256.0 + low, b * 256.0 + (high + 128.0), groups[3 * n:], unit[None]], axis=0
    ).reshape(-1, values.shape[1])


def decode_triples(coded):
    groups = coded.reshape(-1, 8, coded.shape[1])
    n = (groups.shape[0] - 2) // 2
    first, second, rest, unit = groups[:n], groups[n:2 * n], groups[2 * n:-1], groups[-1]
    a = jnp.floor(first * (1.0 / 256.0))
    b = jnp.floor(second * (1.0 / 256.0))
    c = (second - b * 256.0 - 128.0) * 256.0 + (first - a * 256.0)
    return jnp.concatenate([a * unit, b * unit, c * unit, rest], axis=0).reshape(-1, coded.shape[1])


def kernel(
    tokens_hbm, gain_ref, up_hbm, down_hbm, out_hbm,
    tokens_ref, up_ref, down_ref, out_ref, tok, upw, dnw, pre, hid, part, first, last, first_out, last_out,
    up_recv, dn_recv, up_pair, dn_pair, tok_recv, first_recv, last_recv,
    up_send, dn_send, up_pair_send, dn_pair_send, tok_send, rs_send, load, store,
):
    rows, width = tokens_ref.shape
    half = up_ref.shape[1] // 2
    depth = up_ref.shape[0]
    blocks = SIDE * SIDE
    fs = lax.axis_index("fs")
    tp = lax.axis_index("tp")
    z, y, x, core = fs // SIDE, fs % SIDE, tp // 2, tp % 2

    def near(at, by):
        return (at + (by + SIDE)) % SIDE

    def device(dz=0, dy=0, dx=0):
        return {"fs": near(z, dz) * SIDE + near(y, dy), "tp": near(x, dx) * 2 + core}

    partner = {"fs": fs, "tp": x * 2 + (1 - core)}

    def copy(src, dst, send_sem, recv_sem, to):
        return pltpu.make_async_remote_copy(
            src_ref=src, dst_ref=dst, send_sem=send_sem, recv_sem=recv_sem,
            device_id=to, device_id_type=MESH,
        )

    barrier = pltpu.get_barrier_semaphore()
    peers = [device(dz=1), device(dz=-1), device(dy=1), device(dy=-1), device(dx=1), device(dx=-1), partner]
    for peer in peers:
        pl.semaphore_signal(barrier, inc=1, device_id=peer, device_id_type=MESH)

    loads = [
        pltpu.make_async_copy(src, dst, load.at[i])
        for i, (src, dst) in enumerate(((up_hbm, up_ref), (tokens_hbm, tokens_ref), (down_hbm, down_ref)))
    ]
    for one in loads:
        one.start()

    def up_at(h, dz, dy, q, n):
        zs, ys = near(z, dz), near(y, dy)
        block = zs * SIDE + ys if h == 0 else ys * SIDE + zs
        row = h * blocks * depth + block * depth + q * (depth // 2)
        return upw.at[pl.ds(pl.multiple_of(row, depth // 2), n * (depth // 2)), :]

    def dn_at(h, dz, dy, q, n):
        block = near(z, dz) * SIDE + near(y, dy)
        row = block * 4 * half + h * half + q * (half // 2)
        return dnw.at[pl.ds(pl.multiple_of(row, half // 2), n * (half // 2)), :]

    class Gather:
        def __init__(self, at, recv, send):
            self.at, self.recv, self.send = at, recv, send

        def piece(self, h, df, ds, q=0, n=2):
            return self.at(h, ds, df, q, n) if h == 0 else self.at(h, df, ds, q, n)

        def peer(self, h, axis, by):
            along_y = (h == 0) == (axis == 0)
            return device(dy=by) if along_y else device(dz=by)

        def post(self, h, stage, slot, df, ds, q=0, n=2):
            ref = self.piece(h, df, ds, q, n)
            by = 1 if slot % 2 == 0 else -1
            copy(ref, ref, self.send, self.recv.at[h, stage, slot], self.peer(h, min(stage, 1), by)).start()

        def wait(self, h, stage, slot, df, ds, q=0, n=2):
            ref = self.piece(h, df, ds, q, n)
            copy(ref, ref, self.send, self.recv.at[h, stage, slot], self.peer(h, 0, 1)).wait_recv()

        def start_first(self):
            for h in (0, 1):
                for slot in (0, 1):
                    self.post(h, 0, slot, 0, 0)

        def start_second(self):
            for h in (0, 1):
                for slot in (0, 1):
                    self.post(h, 1, slot, 0, 0)

        def second(self, h, j):
            for slot in (0, 1):
                self.post(h, 1 + j, slot, OFFSETS[j], 0)

        def first_axis(self):
            for h in (0, 1):
                self.wait(h, 0, 0, -1, 0)
                self.post(h, 0, 2, -1, 0, 0, 1)
                self.wait(h, 0, 1, 1, 0)
                self.post(h, 0, 3, 1, 0, 1, 1)
            for j in (1, 2):
                for h in (0, 1):
                    self.second(h, j)

        def far_first(self):
            for h in (0, 1):
                self.wait(h, 0, 2, 2, 0, 0, 1)
                self.wait(h, 0, 3, 2, 0, 1, 1)
                self.second(h, 3)

        def relay(self, j):
            for h in (0, 1):
                self.wait(h, 1 + j, 0, OFFSETS[j], -1)
                self.post(h, 1 + j, 2, OFFSETS[j], -1, 0, 1)
                self.wait(h, 1 + j, 1, OFFSETS[j], 1)
                self.post(h, 1 + j, 3, OFFSETS[j], 1, 1, 1)

        def far_second(self, j):
            for h in (0, 1):
                self.wait(h, 1 + j, 2, OFFSETS[j], 2, 0, 1)
                self.wait(h, 1 + j, 3, OFFSETS[j], 2, 1, 1)

    up = Gather(up_at, up_recv, up_send)
    dn = Gather(dn_at, dn_recv, dn_send)

    loads[0].wait()
    for h in (0, 1):
        block = fs if h == 0 else y * SIDE + z
        row = pl.multiple_of(h * blocks * depth + block * depth, depth)
        upw[pl.ds(row, depth), :] = up_ref[:, h * half:(h + 1) * half].astype(BF)
    pl.semaphore_wait(barrier, len(peers))
    up.start_first()

    loads[1].wait()
    values = tokens_ref[...].astype(F32)
    scale = lax.rsqrt(jnp.mean(values * values, axis=-1, keepdims=True) + epsilon)
    tok[0:rows, :] = (values * scale * gain_ref[...]).astype(BF)

    def tok_at(slot, q):
        row = slot * rows + q * (rows // 2)
        return tok.at[row:row + rows // 2, :]

    def tok_post(sem, slot, there, q, by):
        copy(tok_at(slot, q), tok_at(there, q), tok_send, tok_recv.at[sem], device(dx=by)).start()

    def tok_wait(sem, slot, q):
        copy(tok_at(slot, q), tok_at(slot, q), tok_send, tok_recv.at[sem], device(dx=1)).wait_recv()

    tok_post(0, 0, 1, 0, 1)
    tok_post(3, 0, 2, 1, -1)
    tok_post(1, 0, 1, 1, 1)
    tok_post(2, 0, 2, 0, -1)
    up.start_second()
    loads[2].wait()

    own = pl.multiple_of(fs * 4 * half, 4 * half)
    dnw[pl.ds(own, 2 * half), :] = down_ref[...].astype(BF)

    def dn_block(b, to_partner):
        block = near(z, ORDER[b][0]) * SIDE + near(y, ORDER[b][1])
        row = block * 4 * half + (2 * half if to_partner else 0)
        return dnw.at[pl.ds(pl.multiple_of(row, 2 * half), 2 * half), :]

    def dn_share(b):
        copy(dn_block(b, False), dn_block(b, True), dn_pair_send, dn_pair.at[b], partner).start()

    def up_plane(h, p, to_partner):
        plane = near(z if h == 0 else y, OFFSETS[p])
        row = (h + (2 if to_partner else 0)) * blocks * depth + plane * SIDE * depth
        return upw.at[pl.ds(pl.multiple_of(row, SIDE * depth), SIDE * depth), :]

    def up_share(j, p):
        for h in (0, 1):
            plane = near(z if h == 0 else y, OFFSETS[p])
            row = (plane * SIDE + near(y if h == 0 else z, OFFSETS[j])) * depth
            mine, theirs = (
                upw.at[pl.ds(pl.multiple_of((h + 2 * side) * blocks * depth + row, depth), depth), :] for side in (0, 1)
            )
            copy(mine, theirs, up_pair_send, up_pair.at[h, p], partner).start()

    def up_shared(p):
        for h in (0, 1):
            ref = up_plane(h, p, True)
            copy(ref, ref, up_pair_send, up_pair.at[h, p], partner).wait_recv()

    up_share(0, 0)
    dn_share(0)

    up.first_axis()
    up_share(1, 0)
    up_share(2, 0)
    up.relay(0)
    up_share(0, 1)
    up_share(0, 2)
    up.far_first()
    up_share(3, 0)
    tok_wait(0, 1, 0)
    tok_post(4, 1, 3, 0, 1)
    tok_wait(3, 2, 1)
    tok_post(5, 2, 3, 1, -1)
    for j in (1, 2, 3):
        up.relay(j)
        up_share(j, 1)
        up_share(j, 2)
    dn.start_first()
    dn.start_second()
    tok_wait(1, 1, 1)
    tok_wait(2, 2, 0)
    tok_wait(4, 3, 0)
    tok_wait(5, 3, 1)

    def columns_of(h, p):
        plane = near(z if h == 0 else y, OFFSETS[p])
        if h == 0:
            return tok[:, pl.ds(pl.multiple_of(plane * SIDE * depth, SIDE * depth), SIDE * depth)]
        return jnp.concatenate(
            [tok[:, pl.ds(pl.multiple_of((a * SIDE + plane) * depth, depth), depth)] for a in range(SIDE)], axis=1
        )

    def dot(a, b):
        return jnp.dot(a, b, preferred_element_type=F32)

    tile = 256

    def early(h, other):
        for n in range(half // tile):
            cols = slice(n * tile, (n + 1) * tile)
            total = sum(dot(columns_of(h, p), up_plane(h, p, other)[:, cols]) for p in (0, 1, 2))
            at = (2 * other + h) * half + n * tile
            pre[:, at:at + tile] = total

    def late(h, other):
        for n in range(half // tile):
            cols = slice(n * tile, (n + 1) * tile)
            at = (2 * other + h) * half + n * tile
            total = pre[:, at:at + tile] + dot(columns_of(h, 3), up_plane(h, 3, other)[:, cols])
            hid[:, at:at + tile] = jnp.square(jnp.maximum(total, 0.0)).astype(BF)

    for h in (0, 1):
        early(h, 0)
    for p in (0, 1, 2):
        up_shared(p)
    for j in (0, 1):
        up.far_second(j)
        up_share(j, 3)
    for h in (0, 1):
        early(h, 1)
    for j in (2, 3):
        up.far_second(j)
        up_share(j, 3)
    for h in (0, 1):
        late(h, 0)
    up_shared(3)
    for h in (0, 1):
        late(h, 1)

    def part_at(b, slot, q=0, n=2):
        row = (b * 3 + slot) * rows + q * (rows // 2)
        return part.at[row:row + n * (rows // 2), :]

    def project(group):
        pieces = []
        for b in group:
            ref = dn_block(b, True)
            copy(ref, ref, dn_pair_send, dn_pair.at[b], partner).wait_recv()
            block = near(z, ORDER[b][0]) * SIDE + near(y, ORDER[b][1])
            pieces.append(dnw[pl.ds(pl.multiple_of(block * 4 * half, 4 * half), 4 * half), :])
        both = dot(hid[...], jnp.concatenate(pieces, axis=1) if len(pieces) > 1 else pieces[0])
        for i, b in enumerate(group):
            terms = both[:, i * rows:(i + 1) * rows]
            for side, by in ((0, 1), (1, -1)):
                row = 3 * rows + side * (rows // 2)
                first_out[side, b] = code_pairs(terms[row:row + rows // 2])
                copy(first_out.at[side, b], first.at[side, b], rs_send, first_recv.at[side, b], device(dx=by)).start()
            part[b * 3 * rows:(b + 1) * 3 * rows, :] = terms[:3 * rows]

    def pass_on(b):
        for side, by in ((0, 1), (1, -1)):
            copy(first.at[side, b], first.at[side, b], rs_send, first_recv.at[side, b], device(dx=by)).wait_recv()
            slot = 2 - side
            near_half, far_half = part_at(b, slot, side, 1)[...], part_at(b, slot, 1 - side, 1)[...]
            summed = near_half + decode_pairs(first[side, b])
            ordered = [summed, far_half] if side == 0 else [far_half, summed]
            last_out[side, b] = code_triples(jnp.concatenate(ordered, axis=0))
            copy(last_out.at[side, b], last.at[side, b], rs_send, last_recv.at[side, b], device(dx=by)).start()

    def stored(b):
        block = near(z, ORDER[b][0]) * SIDE + near(y, ORDER[b][1])
        return pltpu.make_async_copy(
            out_ref.at[b], out_hbm.at[:, pl.ds(pl.multiple_of(block * rows, rows), rows)], store.at[b]
        )

    def finish(b):
        for side, by in ((0, 1), (1, -1)):
            copy(last.at[side, b], last.at[side, b], rs_send, last_recv.at[side, b], device(dx=by)).wait_recv()
        total = part_at(b, 0)[...] + decode_triples(last[0, b]) + decode_triples(last[1, b])
        out_ref[b] = total.astype(BF)
        stored(b).start()

    def step(g):
        if g < len(GROUPS):
            project(GROUPS[g])
        if 0 <= g - 1 < len(GROUPS):
            for b in GROUPS[g - 1]:
                pass_on(b)
        if 0 <= g - 3 < len(GROUPS):
            for b in GROUPS[g - 3]:
                finish(b)

    step(0)
    dn.first_axis()
    dn.relay(0)
    for b in (1, 2, 3, 4):
        dn_share(b)
    dn.far_first()
    step(1)
    dn.relay(1)
    step(2)
    dn.relay(2)
    for b in (5, 6, 7, 8):
        dn_share(b)
    dn.far_second(0)
    for b in (9, 10):
        dn_share(b)
    step(3)
    dn.relay(3)
    step(4)
    dn.far_second(1)
    dn.far_second(2)
    for b in (11, 12, 13, 14):
        dn_share(b)
    step(5)
    dn.far_second(3)
    dn_share(15)
    for g in range(6, len(GROUPS) + 3):
        step(g)

    def drained(ref, sem):
        pltpu.make_async_copy(ref, ref, sem).wait()

    drained(upw.at[pl.ds(0, 15 * 4 * depth // 2), :], up_send)
    drained(dnw.at[pl.ds(0, 15 * 4 * half // 2), :], dn_send)
    drained(upw.at[pl.ds(0, 2 * blocks * depth), :], up_pair_send)
    drained(dnw.at[pl.ds(0, blocks * 2 * half), :], dn_pair_send)
    drained(tok.at[pl.ds(0, 3 * rows), :], tok_send)
    drained(part.at[0:blocks * (5 * rows // 8 + 3 * rows // 2), :], rs_send)
    for b in range(blocks):
        stored(b).wait()


def shards(tokens, norm_gain, up_weight, down_weight):
    rows, width = tokens.shape
    depth, inner = up_weight.shape
    blocks = SIDE * SIDE
    vmem = pl.BlockSpec(memory_space=pltpu.VMEM)
    anywhere = pl.BlockSpec(memory_space=pl.ANY)
    dma = pltpu.SemaphoreType.DMA
    return pl.pallas_call(
        kernel,
        out_shape=jax.ShapeDtypeStruct((rows, width), BF),
        in_specs=[anywhere, vmem, anywhere, anywhere],
        out_specs=anywhere,
        scratch_shapes=[
            pltpu.VMEM(tokens.shape, BF),
            pltpu.VMEM(up_weight.shape, F32),
            pltpu.VMEM(down_weight.shape, F32),
            pltpu.VMEM((blocks, rows, rows), BF),
            pltpu.VMEM((SIDE * rows, width), BF),
            pltpu.VMEM((4 * blocks * depth, inner // 2), BF),
            pltpu.VMEM((blocks * 2 * inner, rows), BF),
            pltpu.VMEM((SIDE * rows, 2 * inner), F32),
            pltpu.VMEM((SIDE * rows, 2 * inner), BF),
            pltpu.VMEM((blocks * 3 * rows, rows), F32),
            pltpu.VMEM((2, blocks, 5 * rows // 16, rows), F32),
            pltpu.VMEM((2, blocks, 3 * rows // 4, rows), F32),
            pltpu.VMEM((2, blocks, 5 * rows // 16, rows), F32),
            pltpu.VMEM((2, blocks, 3 * rows // 4, rows), F32),
            dma((2, 5, 4)), dma((2, 5, 4)), dma((2, 4)), dma((blocks,)), dma((6,)), dma((2, blocks)), dma((2, blocks)),
            dma, dma, dma, dma, dma, dma, dma((3,)), dma((blocks,)),
        ],
        compiler_params=pltpu.CompilerParams(
            collective_id=0, has_side_effects=True, vmem_limit_bytes=60 * 1024 * 1024
        ),
    )(tokens, norm_gain.reshape(1, width), up_weight, down_weight)


def solution(mesh):
    placed = (P(("fs", "tp"), None), P(), P("fs", "tp"), P("tp", "fs"))
    return jax.shard_map(
        shards, mesh=mesh, in_specs=placed, out_specs=P(("fs", "tp"), None), check_vma=False
    )
```

```python
import jax
import jax.numpy as jnp
from jax import lax
from jax.experimental import pallas as pl
from jax.experimental.pallas import tpu as pltpu
from jax.sharding import PartitionSpec as P

epsilon = 1e-06
MESH = pl.DeviceIdType.MESH
SIDE = 4
OFFSETS = (0, -1, 1, 2)
BF = jnp.bfloat16
F32 = jnp.float32

ORDER = (
    (0, 0),
    (0, -1), (0, 1), (-1, 0), (1, 0),
    (-1, -1), (1, 1), (-1, 1), (1, -1),
    (2, 0), (0, 2),
    (-1, 2), (2, -1), (1, 2), (2, 1),
    (2, 2),
)


GROUPS = ((0,), (1, 2), (3, 4), (5, 6), (7, 8), (9, 10), (11, 12), (13, 14), (15,))


def coded_rows(rows):
    n = rows // 8
    return 8 * (2 * (n // 3) + n % 3)


def code(values):
    groups = values.reshape(-1, 8, values.shape[1])
    top = jnp.maximum(jnp.max(jnp.abs(groups), axis=0), 1e-20)
    exponent = jnp.ceil(jnp.log2(top * (1.0 / 32767.0)) + 0.001)
    inverse = jnp.exp2(-exponent)
    n = groups.shape[0] // 3
    a, b, c = (jnp.round(groups[i * n:(i + 1) * n] * inverse) for i in range(3))
    last = jnp.round(groups[-1] * inverse) * 256.0 + (exponent + 128.0)
    high = jnp.floor(c * (1.0 / 256.0))
    low = c - high * 256.0
    parts = [a * 256.0 + low, b * 256.0 + (high + 128.0), groups[3 * n:-1], last[None]]
    return jnp.concatenate([p for p in parts if p.shape[0]], axis=0).reshape(-1, values.shape[1])


def decode(coded):
    groups = coded.reshape(-1, 8, coded.shape[1])
    n = groups.shape[0] // 2 if groups.shape[0] % 2 else groups.shape[0] // 2 - 1
    first, second, rest = groups[:n], groups[n:2 * n], groups[2 * n:-1]
    level = jnp.floor(groups[-1] * (1.0 / 256.0))
    unit = jnp.exp2(groups[-1] - level * 256.0 - 128.0)
    a = jnp.floor(first * (1.0 / 256.0))
    b = jnp.floor(second * (1.0 / 256.0))
    c = (second - b * 256.0 - 128.0) * 256.0 + (first - a * 256.0)
    parts = [a * unit, b * unit, c * unit, rest, (level * unit)[None]]
    return jnp.concatenate([p for p in parts if p.shape[0]], axis=0).reshape(-1, coded.shape[1])


def kernel(
    tokens_hbm, gain_ref, up_hbm, down_hbm, out_hbm,
    tokens_ref, up_ref, down_ref, out_ref, tok, upw, dnw, pre, hid, part, first, last, first_out, last_out,
    up_recv, dn_recv, up_pair, dn_pair, tok_recv, first_recv, last_recv,
    up_send, dn_send, up_pair_send, dn_pair_send, tok_send, rs_send, load, store,
):
    rows, width = tokens_ref.shape
    half = up_ref.shape[1] // 2
    depth = up_ref.shape[0]
    blocks = SIDE * SIDE
    fs = lax.axis_index("fs")
    tp = lax.axis_index("tp")
    z, y, x, core = fs // SIDE, fs % SIDE, tp // 2, tp % 2

    def near(at, by):
        return (at + (by + SIDE)) % SIDE

    def device(dz=0, dy=0, dx=0):
        return {"fs": near(z, dz) * SIDE + near(y, dy), "tp": near(x, dx) * 2 + core}

    partner = {"fs": fs, "tp": x * 2 + (1 - core)}

    def copy(src, dst, send_sem, recv_sem, to):
        return pltpu.make_async_remote_copy(
            src_ref=src, dst_ref=dst, send_sem=send_sem, recv_sem=recv_sem,
            device_id=to, device_id_type=MESH,
        )

    barrier = pltpu.get_barrier_semaphore()
    peers = [device(dz=1), device(dz=-1), device(dy=1), device(dy=-1), device(dx=1), device(dx=-1), partner]
    for peer in peers:
        pl.semaphore_signal(barrier, inc=1, device_id=peer, device_id_type=MESH)

    loads = [
        pltpu.make_async_copy(src, dst, load.at[i])
        for i, (src, dst) in enumerate(((up_hbm, up_ref), (tokens_hbm, tokens_ref), (down_hbm, down_ref)))
    ]
    for one in loads:
        one.start()

    def up_at(h, dz, dy, q, n):
        zs, ys = near(z, dz), near(y, dy)
        block = zs * SIDE + ys if h == 0 else ys * SIDE + zs
        row = h * blocks * depth + block * depth + q * (depth // 2)
        return upw.at[pl.ds(pl.multiple_of(row, depth // 2), n * (depth // 2)), :]

    def dn_at(h, dz, dy, q, n):
        block = near(z, dz) * SIDE + near(y, dy)
        row = block * 4 * half + h * half + q * (half // 2)
        return dnw.at[pl.ds(pl.multiple_of(row, half // 2), n * (half // 2)), :]

    class Gather:
        def __init__(self, at, recv, send):
            self.at, self.recv, self.send = at, recv, send

        def piece(self, h, df, ds, q=0, n=2):
            return self.at(h, ds, df, q, n) if h == 0 else self.at(h, df, ds, q, n)

        def peer(self, h, axis, by):
            along_y = (h == 0) == (axis == 0)
            return device(dy=by) if along_y else device(dz=by)

        def post(self, h, stage, slot, df, ds, q=0, n=2):
            ref = self.piece(h, df, ds, q, n)
            by = 1 if slot % 2 == 0 else -1
            copy(ref, ref, self.send, self.recv.at[h, stage, slot], self.peer(h, min(stage, 1), by)).start()

        def wait(self, h, stage, slot, df, ds, q=0, n=2):
            ref = self.piece(h, df, ds, q, n)
            copy(ref, ref, self.send, self.recv.at[h, stage, slot], self.peer(h, 0, 1)).wait_recv()

        def start_first(self):
            for h in (0, 1):
                for slot in (0, 1):
                    self.post(h, 0, slot, 0, 0)

        def start_second(self):
            for h in (0, 1):
                for slot in (0, 1):
                    self.post(h, 1, slot, 0, 0)

        def second(self, h, j):
            for slot in (0, 1):
                self.post(h, 1 + j, slot, OFFSETS[j], 0)

        def first_axis(self):
            for h in (0, 1):
                self.wait(h, 0, 0, -1, 0)
                self.post(h, 0, 2, -1, 0, 0, 1)
                self.wait(h, 0, 1, 1, 0)
                self.post(h, 0, 3, 1, 0, 1, 1)
            for near_first in (0, 1):
                for h in (0, 1):
                    for slot in (0, 1):
                        j = 1 + (near_first + slot) % 2
                        self.post(h, 1 + j, slot, OFFSETS[j], 0)

        def far_first(self):
            for h in (0, 1):
                self.wait(h, 0, 2, 2, 0, 0, 1)
                self.wait(h, 0, 3, 2, 0, 1, 1)
                self.second(h, 3)

        def relay(self, minus, plus):
            for h in (0, 1):
                for slot, j in ((0, minus), (1, plus)):
                    by = -1 if slot == 0 else 1
                    self.wait(h, 1 + j, slot, OFFSETS[j], by)
                    self.post(h, 1 + j, 2 + slot, OFFSETS[j], by, slot, 1)

        def far_second(self, j):
            for h in (0, 1):
                self.wait(h, 1 + j, 2, OFFSETS[j], 2, 0, 1)
                self.wait(h, 1 + j, 3, OFFSETS[j], 2, 1, 1)

    up = Gather(up_at, up_recv, up_send)
    dn = Gather(dn_at, dn_recv, dn_send)

    loads[0].wait()
    for h in (0, 1):
        block = fs if h == 0 else y * SIDE + z
        row = pl.multiple_of(h * blocks * depth + block * depth, depth)
        upw[pl.ds(row, depth), :] = up_ref[:, h * half:(h + 1) * half].astype(BF)
    pl.semaphore_wait(barrier, len(peers))
    up.start_first()

    loads[1].wait()
    values = tokens_ref[...].astype(F32)
    scale = lax.rsqrt(jnp.mean(values * values, axis=-1, keepdims=True) + epsilon)
    tok[0:rows, :] = (values * scale * gain_ref[...]).astype(BF)

    def tok_at(slot, q):
        row = slot * rows + q * (rows // 2)
        return tok.at[row:row + rows // 2, :]

    def tok_post(sem, slot, there, q, by):
        copy(tok_at(slot, q), tok_at(there, q), tok_send, tok_recv.at[sem], device(dx=by)).start()

    def tok_wait(sem, slot, q):
        copy(tok_at(slot, q), tok_at(slot, q), tok_send, tok_recv.at[sem], device(dx=1)).wait_recv()

    tok_post(0, 0, 1, 0, 1)
    tok_post(3, 0, 2, 1, -1)
    tok_post(1, 0, 1, 1, 1)
    tok_post(2, 0, 2, 0, -1)
    up.start_second()
    loads[2].wait()

    own = pl.multiple_of(fs * 4 * half, 4 * half)
    dnw[pl.ds(own, 2 * half), :] = down_ref[...].astype(BF)

    def dn_block(b, to_partner):
        block = near(z, ORDER[b][0]) * SIDE + near(y, ORDER[b][1])
        row = block * 4 * half + (2 * half if to_partner else 0)
        return dnw.at[pl.ds(pl.multiple_of(row, 2 * half), 2 * half), :]

    def dn_share(b):
        copy(dn_block(b, False), dn_block(b, True), dn_pair_send, dn_pair.at[b], partner).start()

    def up_plane(h, p, to_partner):
        plane = near(z if h == 0 else y, OFFSETS[p])
        row = (h + (2 if to_partner else 0)) * blocks * depth + plane * SIDE * depth
        return upw.at[pl.ds(pl.multiple_of(row, SIDE * depth), SIDE * depth), :]

    def up_share(j, p):
        for h in (0, 1):
            plane = near(z if h == 0 else y, OFFSETS[p])
            row = (plane * SIDE + near(y if h == 0 else z, OFFSETS[j])) * depth
            mine, theirs = (
                upw.at[pl.ds(pl.multiple_of((h + 2 * side) * blocks * depth + row, depth), depth), :] for side in (0, 1)
            )
            copy(mine, theirs, up_pair_send, up_pair.at[h, p], partner).start()

    def up_shared(p):
        for h in (0, 1):
            ref = up_plane(h, p, True)
            copy(ref, ref, up_pair_send, up_pair.at[h, p], partner).wait_recv()

    up_share(0, 0)
    dn_share(0)

    up.first_axis()
    up_share(1, 0)
    up_share(2, 0)
    up.relay(0, 0)
    up_share(0, 1)
    up_share(0, 2)
    up.far_first()
    up_share(3, 0)
    tok_wait(0, 1, 0)
    tok_post(4, 1, 3, 0, 1)
    tok_wait(3, 2, 1)
    tok_post(5, 2, 3, 1, -1)
    for minus, plus in ((1, 2), (2, 1), (3, 3)):
        up.relay(minus, plus)
        up_share(minus, 1)
        up_share(plus, 2)
    dn.start_first()
    dn.start_second()
    tok_wait(1, 1, 1)
    tok_wait(2, 2, 0)
    tok_wait(4, 3, 0)
    tok_wait(5, 3, 1)

    def columns_of(h, p):
        plane = near(z if h == 0 else y, OFFSETS[p])
        if h == 0:
            return tok[:, pl.ds(pl.multiple_of(plane * SIDE * depth, SIDE * depth), SIDE * depth)]
        return jnp.concatenate(
            [tok[:, pl.ds(pl.multiple_of((a * SIDE + plane) * depth, depth), depth)] for a in range(SIDE)], axis=1
        )

    def dot(a, b):
        return jnp.dot(a, b, preferred_element_type=F32)

    tile = 256

    def early(h, other):
        for n in range(half // tile):
            cols = slice(n * tile, (n + 1) * tile)
            total = sum(dot(columns_of(h, p), up_plane(h, p, other)[:, cols]) for p in (0, 1, 2))
            at = (2 * other + h) * half + n * tile
            pre[:, at:at + tile] = total

    def late(h, other):
        for n in range(half // tile):
            cols = slice(n * tile, (n + 1) * tile)
            at = (2 * other + h) * half + n * tile
            total = pre[:, at:at + tile] + dot(columns_of(h, 3), up_plane(h, 3, other)[:, cols])
            hid[:, at:at + tile] = jnp.square(jnp.maximum(total, 0.0)).astype(BF)

    for h in (0, 1):
        early(h, 0)
    for p in (0, 1, 2):
        up_shared(p)
    for j in (0, 1):
        up.far_second(j)
        up_share(j, 3)
    for h in (0, 1):
        early(h, 1)
    for j in (2, 3):
        up.far_second(j)
        up_share(j, 3)
    for h in (0, 1):
        late(h, 0)
    up_shared(3)
    for h in (0, 1):
        late(h, 1)

    def part_at(b, slot, q=0, n=2):
        row = (b * 3 + slot) * rows + q * (rows // 2)
        return part.at[row:row + n * (rows // 2), :]

    def project(group):
        pieces = []
        for b in group:
            ref = dn_block(b, True)
            copy(ref, ref, dn_pair_send, dn_pair.at[b], partner).wait_recv()
            block = near(z, ORDER[b][0]) * SIDE + near(y, ORDER[b][1])
            pieces.append(dnw[pl.ds(pl.multiple_of(block * 4 * half, 4 * half), 4 * half), :])
        both = dot(hid[...], jnp.concatenate(pieces, axis=1) if len(pieces) > 1 else pieces[0])
        g = GROUPS.index(group)
        terms = [both[:, i * rows:(i + 1) * rows] for i in range(len(group))]
        for side, by in ((0, 1), (1, -1)):
            row = 3 * rows + side * (rows // 2)
            out, there = first_at(first_out, side, g), first_at(first, side, g)
            out[...] = code(jnp.concatenate([t[row:row + rows // 2] for t in terms], axis=0))
            copy(out, there, rs_send, first_recv.at[side, g], device(dx=by)).start()
        for b, t in zip(group, terms):
            part[b * 3 * rows:(b + 1) * 3 * rows, :] = t[:3 * rows]

    def first_at(ref, side, g):
        return ref.at[side, g, 0:coded_rows(len(GROUPS[g]) * rows // 2), :]

    def last_at(ref, side, g):
        return ref.at[side, g, 0:coded_rows(len(GROUPS[g]) * rows), :]

    def pass_on(g):
        for side, by in ((0, 1), (1, -1)):
            here = first_at(first, side, g)
            copy(here, here, rs_send, first_recv.at[side, g], device(dx=by)).wait_recv()
            slot = 2 - side
            got = decode(here[...])
            ordered = []
            for i, b in enumerate(GROUPS[g]):
                summed = part_at(b, slot, side, 1)[...] + got[i * (rows // 2):(i + 1) * (rows // 2)]
                other = part_at(b, slot, 1 - side, 1)[...]
                ordered += [summed, other] if side == 0 else [other, summed]
            out, there = last_at(last_out, side, g), last_at(last, side, g)
            out[...] = code(jnp.concatenate(ordered, axis=0))
            copy(out, there, rs_send, last_recv.at[side, g], device(dx=by)).start()

    def stored(b):
        block = near(z, ORDER[b][0]) * SIDE + near(y, ORDER[b][1])
        return pltpu.make_async_copy(
            out_ref.at[b], out_hbm.at[:, pl.ds(pl.multiple_of(block * rows, rows), rows)], store.at[b]
        )

    def finish(g):
        for side, by in ((0, 1), (1, -1)):
            here = last_at(last, side, g)
            copy(here, here, rs_send, last_recv.at[side, g], device(dx=by)).wait_recv()
        got = decode(last_at(last, 0, g)[...]) + decode(last_at(last, 1, g)[...])
        for i, b in enumerate(GROUPS[g]):
            out_ref[b] = (part_at(b, 0)[...] + got[i * rows:(i + 1) * rows]).astype(BF)
            stored(b).start()

    def share(*bs):
        for b in bs:
            dn_share(b)

    project(GROUPS[0])
    dn.first_axis()
    dn.relay(0, 0)
    share(1, 2, 3, 4)
    project(GROUPS[1])
    pass_on(0)
    project(GROUPS[2])
    dn.far_first()
    pass_on(1)
    dn.relay(1, 2)
    share(5, 6)
    pass_on(2)
    finish(0)
    project(GROUPS[3])
    dn.relay(2, 1)
    share(7, 8)
    dn.far_second(0)
    share(9, 10)
    project(GROUPS[4])
    pass_on(3)
    project(GROUPS[5])
    finish(1)
    dn.relay(3, 3)
    pass_on(4)
    dn.far_second(1)
    finish(2)
    dn.far_second(2)
    share(11, 12, 13, 14)
    pass_on(5)
    dn.far_second(3)
    share(15)
    project(GROUPS[6])
    finish(3)
    project(GROUPS[7])
    project(GROUPS[8])
    pass_on(6)
    finish(4)
    pass_on(7)
    pass_on(8)
    for g in (5, 6, 7, 8):
        finish(g)

    def drained(ref, sem):
        pltpu.make_async_copy(ref, ref, sem).wait()

    drained(upw.at[pl.ds(0, 15 * 4 * depth // 2), :], up_send)
    drained(dnw.at[pl.ds(0, 15 * 4 * half // 2), :], dn_send)
    drained(upw.at[pl.ds(0, 2 * blocks * depth), :], up_pair_send)
    drained(dnw.at[pl.ds(0, blocks * 2 * half), :], dn_pair_send)
    drained(tok.at[pl.ds(0, 3 * rows), :], tok_send)
    sent = sum(coded_rows(len(g) * rows // 2) + coded_rows(len(g) * rows) for g in GROUPS)
    drained(part.at[0:2 * sent, :], rs_send)
    for b in range(blocks):
        stored(b).wait()


def shards(tokens, norm_gain, up_weight, down_weight):
    rows, width = tokens.shape
    depth, inner = up_weight.shape
    blocks = SIDE * SIDE
    vmem = pl.BlockSpec(memory_space=pltpu.VMEM)
    anywhere = pl.BlockSpec(memory_space=pl.ANY)
    dma = pltpu.SemaphoreType.DMA
    return pl.pallas_call(
        kernel,
        out_shape=jax.ShapeDtypeStruct((rows, width), BF),
        in_specs=[anywhere, vmem, anywhere, anywhere],
        out_specs=anywhere,
        scratch_shapes=[
            pltpu.VMEM(tokens.shape, BF),
            pltpu.VMEM(up_weight.shape, F32),
            pltpu.VMEM(down_weight.shape, F32),
            pltpu.VMEM((blocks, rows, rows), BF),
            pltpu.VMEM((SIDE * rows, width), BF),
            pltpu.VMEM((4 * blocks * depth, inner // 2), BF),
            pltpu.VMEM((blocks * 2 * inner, rows), BF),
            pltpu.VMEM((SIDE * rows, 2 * inner), F32),
            pltpu.VMEM((SIDE * rows, 2 * inner), BF),
            pltpu.VMEM((blocks * 3 * rows, rows), F32),
            pltpu.VMEM((2, len(GROUPS), coded_rows(rows), rows), F32),
            pltpu.VMEM((2, len(GROUPS), coded_rows(2 * rows), rows), F32),
            pltpu.VMEM((2, len(GROUPS), coded_rows(rows), rows), F32),
            pltpu.VMEM((2, len(GROUPS), coded_rows(2 * rows), rows), F32),
            dma((2, 5, 4)), dma((2, 5, 4)), dma((2, 4)), dma((blocks,)), dma((6,)), dma((2, len(GROUPS))), dma((2, len(GROUPS))),
            dma, dma, dma, dma, dma, dma, dma((3,)), dma((blocks,)),
        ],
        compiler_params=pltpu.CompilerParams(
            collective_id=0, has_side_effects=True, vmem_limit_bytes=60 * 1024 * 1024
        ),
    )(tokens, norm_gain.reshape(1, width), up_weight, down_weight)


def solution(mesh):
    placed = (P(("fs", "tp"), None), P(), P("fs", "tp"), P("tp", "fs"))
    return jax.shard_map(
        shards, mesh=mesh, in_specs=placed, out_specs=P(("fs", "tp"), None), check_vma=False
    )
```

```python
import jax
import jax.numpy as jnp
from jax import lax
from jax.experimental import pallas as pl
from jax.experimental.pallas import tpu as pltpu
from jax.sharding import PartitionSpec as P

epsilon = 1e-06
MESH = pl.DeviceIdType.MESH
SIDE = 4
OFFSETS = (0, -1, 1, 2)
BF = jnp.bfloat16
F32 = jnp.float32

ORDER = (
    (0, 0),
    (0, -1), (0, 1), (-1, 0), (1, 0),
    (-1, -1), (1, 1), (-1, 1), (1, -1),
    (2, 0), (0, 2),
    (-1, 2), (2, -1), (1, 2), (2, 1),
    (2, 2),
)


GROUPS = ((0,), (1, 2), (3, 4), (5, 6), (7, 8), (9, 10), (11, 12), (13, 14), (15,))


def coded_rows(rows):
    n = rows // 8
    return 8 * (2 * (n // 3) + n % 3)


def code(values):
    groups = values.reshape(-1, 8, values.shape[1])
    top = jnp.maximum(jnp.max(jnp.abs(groups), axis=0), 1e-20)
    exponent = jnp.ceil(jnp.log2(top * (1.0 / 32767.0)) + 0.001)
    inverse = jnp.exp2(-exponent)
    n = groups.shape[0] // 3
    a, b, c = (jnp.round(groups[i * n:(i + 1) * n] * inverse) for i in range(3))
    last = jnp.round(groups[-1] * inverse) * 256.0 + (exponent + 128.0)
    high = jnp.floor(c * (1.0 / 256.0))
    low = c - high * 256.0
    parts = [a * 256.0 + low, b * 256.0 + (high + 128.0), groups[3 * n:-1], last[None]]
    return jnp.concatenate([p for p in parts if p.shape[0]], axis=0).reshape(-1, values.shape[1])


def decode(coded):
    groups = coded.reshape(-1, 8, coded.shape[1])
    n = groups.shape[0] // 2 if groups.shape[0] % 2 else groups.shape[0] // 2 - 1
    first, second, rest = groups[:n], groups[n:2 * n], groups[2 * n:-1]
    level = jnp.floor(groups[-1] * (1.0 / 256.0))
    unit = jnp.exp2(groups[-1] - level * 256.0 - 128.0)
    a = jnp.floor(first * (1.0 / 256.0))
    b = jnp.floor(second * (1.0 / 256.0))
    c = (second - b * 256.0 - 128.0) * 256.0 + (first - a * 256.0)
    parts = [a * unit, b * unit, c * unit, rest, (level * unit)[None]]
    return jnp.concatenate([p for p in parts if p.shape[0]], axis=0).reshape(-1, coded.shape[1])


def kernel(
    tokens_hbm, gain_ref, up_hbm, down_hbm, out_hbm,
    tokens_ref, up_ref, down_ref, out_ref, tok, upw, dnw, pre, hid, part, first, last, first_out, last_out,
    up_recv, dn_recv, up_pair, dn_pair, tok_recv, first_recv, last_recv,
    up_send, dn_send, up_pair_send, dn_pair_send, tok_send, rs_send, load, store,
):
    rows, width = tokens_ref.shape
    half = up_ref.shape[1] // 2
    depth = up_ref.shape[0]
    blocks = SIDE * SIDE
    fs = lax.axis_index("fs")
    tp = lax.axis_index("tp")
    z, y, x, core = fs // SIDE, fs % SIDE, tp // 2, tp % 2

    def near(at, by):
        return (at + (by + SIDE)) % SIDE

    def device(dz=0, dy=0, dx=0):
        return {"fs": near(z, dz) * SIDE + near(y, dy), "tp": near(x, dx) * 2 + core}

    partner = {"fs": fs, "tp": x * 2 + (1 - core)}

    def copy(src, dst, send_sem, recv_sem, to):
        return pltpu.make_async_remote_copy(
            src_ref=src, dst_ref=dst, send_sem=send_sem, recv_sem=recv_sem,
            device_id=to, device_id_type=MESH,
        )

    barrier = pltpu.get_barrier_semaphore()
    peers = [device(dz=1), device(dz=-1), device(dy=1), device(dy=-1), device(dx=1), device(dx=-1), partner]
    for peer in peers:
        pl.semaphore_signal(barrier, inc=1, device_id=peer, device_id_type=MESH)

    loads = [
        pltpu.make_async_copy(src, dst, load.at[i])
        for i, (src, dst) in enumerate(((up_hbm, up_ref), (tokens_hbm, tokens_ref), (down_hbm, down_ref)))
    ]
    for one in loads:
        one.start()

    def up_at(h, dz, dy, q, n):
        zs, ys = near(z, dz), near(y, dy)
        block = zs * SIDE + ys if h == 0 else ys * SIDE + zs
        row = h * blocks * depth + block * depth + q * (depth // 2)
        return upw.at[pl.ds(pl.multiple_of(row, depth // 2), n * (depth // 2)), :]

    def dn_at(h, dz, dy, q, n):
        block = near(z, dz) * SIDE + near(y, dy)
        row = block * 4 * half + h * half + q * (half // 2)
        return dnw.at[pl.ds(pl.multiple_of(row, half // 2), n * (half // 2)), :]

    class Gather:
        def __init__(self, at, recv, send):
            self.at, self.recv, self.send = at, recv, send

        def piece(self, h, df, ds, q=0, n=2):
            return self.at(h, ds, df, q, n) if h == 0 else self.at(h, df, ds, q, n)

        def peer(self, h, axis, by):
            along_y = (h == 0) == (axis == 0)
            return device(dy=by) if along_y else device(dz=by)

        def post(self, h, stage, slot, df, ds, q=0, n=2):
            ref = self.piece(h, df, ds, q, n)
            by = 1 if slot % 2 == 0 else -1
            copy(ref, ref, self.send, self.recv.at[h, stage, slot], self.peer(h, min(stage, 1), by)).start()

        def wait(self, h, stage, slot, df, ds, q=0, n=2):
            ref = self.piece(h, df, ds, q, n)
            copy(ref, ref, self.send, self.recv.at[h, stage, slot], self.peer(h, 0, 1)).wait_recv()

        def start_first(self):
            for h in (0, 1):
                for slot in (0, 1):
                    self.post(h, 0, slot, 0, 0)

        def start_second(self):
            for h in (0, 1):
                for slot in (0, 1):
                    self.post(h, 1, slot, 0, 0)

        def second(self, h, j):
            for slot in (0, 1):
                self.post(h, 1 + j, slot, OFFSETS[j], 0)

        def first_axis(self):
            for h in (0, 1):
                self.wait(h, 0, 0, -1, 0)
                self.post(h, 0, 2, -1, 0, 0, 1)
                self.wait(h, 0, 1, 1, 0)
                self.post(h, 0, 3, 1, 0, 1, 1)
            for near_first in (0, 1):
                for h in (0, 1):
                    for slot in (0, 1):
                        j = 1 + (near_first + slot) % 2
                        self.post(h, 1 + j, slot, OFFSETS[j], 0)

        def far_first(self):
            for h in (0, 1):
                self.wait(h, 0, 2, 2, 0, 0, 1)
                self.wait(h, 0, 3, 2, 0, 1, 1)
                self.second(h, 3)

        def relay(self, minus, plus):
            for h in (0, 1):
                for slot, j in ((0, minus), (1, plus)):
                    by = -1 if slot == 0 else 1
                    self.wait(h, 1 + j, slot, OFFSETS[j], by)
                    self.post(h, 1 + j, 2 + slot, OFFSETS[j], by, slot, 1)

        def far_second(self, j):
            for h in (0, 1):
                self.wait(h, 1 + j, 2, OFFSETS[j], 2, 0, 1)
                self.wait(h, 1 + j, 3, OFFSETS[j], 2, 1, 1)

    up = Gather(up_at, up_recv, up_send)
    dn = Gather(dn_at, dn_recv, dn_send)

    loads[0].wait()
    for h in (0, 1):
        block = fs if h == 0 else y * SIDE + z
        row = pl.multiple_of(h * blocks * depth + block * depth, depth)
        upw[pl.ds(row, depth), :] = up_ref[:, h * half:(h + 1) * half].astype(BF)
    pl.semaphore_wait(barrier, len(peers))
    up.start_first()

    loads[1].wait()
    values = tokens_ref[...].astype(F32)
    scale = lax.rsqrt(jnp.mean(values * values, axis=-1, keepdims=True) + epsilon)
    tok[0:rows, :] = (values * scale * gain_ref[...]).astype(BF)

    def tok_at(slot, q):
        row = slot * rows + q * (rows // 2)
        return tok.at[row:row + rows // 2, :]

    def tok_post(sem, slot, there, q, by):
        copy(tok_at(slot, q), tok_at(there, q), tok_send, tok_recv.at[sem], device(dx=by)).start()

    def tok_wait(sem, slot, q):
        copy(tok_at(slot, q), tok_at(slot, q), tok_send, tok_recv.at[sem], device(dx=1)).wait_recv()

    tok_post(0, 0, 1, 0, 1)
    tok_post(3, 0, 2, 1, -1)
    tok_post(1, 0, 1, 1, 1)
    tok_post(2, 0, 2, 0, -1)
    up.start_second()
    loads[2].wait()

    own = pl.multiple_of(fs * 4 * half, 4 * half)
    dnw[pl.ds(own, 2 * half), :] = down_ref[...].astype(BF)

    def dn_block(b, to_partner):
        block = near(z, ORDER[b][0]) * SIDE + near(y, ORDER[b][1])
        row = block * 4 * half + (2 * half if to_partner else 0)
        return dnw.at[pl.ds(pl.multiple_of(row, 2 * half), 2 * half), :]

    def dn_share(h, *bs):
        for b in bs:
            block = near(z, ORDER[b][0]) * SIDE + near(y, ORDER[b][1])
            mine, theirs = (
                dnw.at[pl.ds(pl.multiple_of(block * 4 * half + (2 * side + h) * half, half), half), :] for side in (0, 1)
            )
            copy(mine, theirs, dn_pair_send, dn_pair.at[b], partner).start()

    def up_plane(h, p, to_partner):
        plane = near(z if h == 0 else y, OFFSETS[p])
        row = (h + (2 if to_partner else 0)) * blocks * depth + plane * SIDE * depth
        return upw.at[pl.ds(pl.multiple_of(row, SIDE * depth), SIDE * depth), :]

    def up_share(j, p):
        for h in (0, 1):
            plane = near(z if h == 0 else y, OFFSETS[p])
            row = (plane * SIDE + near(y if h == 0 else z, OFFSETS[j])) * depth
            mine, theirs = (
                upw.at[pl.ds(pl.multiple_of((h + 2 * side) * blocks * depth + row, depth), depth), :] for side in (0, 1)
            )
            copy(mine, theirs, up_pair_send, up_pair.at[h, p], partner).start()

    def up_shared(p):
        for h in (0, 1):
            ref = up_plane(h, p, True)
            copy(ref, ref, up_pair_send, up_pair.at[h, p], partner).wait_recv()

    up_share(0, 0)
    for h in (0, 1):
        dn_share(h, 0)

    up.first_axis()
    up_share(1, 0)
    up_share(2, 0)
    up.relay(0, 0)
    up_share(0, 1)
    up_share(0, 2)
    up.far_first()
    up_share(3, 0)
    tok_wait(0, 1, 0)
    tok_post(4, 1, 3, 0, 1)
    tok_wait(3, 2, 1)
    tok_post(5, 2, 3, 1, -1)
    for minus, plus in ((1, 2), (2, 1), (3, 3)):
        up.relay(minus, plus)
        up_share(minus, 1)
        up_share(plus, 2)
    dn.start_first()
    dn.start_second()
    tok_wait(1, 1, 1)
    tok_wait(2, 2, 0)
    tok_wait(4, 3, 0)
    tok_wait(5, 3, 1)

    def columns_of(h, p):
        plane = near(z if h == 0 else y, OFFSETS[p])
        if h == 0:
            return tok[:, pl.ds(pl.multiple_of(plane * SIDE * depth, SIDE * depth), SIDE * depth)]
        return jnp.concatenate(
            [tok[:, pl.ds(pl.multiple_of((a * SIDE + plane) * depth, depth), depth)] for a in range(SIDE)], axis=1
        )

    def dot(a, b):
        return jnp.dot(a, b, preferred_element_type=F32)

    tile = 256

    def early(h, other):
        for n in range(half // tile):
            cols = slice(n * tile, (n + 1) * tile)
            total = sum(dot(columns_of(h, p), up_plane(h, p, other)[:, cols]) for p in (0, 1, 2))
            at = (2 * other + h) * half + n * tile
            pre[:, at:at + tile] = total

    def late(h, other):
        for n in range(half // tile):
            cols = slice(n * tile, (n + 1) * tile)
            at = (2 * other + h) * half + n * tile
            total = pre[:, at:at + tile] + dot(columns_of(h, 3), up_plane(h, 3, other)[:, cols])
            hid[:, at:at + tile] = jnp.square(jnp.maximum(total, 0.0)).astype(BF)

    for h in (0, 1):
        early(h, 0)
    for p in (0, 1, 2):
        up_shared(p)
    for j in (0, 1):
        up.far_second(j)
        up_share(j, 3)
    for h in (0, 1):
        early(h, 1)
    for j in (2, 3):
        up.far_second(j)
        up_share(j, 3)
    for h in (0, 1):
        late(h, 0)
    up_shared(3)
    for h in (0, 1):
        late(h, 1)

    def part_at(b, slot, q=0, n=2):
        row = (b * 3 + slot) * rows + q * (rows // 2)
        return part.at[row:row + n * (rows // 2), :]

    def project(group):
        pieces = []
        for b in group:
            ref = dn_block(b, True)
            copy(ref, ref, dn_pair_send, dn_pair.at[b], partner).wait_recv()
            block = near(z, ORDER[b][0]) * SIDE + near(y, ORDER[b][1])
            pieces.append(dnw[pl.ds(pl.multiple_of(block * 4 * half, 4 * half), 4 * half), :])
        weights = jnp.concatenate(pieces, axis=1) if len(pieces) > 1 else pieces[0]
        both = dot(hid[:, :2 * half], weights[:2 * half]) + dot(hid[:, 2 * half:], weights[2 * half:])
        g = GROUPS.index(group)
        terms = [both[:, i * rows:(i + 1) * rows] for i in range(len(group))]
        for side, by in ((0, 1), (1, -1)):
            row = 3 * rows + side * (rows // 2)
            out, there = first_at(first_out, side, g), first_at(first, side, g)
            out[...] = code(jnp.concatenate([t[row:row + rows // 2] for t in terms], axis=0))
            copy(out, there, rs_send, first_recv.at[side, g], device(dx=by)).start()
        for b, t in zip(group, terms):
            part[b * 3 * rows:(b + 1) * 3 * rows, :] = t[:3 * rows]

    def first_at(ref, side, g):
        return ref.at[side, g, 0:coded_rows(len(GROUPS[g]) * rows // 2), :]

    def last_at(ref, side, g):
        return ref.at[side, g, 0:coded_rows(len(GROUPS[g]) * rows), :]

    def pass_on(g):
        for side, by in ((0, 1), (1, -1)):
            here = first_at(first, side, g)
            copy(here, here, rs_send, first_recv.at[side, g], device(dx=by)).wait_recv()
            slot = 2 - side
            got = decode(here[...])
            ordered = []
            for i, b in enumerate(GROUPS[g]):
                summed = part_at(b, slot, side, 1)[...] + got[i * (rows // 2):(i + 1) * (rows // 2)]
                other = part_at(b, slot, 1 - side, 1)[...]
                ordered += [summed, other] if side == 0 else [other, summed]
            out, there = last_at(last_out, side, g), last_at(last, side, g)
            out[...] = code(jnp.concatenate(ordered, axis=0))
            copy(out, there, rs_send, last_recv.at[side, g], device(dx=by)).start()

    def stored(b):
        block = near(z, ORDER[b][0]) * SIDE + near(y, ORDER[b][1])
        return pltpu.make_async_copy(
            out_ref.at[b], out_hbm.at[:, pl.ds(pl.multiple_of(block * rows, rows), rows)], store.at[b]
        )

    def finish(g):
        for side, by in ((0, 1), (1, -1)):
            here = last_at(last, side, g)
            copy(here, here, rs_send, last_recv.at[side, g], device(dx=by)).wait_recv()
        got = decode(last_at(last, 0, g)[...]) + decode(last_at(last, 1, g)[...])
        for i, b in enumerate(GROUPS[g]):
            out_ref[b] = (part_at(b, 0)[...] + got[i * rows:(i + 1) * rows]).astype(BF)
            stored(b).start()

    project(GROUPS[0])
    dn.first_axis()
    dn_share(0, 1, 2)
    dn_share(1, 3, 4)
    dn.relay(0, 0)
    dn_share(1, 1, 2)
    dn_share(0, 3, 4)
    project(GROUPS[1])
    pass_on(0)
    project(GROUPS[2])
    dn.far_first()
    dn_share(0, 10)
    dn_share(1, 9)
    dn.relay(1, 2)
    for h in (0, 1):
        dn_share(h, 5, 6)
    pass_on(1)
    finish(0)
    project(GROUPS[3])
    pass_on(2)
    dn.relay(2, 1)
    for h in (0, 1):
        dn_share(h, 7, 8)
    dn.far_second(0)
    dn_share(0, 9)
    dn_share(1, 10)
    project(GROUPS[4])
    project(GROUPS[5])
    pass_on(3)
    dn.relay(3, 3)
    dn_share(0, 11, 13)
    dn_share(1, 12, 14)
    finish(1)
    pass_on(4)
    finish(2)
    dn.far_second(1)
    dn_share(1, 11)
    dn_share(0, 12)
    dn.far_second(2)
    dn_share(1, 13)
    dn_share(0, 14)
    pass_on(5)
    dn.far_second(3)
    for h in (0, 1):
        dn_share(h, 15)
    project(GROUPS[6])
    project(GROUPS[7])
    project(GROUPS[8])
    finish(3)
    pass_on(6)
    finish(4)
    pass_on(7)
    pass_on(8)
    for g in (5, 6, 7, 8):
        finish(g)

    def drained(ref, sem):
        pltpu.make_async_copy(ref, ref, sem).wait()

    drained(upw.at[pl.ds(0, 15 * 4 * depth // 2), :], up_send)
    drained(dnw.at[pl.ds(0, 15 * 4 * half // 2), :], dn_send)
    drained(upw.at[pl.ds(0, 2 * blocks * depth), :], up_pair_send)
    drained(dnw.at[pl.ds(0, blocks * 2 * half), :], dn_pair_send)
    drained(tok.at[pl.ds(0, 3 * rows), :], tok_send)
    sent = sum(coded_rows(len(g) * rows // 2) + coded_rows(len(g) * rows) for g in GROUPS)
    drained(part.at[0:2 * sent, :], rs_send)
    for b in range(blocks):
        stored(b).wait()


def shards(tokens, norm_gain, up_weight, down_weight):
    rows, width = tokens.shape
    depth, inner = up_weight.shape
    blocks = SIDE * SIDE
    vmem = pl.BlockSpec(memory_space=pltpu.VMEM)
    anywhere = pl.BlockSpec(memory_space=pl.ANY)
    dma = pltpu.SemaphoreType.DMA
    return pl.pallas_call(
        kernel,
        out_shape=jax.ShapeDtypeStruct((rows, width), BF),
        in_specs=[anywhere, vmem, anywhere, anywhere],
        out_specs=anywhere,
        scratch_shapes=[
            pltpu.VMEM(tokens.shape, BF),
            pltpu.VMEM(up_weight.shape, F32),
            pltpu.VMEM(down_weight.shape, F32),
            pltpu.VMEM((blocks, rows, rows), BF),
            pltpu.VMEM((SIDE * rows, width), BF),
            pltpu.VMEM((4 * blocks * depth, inner // 2), BF),
            pltpu.VMEM((blocks * 2 * inner, rows), BF),
            pltpu.VMEM((SIDE * rows, 2 * inner), F32),
            pltpu.VMEM((SIDE * rows, 2 * inner), BF),
            pltpu.VMEM((blocks * 3 * rows, rows), F32),
            pltpu.VMEM((2, len(GROUPS), coded_rows(rows), rows), F32),
            pltpu.VMEM((2, len(GROUPS), coded_rows(2 * rows), rows), F32),
            pltpu.VMEM((2, len(GROUPS), coded_rows(rows), rows), F32),
            pltpu.VMEM((2, len(GROUPS), coded_rows(2 * rows), rows), F32),
            dma((2, 5, 4)), dma((2, 5, 4)), dma((2, 4)), dma((blocks,)), dma((6,)), dma((2, len(GROUPS))), dma((2, len(GROUPS))),
            dma, dma, dma, dma, dma, dma, dma((3,)), dma((blocks,)),
        ],
        compiler_params=pltpu.CompilerParams(
            collective_id=0, has_side_effects=True, vmem_limit_bytes=56_000_000
        ),
    )(tokens, norm_gain.reshape(1, width), up_weight, down_weight)


def solution(mesh):
    placed = (P(("fs", "tp"), None), P(), P("fs", "tp"), P("tp", "fs"))
    return jax.shard_map(
        shards, mesh=mesh, in_specs=placed, out_specs=P(("fs", "tp"), None), check_vma=False
    )
```

```python
import jax
import jax.numpy as jnp
from jax import lax
from jax.experimental import pallas as pl
from jax.experimental.pallas import tpu as pltpu
from jax.sharding import PartitionSpec as P

epsilon = 1e-06
MESH = pl.DeviceIdType.MESH
SIDE = 4
OFFSETS = (0, -1, 1, 2)
BF = jnp.bfloat16
F32 = jnp.float32

ORDER = (
    (0, 0),
    (0, -1), (0, 1), (-1, 0), (1, 0),
    (-1, -1), (1, 1), (-1, 1), (1, -1),
    (2, 0), (0, 2),
    (-1, 2), (2, -1), (1, 2), (2, 1),
    (2, 2),
)


GROUPS = ((0,), (1, 2), (3, 4), (5, 6), (7, 8), (9, 10), (11, 12), (13, 14), (15,))


def coded_rows(rows):
    n = rows // 8
    return 8 * (2 * (n // 3) + n % 3)


def code(values):
    groups = values.reshape(-1, 8, values.shape[1])
    top = jnp.maximum(jnp.max(jnp.abs(groups), axis=0), 1e-20)
    exponent = jnp.ceil(jnp.log2(top * (1.0 / 32767.0)) + 0.001)
    inverse = jnp.exp2(-exponent)
    n = groups.shape[0] // 3
    a, b, c = (jnp.round(groups[i * n:(i + 1) * n] * inverse) for i in range(3))
    last = jnp.round(groups[-1] * inverse) * 256.0 + (exponent + 128.0)
    high = jnp.floor(c * (1.0 / 256.0))
    low = c - high * 256.0
    parts = [a * 256.0 + low, b * 256.0 + (high + 128.0), groups[3 * n:-1], last[None]]
    return jnp.concatenate([p for p in parts if p.shape[0]], axis=0).reshape(-1, values.shape[1])


def decode(coded):
    groups = coded.reshape(-1, 8, coded.shape[1])
    n = groups.shape[0] // 2 if groups.shape[0] % 2 else groups.shape[0] // 2 - 1
    first, second, rest = groups[:n], groups[n:2 * n], groups[2 * n:-1]
    level = jnp.floor(groups[-1] * (1.0 / 256.0))
    unit = jnp.exp2(groups[-1] - level * 256.0 - 128.0)
    a = jnp.floor(first * (1.0 / 256.0))
    b = jnp.floor(second * (1.0 / 256.0))
    c = (second - b * 256.0 - 128.0) * 256.0 + (first - a * 256.0)
    parts = [a * unit, b * unit, c * unit, rest, (level * unit)[None]]
    return jnp.concatenate([p for p in parts if p.shape[0]], axis=0).reshape(-1, coded.shape[1])


def kernel(
    tokens_hbm, gain_ref, up_hbm, down_hbm, out_ref,
    tokens_ref, up_ref, down_ref, tok, upw, dnw, pre, hid, part, first, last, first_out, last_out,
    up_recv, dn_recv, up_pair, dn_pair, tok_recv, first_recv, last_recv,
    up_send, dn_send, up_pair_send, dn_pair_send, tok_send, rs_send, load,
):
    rows, width = tokens_ref.shape
    half = up_ref.shape[1] // 2
    depth = up_ref.shape[0]
    blocks = SIDE * SIDE
    fs = lax.axis_index("fs")
    tp = lax.axis_index("tp")
    z, y, x, core = fs // SIDE, fs % SIDE, tp // 2, tp % 2

    def near(at, by):
        return (at + (by + SIDE)) % SIDE

    def device(dz=0, dy=0, dx=0):
        return {"fs": near(z, dz) * SIDE + near(y, dy), "tp": near(x, dx) * 2 + core}

    partner = {"fs": fs, "tp": x * 2 + (1 - core)}

    def copy(src, dst, send_sem, recv_sem, to):
        return pltpu.make_async_remote_copy(
            src_ref=src, dst_ref=dst, send_sem=send_sem, recv_sem=recv_sem,
            device_id=to, device_id_type=MESH,
        )

    barrier = pltpu.get_barrier_semaphore()
    peers = [device(dz=1), device(dz=-1), device(dy=1), device(dy=-1), device(dx=1), device(dx=-1), partner]
    for peer in peers:
        pl.semaphore_signal(barrier, inc=1, device_id=peer, device_id_type=MESH)

    loads = [
        pltpu.make_async_copy(src, dst, load.at[i])
        for i, (src, dst) in enumerate(((up_hbm, up_ref), (tokens_hbm, tokens_ref), (down_hbm, down_ref)))
    ]
    for one in loads:
        one.start()

    def up_at(h, dz, dy, q, n):
        zs, ys = near(z, dz), near(y, dy)
        block = zs * SIDE + ys if h == 0 else ys * SIDE + zs
        row = h * blocks * depth + block * depth + q * (depth // 2)
        return upw.at[pl.ds(pl.multiple_of(row, depth // 2), n * (depth // 2)), :]

    def dn_at(h, dz, dy, q, n):
        block = near(z, dz) * SIDE + near(y, dy)
        row = block * 4 * half + h * half + q * (half // 2)
        return dnw.at[pl.ds(pl.multiple_of(row, half // 2), n * (half // 2)), :]

    class Gather:
        def __init__(self, at, span, recv, send):
            self.at, self.span, self.recv, self.send = at, span, recv, send

        def piece(self, h, df, ds, q=0, n=2):
            return self.at(h, ds, df, q, n) if h == 0 else self.at(h, df, ds, q, n)

        def post(self, h, axis, sem, by, df, ds, q=0, n=2):
            ref = self.piece(h, df, ds, q, n)
            to = device(dy=by) if (h == 0) == (axis == 0) else device(dz=by)
            copy(ref, ref, self.send, self.recv.at[sem], to).start()

        def wait(self, sem, quarters):
            ref = self.span(quarters)
            copy(ref, ref, self.send, self.recv.at[sem], partner).wait_recv()

        def start_first(self):
            for h in (0, 1):
                for by in (1, -1):
                    self.post(h, 0, 0, by, 0, 0)

        def start_second(self):
            for h in (0, 1):
                for by in (1, -1):
                    self.post(h, 1, 2, by, 0, 0)

        def first_axis(self):
            self.wait(0, 8)
            for h in (0, 1):
                for q, by in ((0, 1), (1, -1)):
                    self.post(h, 0, 1, by, -by, 0, q, 1)
            for turn in (0, 1):
                for h in (0, 1):
                    for by in (1, -1):
                        self.post(h, 1, 3 + turn, by, -by if turn == 0 else by, 0)

        def far_first(self):
            self.wait(1, 4)
            for h in (0, 1):
                for by in (1, -1):
                    self.post(h, 1, 5, by, 2, 0)

        def relay(self, minus, plus):
            self.wait(2 + minus, 8)
            for h in (0, 1):
                for q, by, j in ((0, 1, minus), (1, -1, plus)):
                    self.post(h, 1, 6 + j, by, OFFSETS[j], -by, q, 1)

        def far_second(self, j):
            self.wait(6 + j, 4)

    up = Gather(up_at, lambda n: upw.at[0:n * (depth // 2), :], up_recv, up_send)
    dn = Gather(dn_at, lambda n: dnw.at[0:n * (half // 2), :], dn_recv, dn_send)

    loads[0].wait()
    for h in (0, 1):
        block = fs if h == 0 else y * SIDE + z
        row = pl.multiple_of(h * blocks * depth + block * depth, depth)
        upw[pl.ds(row, depth), :] = up_ref[:, h * half:(h + 1) * half].astype(BF)
    pl.semaphore_wait(barrier, len(peers))
    up.start_first()

    loads[1].wait()
    values = tokens_ref[...].astype(F32)
    scale = lax.rsqrt(jnp.mean(values * values, axis=-1, keepdims=True) + epsilon)
    tok[0:rows, :] = (values * scale * gain_ref[...]).astype(BF)

    def tok_at(slot, q):
        row = slot * rows + q * (rows // 2)
        return tok.at[row:row + rows // 2, :]

    def tok_post(sem, slot, there, q, by):
        copy(tok_at(slot, q), tok_at(there, q), tok_send, tok_recv.at[sem], device(dx=by)).start()

    def tok_wait(sem, halves):
        ref = tok.at[0:halves * (rows // 2), :]
        copy(ref, ref, tok_send, tok_recv.at[sem], partner).wait_recv()

    tok_post(0, 0, 1, 0, 1)
    tok_post(0, 0, 2, 1, -1)
    tok_post(1, 0, 1, 1, 1)
    tok_post(1, 0, 2, 0, -1)
    up.start_second()
    loads[2].wait()

    own = pl.multiple_of(fs * 4 * half, 4 * half)
    dnw[pl.ds(own, 2 * half), :] = down_ref[...].astype(BF)

    def dn_block(b, to_partner):
        block = near(z, ORDER[b][0]) * SIDE + near(y, ORDER[b][1])
        row = block * 4 * half + (2 * half if to_partner else 0)
        return dnw.at[pl.ds(pl.multiple_of(row, 2 * half), 2 * half), :]

    def dn_share(h, *bs):
        for b in bs:
            block = near(z, ORDER[b][0]) * SIDE + near(y, ORDER[b][1])
            mine, theirs = (
                dnw.at[pl.ds(pl.multiple_of(block * 4 * half + (2 * side + h) * half, half), half), :] for side in (0, 1)
            )
            copy(mine, theirs, dn_pair_send, dn_pair.at[(b + 1) // 2], partner).start()

    def up_plane(h, p, to_partner):
        plane = near(z if h == 0 else y, OFFSETS[p])
        row = (h + (2 if to_partner else 0)) * blocks * depth + plane * SIDE * depth
        return upw.at[pl.ds(pl.multiple_of(row, SIDE * depth), SIDE * depth), :]

    def up_share(j, p):
        for h in (0, 1):
            plane = near(z if h == 0 else y, OFFSETS[p])
            row = (plane * SIDE + near(y if h == 0 else z, OFFSETS[j])) * depth
            mine, theirs = (
                upw.at[pl.ds(pl.multiple_of((h + 2 * side) * blocks * depth + row, depth), depth), :] for side in (0, 1)
            )
            copy(mine, theirs, up_pair_send, up_pair.at[p], partner).start()

    def up_shared(p):
        ref = upw.at[0:2 * SIDE * depth, :]
        copy(ref, ref, up_pair_send, up_pair.at[p], partner).wait_recv()

    up_share(0, 0)
    for h in (0, 1):
        dn_share(h, 0)

    up.first_axis()
    up_share(1, 0)
    up_share(2, 0)
    up.relay(0, 0)
    up_share(0, 1)
    up_share(0, 2)
    up.far_first()
    up_share(3, 0)
    tok_wait(0, 2)
    tok_post(1, 1, 3, 0, 1)
    tok_post(1, 2, 3, 1, -1)
    for minus, plus in ((1, 2), (2, 1), (3, 3)):
        up.relay(minus, plus)
        up_share(minus, 1)
        up_share(plus, 2)
    dn.start_first()
    dn.start_second()
    tok_wait(1, 4)

    def columns_of(h, p):
        plane = near(z if h == 0 else y, OFFSETS[p])
        if h == 0:
            return tok[:, pl.ds(pl.multiple_of(plane * SIDE * depth, SIDE * depth), SIDE * depth)]
        return jnp.concatenate(
            [tok[:, pl.ds(pl.multiple_of((a * SIDE + plane) * depth, depth), depth)] for a in range(SIDE)], axis=1
        )

    def dot(a, b):
        return jnp.dot(a, b, preferred_element_type=F32)

    tile = 256

    def early(h, other):
        for n in range(half // tile):
            cols = slice(n * tile, (n + 1) * tile)
            total = sum(dot(columns_of(h, p), up_plane(h, p, other)[:, cols]) for p in (0, 1, 2))
            at = (2 * other + h) * half + n * tile
            pre[:, at:at + tile] = total

    def late(h, other):
        for n in range(half // tile):
            cols = slice(n * tile, (n + 1) * tile)
            at = (2 * other + h) * half + n * tile
            total = pre[:, at:at + tile] + dot(columns_of(h, 3), up_plane(h, 3, other)[:, cols])
            hid[:, at:at + tile] = jnp.square(jnp.maximum(total, 0.0)).astype(BF)

    for h in (0, 1):
        early(h, 0)
    for p in (0, 1, 2):
        up_shared(p)
    for j in (0, 1):
        up.far_second(j)
        up_share(j, 3)
    for h in (0, 1):
        early(h, 1)
    for j in (2, 3):
        up.far_second(j)
        up_share(j, 3)
    for h in (0, 1):
        late(h, 0)
    up_shared(3)
    for h in (0, 1):
        late(h, 1)

    def part_at(b, slot, q=0, n=2):
        row = (b * 3 + slot) * rows + q * (rows // 2)
        return part.at[row:row + n * (rows // 2), :]

    def project(group):
        pieces = []
        g = GROUPS.index(group)
        ref = dnw.at[0:len(group) * 2 * half, :]
        copy(ref, ref, dn_pair_send, dn_pair.at[g], partner).wait_recv()
        for b in group:
            block = near(z, ORDER[b][0]) * SIDE + near(y, ORDER[b][1])
            pieces.append(dnw[pl.ds(pl.multiple_of(block * 4 * half, 4 * half), 4 * half), :])
        weights = jnp.concatenate(pieces, axis=1) if len(pieces) > 1 else pieces[0]
        both = jnp.concatenate([dot(hid[at:at + 2 * rows, :], weights) for at in (0, 2 * rows)], axis=0)
        terms = [both[:, i * rows:(i + 1) * rows] for i in range(len(group))]
        for side, by in ((0, 1), (1, -1)):
            row = 3 * rows + side * (rows // 2)
            out, there = first_at(first_out, side, g), first_at(first, side, g)
            out[...] = code(jnp.concatenate([t[row:row + rows // 2] for t in terms], axis=0))
            copy(out, there, rs_send, first_recv.at[g], device(dx=by)).start()
        for b, t in zip(group, terms):
            part[b * 3 * rows:(b + 1) * 3 * rows, :] = t[:3 * rows]

    def first_at(ref, side, g):
        return ref.at[side, g, 0:coded_rows(len(GROUPS[g]) * rows // 2), :]

    def last_at(ref, side, g):
        return ref.at[side, g, 0:coded_rows(len(GROUPS[g]) * rows), :]

    def pass_on(g):
        came = part.at[0:2 * coded_rows(len(GROUPS[g]) * rows // 2), :]
        copy(came, came, rs_send, first_recv.at[g], partner).wait_recv()
        for side, by in ((0, 1), (1, -1)):
            slot = 2 - side
            got = decode(first_at(first, side, g)[...])
            ordered = []
            for i, b in enumerate(GROUPS[g]):
                summed = part_at(b, slot, side, 1)[...] + got[i * (rows // 2):(i + 1) * (rows // 2)]
                other = part_at(b, slot, 1 - side, 1)[...]
                ordered += [summed, other] if side == 0 else [other, summed]
            out, there = last_at(last_out, side, g), last_at(last, side, g)
            out[...] = code(jnp.concatenate(ordered, axis=0))
            copy(out, there, rs_send, last_recv.at[g], device(dx=by)).start()

    def finish(g):
        came = part.at[0:2 * coded_rows(len(GROUPS[g]) * rows), :]
        copy(came, came, rs_send, last_recv.at[g], partner).wait_recv()
        got = decode(last_at(last, 0, g)[...]) + decode(last_at(last, 1, g)[...])
        for i, b in enumerate(GROUPS[g]):
            block = near(z, ORDER[b][0]) * SIDE + near(y, ORDER[b][1])
            total = part_at(b, 0)[...] + got[i * rows:(i + 1) * rows]
            out_ref[:, pl.ds(pl.multiple_of(block * rows, rows), rows)] = total.astype(BF)

    dn.first_axis()
    dn_share(0, 1, 2)
    dn_share(1, 3, 4)
    project(GROUPS[0])
    dn.relay(0, 0)
    dn_share(1, 1, 2)
    dn_share(0, 3, 4)
    project(GROUPS[1])
    pass_on(0)
    project(GROUPS[2])
    dn.far_first()
    dn_share(0, 10)
    dn_share(1, 9)
    dn.relay(1, 2)
    for h in (0, 1):
        dn_share(h, 5, 6)
    pass_on(1)
    finish(0)
    project(GROUPS[3])
    pass_on(2)
    dn.relay(2, 1)
    for h in (0, 1):
        dn_share(h, 7, 8)
    dn.far_second(0)
    dn_share(0, 9)
    dn_share(1, 10)
    project(GROUPS[4])
    project(GROUPS[5])
    pass_on(3)
    dn.relay(3, 3)
    dn_share(0, 11, 13)
    dn_share(1, 12, 14)
    finish(1)
    pass_on(4)
    finish(2)
    dn.far_second(1)
    dn_share(1, 11)
    dn_share(0, 12)
    dn.far_second(2)
    dn_share(1, 13)
    dn_share(0, 14)
    project(GROUPS[6])
    dn.far_second(3)
    for h in (0, 1):
        dn_share(h, 15)
    project(GROUPS[7])
    pass_on(5)
    project(GROUPS[8])
    finish(3)
    pass_on(6)
    finish(4)
    pass_on(7)
    pass_on(8)
    for g in (5, 6, 7, 8):
        finish(g)

    def drained(ref, sem):
        pltpu.make_async_copy(ref, ref, sem).wait()

    drained(upw.at[pl.ds(0, 15 * 4 * depth // 2), :], up_send)
    drained(dnw.at[pl.ds(0, 15 * 4 * half // 2), :], dn_send)
    drained(upw.at[pl.ds(0, 2 * blocks * depth), :], up_pair_send)
    drained(dnw.at[pl.ds(0, blocks * 2 * half), :], dn_pair_send)
    drained(tok.at[pl.ds(0, 3 * rows), :], tok_send)
    sent = sum(coded_rows(len(g) * rows // 2) + coded_rows(len(g) * rows) for g in GROUPS)
    drained(part.at[0:2 * sent, :], rs_send)


def shards(tokens, norm_gain, up_weight, down_weight):
    rows, width = tokens.shape
    depth, inner = up_weight.shape
    blocks = SIDE * SIDE
    vmem = pl.BlockSpec(memory_space=pltpu.VMEM)
    anywhere = pl.BlockSpec(memory_space=pl.ANY)
    dma = pltpu.SemaphoreType.DMA
    return pl.pallas_call(
        kernel,
        out_shape=jax.ShapeDtypeStruct((rows, width), BF),
        in_specs=[anywhere, vmem, anywhere, anywhere],
        out_specs=vmem,
        scratch_shapes=[
            pltpu.VMEM(tokens.shape, BF),
            pltpu.VMEM(up_weight.shape, F32),
            pltpu.VMEM(down_weight.shape, F32),
            pltpu.VMEM((SIDE * rows, width), BF),
            pltpu.VMEM((4 * blocks * depth, inner // 2), BF),
            pltpu.VMEM((blocks * 2 * inner, rows), BF),
            pltpu.VMEM((SIDE * rows, 2 * inner), F32),
            pltpu.VMEM((SIDE * rows, 2 * inner), BF),
            pltpu.VMEM((blocks * 3 * rows, rows), F32),
            pltpu.VMEM((2, len(GROUPS), coded_rows(rows), rows), F32),
            pltpu.VMEM((2, len(GROUPS), coded_rows(2 * rows), rows), F32),
            pltpu.VMEM((2, len(GROUPS), coded_rows(rows), rows), F32),
            pltpu.VMEM((2, len(GROUPS), coded_rows(2 * rows), rows), F32),
            dma((10,)), dma((10,)), dma((4,)), dma((len(GROUPS),)), dma((2,)), dma((len(GROUPS),)), dma((len(GROUPS),)),
            dma, dma, dma, dma, dma, dma, dma((3,)),
        ],
        compiler_params=pltpu.CompilerParams(
            collective_id=0, has_side_effects=True, vmem_limit_bytes=56_000_000
        ),
    )(tokens, norm_gain.reshape(1, width), up_weight, down_weight)


def solution(mesh):
    placed = (P(("fs", "tp"), None), P(), P("fs", "tp"), P("tp", "fs"))
    return jax.shard_map(
        shards, mesh=mesh, in_specs=placed, out_specs=P(("fs", "tp"), None), check_vma=False
    )
```

```python
import jax
import jax.numpy as jnp
from jax import lax
from jax.experimental import pallas as pl
from jax.experimental.pallas import tpu as pltpu
from jax.sharding import PartitionSpec as P

epsilon = 1e-06
MESH = pl.DeviceIdType.MESH
SIDE = 4
OFFSETS = (0, -1, 1, 2)
BF = jnp.bfloat16
F32 = jnp.float32

ORDER = (
    (0, 0),
    (0, -1), (0, 1), (-1, 0), (1, 0),
    (-1, -1), (1, 1), (-1, 1), (1, -1),
    (2, 0), (0, 2),
    (-1, 2), (2, -1), (1, 2), (2, 1),
    (2, 2),
)


GROUPS = ((0,), (1, 2), (3, 4), (5, 6), (7, 8), (9, 10), (11, 12), (13, 14), (15,))


LEVELS = 248 * 128 - 1
LOWEST = 123.0


def coded_rows(rows):
    return rows + 16


def code(values):
    groups = values.reshape(-1, 8, values.shape[1])
    top = jnp.maximum(jnp.max(jnp.abs(groups), axis=0), 1e-20)
    exponent = jnp.ceil(jnp.log2(top * (1.0 / LEVELS)) + 0.001)
    scaled = groups * jnp.exp2(-exponent)
    level = jnp.round(jnp.abs(scaled))
    e = jnp.floor(level * (1.0 / 128.0))
    word = jnp.exp2(e - LOWEST) * (level * (1.0 / 128.0) + (1.0 - e))
    word = jnp.where(scaled < 0.0, -word, word)
    both = jnp.concatenate([word, exponent[None], exponent[None]], axis=0)
    return both.reshape(-1, values.shape[1]).astype(BF)


def decode(coded):
    groups = coded.astype(F32).reshape(-1, 8, coded.shape[1])
    words, unit = groups[:-2], jnp.exp2(groups[-1])
    size = jnp.abs(words)
    e = jnp.floor(jnp.log2(size) + 0.001)
    level = (e + size * jnp.exp2(-e)) * 128.0 + (LOWEST - 1.0) * 128.0
    return (jnp.where(words < 0.0, -level, level) * unit).reshape(-1, coded.shape[1])


def kernel(
    tokens_hbm, gain_ref, up_hbm, down_hbm, out_ref,
    tokens_ref, up_ref, down_ref, tok, upw, dnw, pre, hid, part, first, last, first_out, last_out,
    up_recv, dn_recv, up_pair, dn_pair, tok_recv, first_recv, last_recv,
    up_send, dn_send, up_pair_send, dn_pair_send, tok_send, rs_send, load,
):
    rows, width = tokens_ref.shape
    half = up_ref.shape[1] // 2
    depth = up_ref.shape[0]
    blocks = SIDE * SIDE
    fs = lax.axis_index("fs")
    tp = lax.axis_index("tp")
    z, y, x, core = fs // SIDE, fs % SIDE, tp // 2, tp % 2

    def near(at, by):
        return (at + (by + SIDE)) % SIDE

    def device(dz=0, dy=0, dx=0):
        return {"fs": near(z, dz) * SIDE + near(y, dy), "tp": near(x, dx) * 2 + core}

    partner = {"fs": fs, "tp": x * 2 + (1 - core)}

    def copy(src, dst, send_sem, recv_sem, to):
        return pltpu.make_async_remote_copy(
            src_ref=src, dst_ref=dst, send_sem=send_sem, recv_sem=recv_sem,
            device_id=to, device_id_type=MESH,
        )

    barrier = pltpu.get_barrier_semaphore()
    peers = [device(dz=1), device(dz=-1), device(dy=1), device(dy=-1), device(dx=1), device(dx=-1), partner]
    for peer in peers:
        pl.semaphore_signal(barrier, inc=1, device_id=peer, device_id_type=MESH)

    loads = [
        pltpu.make_async_copy(src, dst, load.at[i])
        for i, (src, dst) in enumerate(((up_hbm, up_ref), (tokens_hbm, tokens_ref), (down_hbm, down_ref)))
    ]
    for one in loads:
        one.start()

    def up_at(h, dz, dy, q, n):
        zs, ys = near(z, dz), near(y, dy)
        block = zs * SIDE + ys if h == 0 else ys * SIDE + zs
        row = h * blocks * depth + block * depth + q * (depth // 2)
        return upw.at[pl.ds(pl.multiple_of(row, depth // 2), n * (depth // 2)), :]

    def dn_at(h, dz, dy, q, n):
        block = near(z, dz) * SIDE + near(y, dy)
        row = block * 4 * half + h * half + q * (half // 2)
        return dnw.at[pl.ds(pl.multiple_of(row, half // 2), n * (half // 2)), :]

    class Gather:
        def __init__(self, at, span, recv, send):
            self.at, self.span, self.recv, self.send = at, span, recv, send

        def piece(self, h, df, ds, q=0, n=2):
            return self.at(h, ds, df, q, n) if h == 0 else self.at(h, df, ds, q, n)

        def post(self, h, axis, sem, by, df, ds, q=0, n=2):
            ref = self.piece(h, df, ds, q, n)
            to = device(dy=by) if (h == 0) == (axis == 0) else device(dz=by)
            copy(ref, ref, self.send, self.recv.at[sem], to).start()

        def wait(self, sem, quarters):
            ref = self.span(quarters)
            copy(ref, ref, self.send, self.recv.at[sem], partner).wait_recv()

        def start_first(self):
            for h in (0, 1):
                for by in (1, -1):
                    self.post(h, 0, 0, by, 0, 0)

        def start_second(self):
            for h in (0, 1):
                for by in (1, -1):
                    self.post(h, 1, 2, by, 0, 0)

        def first_axis(self):
            self.wait(0, 8)
            for h in (0, 1):
                for q, by in ((0, 1), (1, -1)):
                    self.post(h, 0, 1, by, -by, 0, q, 1)
            for turn in (0, 1):
                for h in (0, 1):
                    for by in (1, -1):
                        self.post(h, 1, 3 + turn, by, -by if turn == 0 else by, 0)

        def far_first(self):
            self.wait(1, 4)
            for h in (0, 1):
                for by in (1, -1):
                    self.post(h, 1, 5, by, 2, 0)

        def relay(self, minus, plus):
            self.wait(2 + minus, 8)
            for h in (0, 1):
                for q, by, j in ((0, 1, minus), (1, -1, plus)):
                    self.post(h, 1, 6 + j, by, OFFSETS[j], -by, q, 1)

        def far_second(self, j):
            self.wait(6 + j, 4)

    up = Gather(up_at, lambda n: upw.at[0:n * (depth // 2), :], up_recv, up_send)
    dn = Gather(dn_at, lambda n: dnw.at[0:n * (half // 2), :], dn_recv, dn_send)

    loads[0].wait()
    for h in (0, 1):
        block = fs if h == 0 else y * SIDE + z
        row = pl.multiple_of(h * blocks * depth + block * depth, depth)
        upw[pl.ds(row, depth), :] = up_ref[:, h * half:(h + 1) * half].astype(BF)
    pl.semaphore_wait(barrier, len(peers))
    up.start_first()

    loads[1].wait()
    values = tokens_ref[...].astype(F32)
    scale = lax.rsqrt(jnp.mean(values * values, axis=-1, keepdims=True) + epsilon)
    tok[0:rows, :] = (values * scale * gain_ref[...]).astype(BF)

    def tok_at(slot, q):
        row = slot * rows + q * (rows // 2)
        return tok.at[row:row + rows // 2, :]

    def tok_post(sem, slot, there, q, by):
        copy(tok_at(slot, q), tok_at(there, q), tok_send, tok_recv.at[sem], device(dx=by)).start()

    def tok_wait(sem, halves):
        ref = tok.at[0:halves * (rows // 2), :]
        copy(ref, ref, tok_send, tok_recv.at[sem], partner).wait_recv()

    tok_post(0, 0, 1, 0, 1)
    tok_post(0, 0, 2, 1, -1)
    tok_post(1, 0, 1, 1, 1)
    tok_post(1, 0, 2, 0, -1)
    up.start_second()
    loads[2].wait()

    own = pl.multiple_of(fs * 4 * half, 4 * half)
    dnw[pl.ds(own, 2 * half), :] = down_ref[...].astype(BF)

    def dn_block(b, to_partner):
        block = near(z, ORDER[b][0]) * SIDE + near(y, ORDER[b][1])
        row = block * 4 * half + (2 * half if to_partner else 0)
        return dnw.at[pl.ds(pl.multiple_of(row, 2 * half), 2 * half), :]

    def dn_share(h, *bs):
        for b in bs:
            block = near(z, ORDER[b][0]) * SIDE + near(y, ORDER[b][1])
            mine, theirs = (
                dnw.at[pl.ds(pl.multiple_of(block * 4 * half + (2 * side + h) * half, half), half), :] for side in (0, 1)
            )
            copy(mine, theirs, dn_pair_send, dn_pair.at[(b + 1) // 2], partner).start()

    def up_plane(h, p, to_partner):
        plane = near(z if h == 0 else y, OFFSETS[p])
        row = (h + (2 if to_partner else 0)) * blocks * depth + plane * SIDE * depth
        return upw.at[pl.ds(pl.multiple_of(row, SIDE * depth), SIDE * depth), :]

    def up_share(j, p):
        for h in (0, 1):
            plane = near(z if h == 0 else y, OFFSETS[p])
            row = (plane * SIDE + near(y if h == 0 else z, OFFSETS[j])) * depth
            mine, theirs = (
                upw.at[pl.ds(pl.multiple_of((h + 2 * side) * blocks * depth + row, depth), depth), :] for side in (0, 1)
            )
            copy(mine, theirs, up_pair_send, up_pair.at[p], partner).start()

    def up_shared(p):
        ref = upw.at[0:2 * SIDE * depth, :]
        copy(ref, ref, up_pair_send, up_pair.at[p], partner).wait_recv()

    dn.start_first()
    up_share(0, 0)
    for h in (0, 1):
        dn_share(h, 0)

    up.first_axis()
    up_share(1, 0)
    up_share(2, 0)
    up.relay(0, 0)
    up_share(0, 1)
    up_share(0, 2)
    up.far_first()
    up_share(3, 0)
    tok_wait(0, 2)
    tok_post(1, 1, 3, 0, 1)
    tok_post(1, 2, 3, 1, -1)
    for minus, plus in ((1, 2), (2, 1), (3, 3)):
        up.relay(minus, plus)
        up_share(minus, 1)
        up_share(plus, 2)
    dn.start_second()
    dn.first_axis()
    dn_share(0, 1, 2)
    dn_share(1, 3, 4)
    tok_wait(1, 4)

    def columns_of(h, p):
        plane = near(z if h == 0 else y, OFFSETS[p])
        if h == 0:
            return tok[:, pl.ds(pl.multiple_of(plane * SIDE * depth, SIDE * depth), SIDE * depth)]
        return jnp.concatenate(
            [tok[:, pl.ds(pl.multiple_of((a * SIDE + plane) * depth, depth), depth)] for a in range(SIDE)], axis=1
        )

    def dot(a, b):
        return jnp.dot(a, b, preferred_element_type=F32)

    tile = 256

    def early(h, other):
        for n in range(half // tile):
            cols = slice(n * tile, (n + 1) * tile)
            total = sum(dot(columns_of(h, p), up_plane(h, p, other)[:, cols]) for p in (0, 1, 2))
            at = (2 * other + h) * half + n * tile
            pre[:, at:at + tile] = total

    def late(h, other):
        for n in range(half // tile):
            cols = slice(n * tile, (n + 1) * tile)
            at = (2 * other + h) * half + n * tile
            total = pre[:, at:at + tile] + dot(columns_of(h, 3), up_plane(h, 3, other)[:, cols])
            hid[:, at:at + tile] = jnp.square(jnp.maximum(total, 0.0)).astype(BF)

    for h in (0, 1):
        early(h, 0)
    for p in (0, 1, 2):
        up_shared(p)
    for j in (0, 1):
        up.far_second(j)
        up_share(j, 3)
    for h in (0, 1):
        early(h, 1)
    for j in (2, 3):
        up.far_second(j)
        up_share(j, 3)
    for h in (0, 1):
        late(h, 0)
    up_shared(3)
    for h in (0, 1):
        late(h, 1)

    def part_at(b, slot, q=0, n=2):
        row = (b * 3 + slot) * rows + q * (rows // 2)
        return part.at[row:row + n * (rows // 2), :]

    def project(group):
        pieces = []
        g = GROUPS.index(group)
        ref = dnw.at[0:len(group) * 2 * half, :]
        copy(ref, ref, dn_pair_send, dn_pair.at[g], partner).wait_recv()
        for b in group:
            block = near(z, ORDER[b][0]) * SIDE + near(y, ORDER[b][1])
            pieces.append(dnw[pl.ds(pl.multiple_of(block * 4 * half, 4 * half), 4 * half), :])
        weights = jnp.concatenate(pieces, axis=1) if len(pieces) > 1 else pieces[0]
        both = jnp.concatenate([dot(hid[at:at + 2 * rows, :], weights) for at in (0, 2 * rows)], axis=0)
        terms = [both[:, i * rows:(i + 1) * rows] for i in range(len(group))]
        for side, by in ((0, 1), (1, -1)):
            row = 3 * rows + side * (rows // 2)
            out, there = first_at(first_out, side, g), first_at(first, side, g)
            out[...] = code(jnp.concatenate([t[row:row + rows // 2] for t in terms], axis=0))
            copy(out, there, rs_send, first_recv.at[g], device(dx=by)).start()
        for b, t in zip(group, terms):
            part[b * 3 * rows:(b + 1) * 3 * rows, :] = t[:3 * rows]

    def first_at(ref, side, g):
        return ref.at[side, g, 0:coded_rows(len(GROUPS[g]) * rows // 2), :]

    def last_at(ref, side, g):
        return ref.at[side, g, 0:coded_rows(len(GROUPS[g]) * rows), :]

    def pass_on(g):
        came = dnw.at[0:2 * coded_rows(len(GROUPS[g]) * rows // 2), :]
        copy(came, came, rs_send, first_recv.at[g], partner).wait_recv()
        for side, by in ((0, 1), (1, -1)):
            slot = 2 - side
            got = decode(first_at(first, side, g)[...])
            ordered = []
            for i, b in enumerate(GROUPS[g]):
                summed = part_at(b, slot, side, 1)[...] + got[i * (rows // 2):(i + 1) * (rows // 2)]
                other = part_at(b, slot, 1 - side, 1)[...]
                ordered += [summed, other] if side == 0 else [other, summed]
            out, there = last_at(last_out, side, g), last_at(last, side, g)
            out[...] = code(jnp.concatenate(ordered, axis=0))
            copy(out, there, rs_send, last_recv.at[g], device(dx=by)).start()

    def finish(g):
        came = dnw.at[0:2 * coded_rows(len(GROUPS[g]) * rows), :]
        copy(came, came, rs_send, last_recv.at[g], partner).wait_recv()
        got = decode(last_at(last, 0, g)[...]) + decode(last_at(last, 1, g)[...])
        for i, b in enumerate(GROUPS[g]):
            block = near(z, ORDER[b][0]) * SIDE + near(y, ORDER[b][1])
            total = part_at(b, 0)[...] + got[i * rows:(i + 1) * rows]
            out_ref[:, pl.ds(pl.multiple_of(block * rows, rows), rows)] = total.astype(BF)

    project(GROUPS[0])
    dn.relay(0, 0)
    dn_share(1, 1, 2)
    dn_share(0, 3, 4)
    dn.far_first()
    dn_share(0, 10)
    dn_share(1, 9)
    project(GROUPS[1])
    project(GROUPS[2])
    pass_on(0)
    dn.relay(1, 2)
    for h in (0, 1):
        dn_share(h, 5, 6)
    pass_on(1)
    project(GROUPS[3])
    pass_on(2)
    dn.relay(2, 1)
    for h in (0, 1):
        dn_share(h, 7, 8)
    dn.far_second(0)
    dn_share(0, 9)
    dn_share(1, 10)
    finish(0)
    project(GROUPS[4])
    project(GROUPS[5])
    pass_on(3)
    dn.relay(3, 3)
    dn_share(0, 11, 13)
    dn_share(1, 12, 14)
    finish(1)
    dn.far_second(1)
    dn_share(1, 11)
    dn_share(0, 12)
    pass_on(4)
    dn.far_second(2)
    dn_share(1, 13)
    dn_share(0, 14)
    project(GROUPS[6])
    dn.far_second(3)
    for h in (0, 1):
        dn_share(h, 15)
    project(GROUPS[7])
    pass_on(5)
    project(GROUPS[8])
    finish(2)
    finish(3)
    pass_on(6)
    finish(4)
    pass_on(7)
    pass_on(8)
    for g in (5, 6, 7, 8):
        finish(g)

    def drained(ref, sem):
        pltpu.make_async_copy(ref, ref, sem).wait()

    drained(upw.at[pl.ds(0, 15 * 4 * depth // 2), :], up_send)
    drained(dnw.at[pl.ds(0, 15 * 4 * half // 2), :], dn_send)
    drained(upw.at[pl.ds(0, 2 * blocks * depth), :], up_pair_send)
    drained(dnw.at[pl.ds(0, blocks * 2 * half), :], dn_pair_send)
    drained(tok.at[pl.ds(0, 3 * rows), :], tok_send)
    sent = sum(coded_rows(len(g) * rows // 2) + coded_rows(len(g) * rows) for g in GROUPS)
    drained(dnw.at[0:2 * sent, :], rs_send)


def shards(tokens, norm_gain, up_weight, down_weight):
    rows, width = tokens.shape
    depth, inner = up_weight.shape
    blocks = SIDE * SIDE
    vmem = pl.BlockSpec(memory_space=pltpu.VMEM)
    anywhere = pl.BlockSpec(memory_space=pl.ANY)
    dma = pltpu.SemaphoreType.DMA
    return pl.pallas_call(
        kernel,
        out_shape=jax.ShapeDtypeStruct((rows, width), BF),
        in_specs=[anywhere, vmem, anywhere, anywhere],
        out_specs=vmem,
        scratch_shapes=[
            pltpu.VMEM(tokens.shape, BF),
            pltpu.VMEM(up_weight.shape, F32),
            pltpu.VMEM(down_weight.shape, F32),
            pltpu.VMEM((SIDE * rows, width), BF),
            pltpu.VMEM((4 * blocks * depth, inner // 2), BF),
            pltpu.VMEM((blocks * 2 * inner, rows), BF),
            pltpu.VMEM((SIDE * rows, 2 * inner), F32),
            pltpu.VMEM((SIDE * rows, 2 * inner), BF),
            pltpu.VMEM((blocks * 3 * rows, rows), F32),
            pltpu.VMEM((2, len(GROUPS), coded_rows(rows), rows), BF),
            pltpu.VMEM((2, len(GROUPS), coded_rows(2 * rows), rows), BF),
            pltpu.VMEM((2, len(GROUPS), coded_rows(rows), rows), BF),
            pltpu.VMEM((2, len(GROUPS), coded_rows(2 * rows), rows), BF),
            dma((10,)), dma((10,)), dma((4,)), dma((len(GROUPS),)), dma((2,)), dma((len(GROUPS),)), dma((len(GROUPS),)),
            dma, dma, dma, dma, dma, dma, dma((3,)),
        ],
        compiler_params=pltpu.CompilerParams(
            collective_id=0, has_side_effects=True, vmem_limit_bytes=56_000_000
        ),
    )(tokens, norm_gain.reshape(1, width), up_weight, down_weight)


def solution(mesh):
    placed = (P(("fs", "tp"), None), P(), P("fs", "tp"), P("tp", "fs"))
    return jax.shard_map(
        shards, mesh=mesh, in_specs=placed, out_specs=P(("fs", "tp"), None), check_vma=False
    )
```

```python
import jax
import jax.numpy as jnp
from jax import lax
from jax.experimental import pallas as pl
from jax.experimental.pallas import tpu as pltpu
from jax.sharding import PartitionSpec as P

epsilon = 1e-06
MESH = pl.DeviceIdType.MESH
SIDE = 4
OFFSETS = (0, -1, 1, 2)
BF = jnp.bfloat16
F32 = jnp.float32

ORDER = (
    (0, 0),
    (0, -1), (0, 1), (-1, 0), (1, 0),
    (-1, -1), (1, 1), (-1, 1), (1, -1),
    (2, 0), (0, 2),
    (-1, 2), (2, -1), (1, 2), (2, 1),
    (2, 2),
)


GROUPS = ((0,), (1, 2), (3, 4), (5, 6), (7, 8), (9, 10), (11, 12), (13, 14), (15,))


LEVELS = 248 * 128 - 1
LOWEST = 123.0


def coded_rows(rows):
    return rows + 16


def code(values):
    groups = values.reshape(-1, 8, values.shape[1])
    top = jnp.maximum(jnp.max(jnp.abs(groups), axis=0), 1e-20)
    exponent = jnp.ceil(jnp.log2(top * (1.0 / LEVELS)) + 0.001)
    scaled = groups * jnp.exp2(-exponent)
    level = jnp.round(jnp.abs(scaled))
    e = jnp.floor(level * (1.0 / 128.0))
    word = jnp.exp2(e - LOWEST) * (level * (1.0 / 128.0) + (1.0 - e))
    word = jnp.where(scaled < 0.0, -word, word)
    both = jnp.concatenate([word, exponent[None], exponent[None]], axis=0)
    return both.reshape(-1, values.shape[1]).astype(BF)


def decode(coded):
    groups = coded.astype(F32).reshape(-1, 8, coded.shape[1])
    words, unit = groups[:-2], jnp.exp2(groups[-1])
    size = jnp.abs(words)
    e = jnp.floor(jnp.log2(size) + 0.001)
    level = (e + size * jnp.exp2(-e)) * 128.0 + (LOWEST - 1.0) * 128.0
    return (jnp.where(words < 0.0, -level, level) * unit).reshape(-1, coded.shape[1])


def kernel(
    tokens_hbm, gain_ref, up_hbm, down_hbm, out_ref,
    tokens_ref, up_ref, down_ref, tok, upw, dnw, pre, hid, part, first, last, first_out, last_out,
    up_recv, dn_recv, up_pair, dn_pair, tok_recv, first_recv, last_recv,
    up_send, dn_send, up_pair_send, dn_pair_send, tok_send, rs_send, load,
):
    rows, width = tokens_ref.shape
    half = up_ref.shape[1] // 2
    depth = up_ref.shape[0]
    blocks = SIDE * SIDE
    fs = lax.axis_index("fs")
    tp = lax.axis_index("tp")
    z, y, x, core = fs // SIDE, fs % SIDE, tp // 2, tp % 2

    def near(at, by):
        return (at + (by + SIDE)) % SIDE

    def device(dz=0, dy=0, dx=0):
        return {"fs": near(z, dz) * SIDE + near(y, dy), "tp": near(x, dx) * 2 + core}

    partner = {"fs": fs, "tp": x * 2 + (1 - core)}

    def copy(src, dst, send_sem, recv_sem, to):
        return pltpu.make_async_remote_copy(
            src_ref=src, dst_ref=dst, send_sem=send_sem, recv_sem=recv_sem,
            device_id=to, device_id_type=MESH,
        )

    barrier = pltpu.get_barrier_semaphore()
    peers = [device(dz=1), device(dz=-1), device(dy=1), device(dy=-1), device(dx=1), device(dx=-1), partner]
    for peer in peers:
        pl.semaphore_signal(barrier, inc=1, device_id=peer, device_id_type=MESH)

    loads = [
        pltpu.make_async_copy(src, dst, load.at[i])
        for i, (src, dst) in enumerate(((up_hbm, up_ref), (tokens_hbm, tokens_ref), (down_hbm, down_ref)))
    ]
    loads[0].start()

    def up_at(h, dz, dy, q, n):
        zs, ys = near(z, dz), near(y, dy)
        block = zs * SIDE + ys if h == 0 else ys * SIDE + zs
        row = h * blocks * depth + block * depth + q * (depth // 2)
        return upw.at[pl.ds(pl.multiple_of(row, depth // 2), n * (depth // 2)), :]

    def dn_at(h, dz, dy, q, n):
        block = near(z, dz) * SIDE + near(y, dy)
        row = block * 4 * half + h * half + q * (half // 2)
        return dnw.at[pl.ds(pl.multiple_of(row, half // 2), n * (half // 2)), :]

    class Gather:
        def __init__(self, at, span, recv, send):
            self.at, self.span, self.recv, self.send = at, span, recv, send

        def piece(self, h, df, ds, q=0, n=2):
            return self.at(h, ds, df, q, n) if h == 0 else self.at(h, df, ds, q, n)

        def post(self, h, axis, sem, by, df, ds, q=0, n=2):
            ref = self.piece(h, df, ds, q, n)
            to = device(dy=by) if (h == 0) == (axis == 0) else device(dz=by)
            copy(ref, ref, self.send, self.recv.at[sem], to).start()

        def wait(self, sem, quarters):
            ref = self.span(quarters)
            copy(ref, ref, self.send, self.recv.at[sem], partner).wait_recv()

        def start_first(self):
            for h in (0, 1):
                for by in (1, -1):
                    self.post(h, 0, 0, by, 0, 0)

        def start_second(self):
            for h in (0, 1):
                for by in (1, -1):
                    self.post(h, 1, 2, by, 0, 0)

        def first_axis(self):
            self.wait(0, 8)
            for h in (0, 1):
                for q, by in ((0, 1), (1, -1)):
                    self.post(h, 0, 1, by, -by, 0, q, 1)
            for turn in (0, 1):
                for h in (0, 1):
                    for by in (1, -1):
                        self.post(h, 1, 3 + turn, by, -by if turn == 0 else by, 0)

        def far_first(self):
            self.wait(1, 4)
            for h in (0, 1):
                for by in (1, -1):
                    self.post(h, 1, 5, by, 2, 0)

        def relay(self, minus, plus):
            self.wait(2 + minus, 8)
            for h in (0, 1):
                for q, by, j in ((0, 1, minus), (1, -1, plus)):
                    self.post(h, 1, 6 + j, by, OFFSETS[j], -by, q, 1)

        def far_second(self, j):
            self.wait(6 + j, 4)

    up = Gather(up_at, lambda n: upw.at[0:n * (depth // 2), :], up_recv, up_send)
    dn = Gather(dn_at, lambda n: dnw.at[0:n * (half // 2), :], dn_recv, dn_send)

    loads[0].wait()
    loads[1].start()
    loads[2].start()
    for h in (0, 1):
        block = fs if h == 0 else y * SIDE + z
        row = pl.multiple_of(h * blocks * depth + block * depth, depth)
        upw[pl.ds(row, depth), :] = up_ref[:, h * half:(h + 1) * half].astype(BF)
    pl.semaphore_wait(barrier, len(peers))
    up.start_first()

    loads[1].wait()
    values = tokens_ref[...].astype(F32)
    scale = lax.rsqrt(jnp.mean(values * values, axis=-1, keepdims=True) + epsilon)
    tok[0:rows, :] = (values * scale * gain_ref[...]).astype(BF)

    def tok_at(slot, q):
        row = slot * rows + q * (rows // 2)
        return tok.at[row:row + rows // 2, :]

    def tok_post(sem, slot, there, q, by):
        copy(tok_at(slot, q), tok_at(there, q), tok_send, tok_recv.at[sem], device(dx=by)).start()

    def tok_wait(sem, halves):
        ref = tok.at[0:halves * (rows // 2), :]
        copy(ref, ref, tok_send, tok_recv.at[sem], partner).wait_recv()

    tok_post(0, 0, 1, 0, 1)
    tok_post(0, 0, 2, 1, -1)
    tok_post(1, 0, 1, 1, 1)
    tok_post(1, 0, 2, 0, -1)
    up.start_second()
    loads[2].wait()

    own = pl.multiple_of(fs * 4 * half, 4 * half)
    dnw[pl.ds(own, 2 * half), :] = down_ref[...].astype(BF)

    def dn_block(b, to_partner):
        block = near(z, ORDER[b][0]) * SIDE + near(y, ORDER[b][1])
        row = block * 4 * half + (2 * half if to_partner else 0)
        return dnw.at[pl.ds(pl.multiple_of(row, 2 * half), 2 * half), :]

    def dn_share(h, *bs):
        for b in bs:
            block = near(z, ORDER[b][0]) * SIDE + near(y, ORDER[b][1])
            mine, theirs = (
                dnw.at[pl.ds(pl.multiple_of(block * 4 * half + (2 * side + h) * half, half), half), :] for side in (0, 1)
            )
            copy(mine, theirs, dn_pair_send, dn_pair.at[(b + 1) // 2], partner).start()

    def up_plane(h, p, to_partner):
        plane = near(z if h == 0 else y, OFFSETS[p])
        row = (h + (2 if to_partner else 0)) * blocks * depth + plane * SIDE * depth
        return upw.at[pl.ds(pl.multiple_of(row, SIDE * depth), SIDE * depth), :]

    def up_share(j, p):
        for h in (0, 1):
            plane = near(z if h == 0 else y, OFFSETS[p])
            row = (plane * SIDE + near(y if h == 0 else z, OFFSETS[j])) * depth
            mine, theirs = (
                upw.at[pl.ds(pl.multiple_of((h + 2 * side) * blocks * depth + row, depth), depth), :] for side in (0, 1)
            )
            copy(mine, theirs, up_pair_send, up_pair.at[p], partner).start()

    def up_shared(p):
        ref = upw.at[0:2 * SIDE * depth, :]
        copy(ref, ref, up_pair_send, up_pair.at[p], partner).wait_recv()

    dn.start_first()
    up_share(0, 0)
    for h in (0, 1):
        dn_share(h, 0)

    up.first_axis()
    up_share(1, 0)
    up_share(2, 0)
    up.relay(0, 0)
    up_share(0, 1)
    up_share(0, 2)
    up.far_first()
    up_share(3, 0)
    tok_wait(0, 2)
    tok_post(1, 1, 3, 0, 1)
    tok_post(1, 2, 3, 1, -1)
    for minus, plus in ((1, 2), (2, 1), (3, 3)):
        up.relay(minus, plus)
        up_share(minus, 1)
        up_share(plus, 2)
    dn.start_second()
    dn.first_axis()
    dn_share(0, 1, 2)
    dn_share(1, 3, 4)
    tok_wait(1, 4)

    def columns_of(h, p):
        plane = near(z if h == 0 else y, OFFSETS[p])
        if h == 0:
            return tok[:, pl.ds(pl.multiple_of(plane * SIDE * depth, SIDE * depth), SIDE * depth)]
        return jnp.concatenate(
            [tok[:, pl.ds(pl.multiple_of((a * SIDE + plane) * depth, depth), depth)] for a in range(SIDE)], axis=1
        )

    def dot(a, b):
        return jnp.dot(a, b, preferred_element_type=F32)

    tile = 256

    def early(h, other):
        for n in range(half // tile):
            cols = slice(n * tile, (n + 1) * tile)
            total = sum(dot(columns_of(h, p), up_plane(h, p, other)[:, cols]) for p in (0, 1, 2))
            at = (2 * other + h) * half + n * tile
            pre[:, at:at + tile] = total

    def late(h, other):
        for n in range(half // tile):
            cols = slice(n * tile, (n + 1) * tile)
            at = (2 * other + h) * half + n * tile
            total = pre[:, at:at + tile] + dot(columns_of(h, 3), up_plane(h, 3, other)[:, cols])
            hid[:, at:at + tile] = jnp.square(jnp.maximum(total, 0.0)).astype(BF)

    for h in (0, 1):
        early(h, 0)
    for p in (0, 1, 2):
        up_shared(p)
    for j in (0, 1):
        up.far_second(j)
        up_share(j, 3)
    for h in (0, 1):
        early(h, 1)
    for j in (2, 3):
        up.far_second(j)
        up_share(j, 3)
    for h in (0, 1):
        late(h, 0)
    up_shared(3)
    for h in (0, 1):
        late(h, 1)

    def part_at(b, slot, q=0, n=2):
        row = (b * 3 + slot) * rows + q * (rows // 2)
        return part.at[row:row + n * (rows // 2), :]

    def project(group):
        pieces = []
        g = GROUPS.index(group)
        ref = dnw.at[0:len(group) * 2 * half, :]
        copy(ref, ref, dn_pair_send, dn_pair.at[g], partner).wait_recv()
        for b in group:
            block = near(z, ORDER[b][0]) * SIDE + near(y, ORDER[b][1])
            pieces.append(dnw[pl.ds(pl.multiple_of(block * 4 * half, 4 * half), 4 * half), :])
        weights = jnp.concatenate(pieces, axis=1) if len(pieces) > 1 else pieces[0]
        both = jnp.concatenate([dot(hid[at:at + 2 * rows, :], weights) for at in (0, 2 * rows)], axis=0)
        terms = [both[:, i * rows:(i + 1) * rows] for i in range(len(group))]
        for side, by in ((0, 1), (1, -1)):
            row = 3 * rows + side * (rows // 2)
            out, there = first_at(first_out, side, g), first_at(first, side, g)
            out[...] = code(jnp.concatenate([t[row:row + rows // 2] for t in terms], axis=0))
            copy(out, there, rs_send, first_recv.at[g], device(dx=by)).start()
        for b, t in zip(group, terms):
            part[b * 3 * rows:(b + 1) * 3 * rows, :] = t[:3 * rows]

    def first_at(ref, side, g):
        return ref.at[side, g, 0:coded_rows(len(GROUPS[g]) * rows // 2), :]

    def last_at(ref, side, g):
        return ref.at[side, g, 0:coded_rows(len(GROUPS[g]) * rows), :]

    def pass_on(g):
        came = dnw.at[0:2 * coded_rows(len(GROUPS[g]) * rows // 2), :]
        copy(came, came, rs_send, first_recv.at[g], partner).wait_recv()
        for side, by in ((0, 1), (1, -1)):
            slot = 2 - side
            got = decode(first_at(first, side, g)[...])
            ordered = []
            for i, b in enumerate(GROUPS[g]):
                summed = part_at(b, slot, side, 1)[...] + got[i * (rows // 2):(i + 1) * (rows // 2)]
                other = part_at(b, slot, 1 - side, 1)[...]
                ordered += [summed, other] if side == 0 else [other, summed]
            out, there = last_at(last_out, side, g), last_at(last, side, g)
            out[...] = code(jnp.concatenate(ordered, axis=0))
            copy(out, there, rs_send, last_recv.at[g], device(dx=by)).start()

    def finish(g):
        came = dnw.at[0:2 * coded_rows(len(GROUPS[g]) * rows), :]
        copy(came, came, rs_send, last_recv.at[g], partner).wait_recv()
        got = decode(last_at(last, 0, g)[...]) + decode(last_at(last, 1, g)[...])
        for i, b in enumerate(GROUPS[g]):
            block = near(z, ORDER[b][0]) * SIDE + near(y, ORDER[b][1])
            total = part_at(b, 0)[...] + got[i * rows:(i + 1) * rows]
            out_ref[:, pl.ds(pl.multiple_of(block * rows, rows), rows)] = total.astype(BF)

    project(GROUPS[0])
    dn.relay(0, 0)
    dn_share(1, 1, 2)
    dn_share(0, 3, 4)
    project(GROUPS[1])
    dn.far_first()
    dn_share(0, 10)
    dn_share(1, 9)
    project(GROUPS[2])
    pass_on(0)
    dn.relay(1, 2)
    for h in (0, 1):
        dn_share(h, 5, 6)
    pass_on(1)
    project(GROUPS[3])
    dn.relay(2, 1)
    for h in (0, 1):
        dn_share(h, 7, 8)
    pass_on(2)
    dn.far_second(0)
    dn_share(0, 9)
    dn_share(1, 10)
    project(GROUPS[4])
    finish(0)
    project(GROUPS[5])
    dn.relay(3, 3)
    dn_share(0, 11, 13)
    dn_share(1, 12, 14)
    pass_on(3)
    finish(1)
    dn.far_second(1)
    dn_share(1, 11)
    dn_share(0, 12)
    pass_on(4)
    dn.far_second(2)
    dn_share(1, 13)
    dn_share(0, 14)
    project(GROUPS[6])
    project(GROUPS[7])
    pass_on(5)
    dn.far_second(3)
    for h in (0, 1):
        dn_share(h, 15)
    finish(2)
    finish(3)
    project(GROUPS[8])
    pass_on(6)
    finish(4)
    pass_on(7)
    pass_on(8)
    for g in (5, 6, 7, 8):
        finish(g)

    def drained(ref, sem):
        pltpu.make_async_copy(ref, ref, sem).wait()

    drained(upw.at[pl.ds(0, 15 * 4 * depth // 2), :], up_send)
    drained(dnw.at[pl.ds(0, 15 * 4 * half // 2), :], dn_send)
    drained(upw.at[pl.ds(0, 2 * blocks * depth), :], up_pair_send)
    drained(dnw.at[pl.ds(0, blocks * 2 * half), :], dn_pair_send)
    drained(tok.at[pl.ds(0, 3 * rows), :], tok_send)
    sent = sum(coded_rows(len(g) * rows // 2) + coded_rows(len(g) * rows) for g in GROUPS)
    drained(dnw.at[0:2 * sent, :], rs_send)


def shards(tokens, norm_gain, up_weight, down_weight):
    rows, width = tokens.shape
    depth, inner = up_weight.shape
    blocks = SIDE * SIDE
    vmem = pl.BlockSpec(memory_space=pltpu.VMEM)
    anywhere = pl.BlockSpec(memory_space=pl.ANY)
    dma = pltpu.SemaphoreType.DMA
    return pl.pallas_call(
        kernel,
        out_shape=jax.ShapeDtypeStruct((rows, width), BF),
        in_specs=[anywhere, vmem, anywhere, anywhere],
        out_specs=vmem,
        scratch_shapes=[
            pltpu.VMEM(tokens.shape, BF),
            pltpu.VMEM(up_weight.shape, F32),
            pltpu.VMEM(down_weight.shape, F32),
            pltpu.VMEM((SIDE * rows, width), BF),
            pltpu.VMEM((4 * blocks * depth, inner // 2), BF),
            pltpu.VMEM((blocks * 2 * inner, rows), BF),
            pltpu.VMEM((SIDE * rows, 2 * inner), F32),
            pltpu.VMEM((SIDE * rows, 2 * inner), BF),
            pltpu.VMEM((blocks * 3 * rows, rows), F32),
            pltpu.VMEM((2, len(GROUPS), coded_rows(rows), rows), BF),
            pltpu.VMEM((2, len(GROUPS), coded_rows(2 * rows), rows), BF),
            pltpu.VMEM((2, len(GROUPS), coded_rows(rows), rows), BF),
            pltpu.VMEM((2, len(GROUPS), coded_rows(2 * rows), rows), BF),
            dma((10,)), dma((10,)), dma((4,)), dma((len(GROUPS),)), dma((2,)), dma((len(GROUPS),)), dma((len(GROUPS),)),
            dma, dma, dma, dma, dma, dma, dma((3,)),
        ],
        compiler_params=pltpu.CompilerParams(
            collective_id=0, has_side_effects=True, vmem_limit_bytes=56_000_000
        ),
    )(tokens, norm_gain.reshape(1, width), up_weight, down_weight)


def solution(mesh):
    placed = (P(("fs", "tp"), None), P(), P("fs", "tp"), P("tp", "fs"))
    return jax.shard_map(
        shards, mesh=mesh, in_specs=placed, out_specs=P(("fs", "tp"), None), check_vma=False
    )
```

```python
import jax
import jax.numpy as jnp
from jax import lax
from jax.experimental import pallas as pl
from jax.experimental.pallas import tpu as pltpu
from jax.sharding import PartitionSpec as P

epsilon = 1e-06
MESH = pl.DeviceIdType.MESH
SIDE = 4
OFFSETS = (0, -1, 1, 2)
BF = jnp.bfloat16
F32 = jnp.float32

ORDER = (
    (0, 0),
    (0, -1), (0, 1), (-1, 0), (1, 0),
    (-1, -1), (1, 1), (-1, 1), (1, -1),
    (2, 0), (0, 2),
    (-1, 2), (2, -1), (1, 2), (2, 1),
    (2, 2),
)


GROUPS = ((0,), (1, 2), (3, 4), (5, 6), (7, 8), (9, 10), (11, 12), (13, 14), (15,))


LEVELS = 248 * 128 - 1
LOWEST = 123.0


def coded_rows(rows):
    return rows + 16


def code(values):
    groups = values.reshape(-1, 8, values.shape[1])
    top = jnp.maximum(jnp.max(jnp.abs(groups), axis=0), 1e-20)
    exponent = jnp.ceil(jnp.log2(top * (1.0 / LEVELS)) + 0.001)
    scaled = groups * jnp.exp2(-exponent)
    level = jnp.round(jnp.abs(scaled))
    e = jnp.floor(level * (1.0 / 128.0))
    word = jnp.exp2(e - LOWEST) * (level * (1.0 / 128.0) + (1.0 - e))
    word = jnp.where(scaled < 0.0, -word, word)
    both = jnp.concatenate([word, exponent[None], exponent[None]], axis=0)
    return both.reshape(-1, values.shape[1]).astype(BF)


def decode(coded):
    groups = coded.astype(F32).reshape(-1, 8, coded.shape[1])
    words, unit = groups[:-2], jnp.exp2(groups[-1])
    size = jnp.abs(words)
    e = jnp.floor(jnp.log2(size) + 0.001)
    level = (e + size * jnp.exp2(-e)) * 128.0 + (LOWEST - 1.0) * 128.0
    return (jnp.where(words < 0.0, -level, level) * unit).reshape(-1, coded.shape[1])


def kernel(
    tokens_hbm, gain_ref, up_hbm, down_hbm, out_ref,
    tokens_ref, up_ref, down_ref, tok, upw, dnw, pre, hid, part, first, last, first_out, last_out,
    up_recv, dn_recv, up_pair, dn_pair, tok_recv, first_recv, last_recv,
    up_send, dn_send, up_pair_send, dn_pair_send, tok_send, rs_send, load,
):
    rows, width = tokens_ref.shape
    half = up_ref.shape[1] // 2
    depth = up_ref.shape[0]
    blocks = SIDE * SIDE
    fs = lax.axis_index("fs")
    tp = lax.axis_index("tp")
    z, y, x, core = fs // SIDE, fs % SIDE, tp // 2, tp % 2

    def near(at, by):
        return (at + (by + SIDE)) % SIDE

    def device(dz=0, dy=0, dx=0):
        return {"fs": near(z, dz) * SIDE + near(y, dy), "tp": near(x, dx) * 2 + core}

    partner = {"fs": fs, "tp": x * 2 + (1 - core)}

    def copy(src, dst, send_sem, recv_sem, to):
        return pltpu.make_async_remote_copy(
            src_ref=src, dst_ref=dst, send_sem=send_sem, recv_sem=recv_sem,
            device_id=to, device_id_type=MESH,
        )

    barrier = pltpu.get_barrier_semaphore()
    peers = [device(dz=1), device(dz=-1), device(dy=1), device(dy=-1), device(dx=1), device(dx=-1), partner]
    for peer in peers:
        pl.semaphore_signal(barrier, inc=1, device_id=peer, device_id_type=MESH)

    loads = [
        pltpu.make_async_copy(src, dst, load.at[i])
        for i, (src, dst) in enumerate(((up_hbm, up_ref), (tokens_hbm, tokens_ref), (down_hbm, down_ref)))
    ]
    loads[0].start()

    def up_at(h, dz, dy, q, n):
        zs, ys = near(z, dz), near(y, dy)
        block = zs * SIDE + ys if h == 0 else ys * SIDE + zs
        row = h * blocks * depth + block * depth + q * (depth // 2)
        return upw.at[pl.ds(pl.multiple_of(row, depth // 2), n * (depth // 2)), :]

    def dn_at(h, dz, dy, q, n):
        block = near(z, dz) * SIDE + near(y, dy)
        row = block * 4 * half + h * half + q * (half // 2)
        return dnw.at[pl.ds(pl.multiple_of(row, half // 2), n * (half // 2)), :]

    class Gather:
        def __init__(self, at, span, recv, send):
            self.at, self.span, self.recv, self.send = at, span, recv, send

        def piece(self, h, df, ds, q=0, n=2):
            return self.at(h, ds, df, q, n) if h == 0 else self.at(h, df, ds, q, n)

        def post(self, h, axis, sem, by, df, ds, q=0, n=2):
            ref = self.piece(h, df, ds, q, n)
            to = device(dy=by) if (h == 0) == (axis == 0) else device(dz=by)
            copy(ref, ref, self.send, self.recv.at[sem], to).start()

        def wait(self, sem, quarters):
            ref = self.span(quarters)
            copy(ref, ref, self.send, self.recv.at[sem], partner).wait_recv()

        def start_first(self):
            for h in (0, 1):
                for by in (1, -1):
                    self.post(h, 0, 0, by, 0, 0)

        def start_second(self):
            for h in (0, 1):
                for by in (1, -1):
                    self.post(h, 1, 2, by, 0, 0)

        def first_axis(self):
            self.wait(0, 8)
            for h in (0, 1):
                for q, by in ((0, 1), (1, -1)):
                    self.post(h, 0, 1, by, -by, 0, q, 1)
            for turn in (0, 1):
                for h in (0, 1):
                    for by in (1, -1):
                        self.post(h, 1, 3 + turn, by, -by if turn == 0 else by, 0)

        def far_first(self):
            self.wait(1, 4)
            for h in (0, 1):
                for by in (1, -1):
                    self.post(h, 1, 5, by, 2, 0)

        def relay(self, minus, plus):
            self.wait(2 + minus, 8)
            for h in (0, 1):
                for q, by, j in ((0, 1, minus), (1, -1, plus)):
                    self.post(h, 1, 6 + j, by, OFFSETS[j], -by, q, 1)

        def far_second(self, j):
            self.wait(6 + j, 4)

    up = Gather(up_at, lambda n: upw.at[0:n * (depth // 2), :], up_recv, up_send)
    dn = Gather(dn_at, lambda n: dnw.at[0:n * (half // 2), :], dn_recv, dn_send)

    loads[0].wait()
    loads[1].start()
    loads[2].start()
    for h in (0, 1):
        block = fs if h == 0 else y * SIDE + z
        row = pl.multiple_of(h * blocks * depth + block * depth, depth)
        upw[pl.ds(row, depth), :] = up_ref[:, h * half:(h + 1) * half].astype(BF)
    pl.semaphore_wait(barrier, len(peers))
    up.start_first()

    loads[1].wait()
    values = tokens_ref[...].astype(F32)
    scale = lax.rsqrt(jnp.mean(values * values, axis=-1, keepdims=True) + epsilon)
    tok[0:rows, :] = (values * scale * gain_ref[...]).astype(BF)

    def tok_at(slot, q):
        row = slot * rows + q * (rows // 2)
        return tok.at[row:row + rows // 2, :]

    def tok_post(sem, slot, there, q, by):
        copy(tok_at(slot, q), tok_at(there, q), tok_send, tok_recv.at[sem], device(dx=by)).start()

    def tok_wait(sem, halves):
        ref = tok.at[0:halves * (rows // 2), :]
        copy(ref, ref, tok_send, tok_recv.at[sem], partner).wait_recv()

    tok_post(0, 0, 1, 0, 1)
    tok_post(0, 0, 2, 1, -1)
    tok_post(1, 0, 1, 1, 1)
    tok_post(1, 0, 2, 0, -1)
    up.start_second()
    loads[2].wait()

    own = pl.multiple_of(fs * 4 * half, 4 * half)
    dnw[pl.ds(own, 2 * half), :] = down_ref[...].astype(BF)

    def dn_block(b, to_partner):
        block = near(z, ORDER[b][0]) * SIDE + near(y, ORDER[b][1])
        row = block * 4 * half + (2 * half if to_partner else 0)
        return dnw.at[pl.ds(pl.multiple_of(row, 2 * half), 2 * half), :]

    def dn_share(h, *bs):
        for b in bs:
            block = near(z, ORDER[b][0]) * SIDE + near(y, ORDER[b][1])
            mine, theirs = (
                dnw.at[pl.ds(pl.multiple_of(block * 4 * half + (2 * side + h) * half, half), half), :] for side in (0, 1)
            )
            copy(mine, theirs, dn_pair_send, dn_pair.at[(b + 1) // 2], partner).start()

    def up_plane(h, p, to_partner):
        plane = near(z if h == 0 else y, OFFSETS[p])
        row = (h + (2 if to_partner else 0)) * blocks * depth + plane * SIDE * depth
        return upw.at[pl.ds(pl.multiple_of(row, SIDE * depth), SIDE * depth), :]

    def up_share(j, p):
        for h in (0, 1):
            plane = near(z if h == 0 else y, OFFSETS[p])
            row = (plane * SIDE + near(y if h == 0 else z, OFFSETS[j])) * depth
            mine, theirs = (
                upw.at[pl.ds(pl.multiple_of((h + 2 * side) * blocks * depth + row, depth), depth), :] for side in (0, 1)
            )
            copy(mine, theirs, up_pair_send, up_pair.at[p], partner).start()

    def up_shared(p):
        ref = upw.at[0:2 * SIDE * depth, :]
        copy(ref, ref, up_pair_send, up_pair.at[p], partner).wait_recv()

    dn.start_first()
    up_share(0, 0)
    for h in (0, 1):
        dn_share(h, 0)

    up.first_axis()
    up_share(1, 0)
    up_share(2, 0)
    up.relay(0, 0)
    up_share(0, 1)
    up_share(0, 2)
    up.far_first()
    up_share(3, 0)
    tok_wait(0, 2)
    tok_post(1, 1, 3, 0, 1)
    tok_post(1, 2, 3, 1, -1)
    for minus, plus in ((1, 2), (2, 1), (3, 3)):
        up.relay(minus, plus)
        up_share(minus, 1)
        up_share(plus, 2)
    dn.start_second()
    dn.first_axis()
    dn_share(0, 1, 2)
    dn_share(1, 3, 4)
    tok_wait(1, 4)

    def columns_of(h, p):
        plane = near(z if h == 0 else y, OFFSETS[p])
        if h == 0:
            return tok[:, pl.ds(pl.multiple_of(plane * SIDE * depth, SIDE * depth), SIDE * depth)]
        return jnp.concatenate(
            [tok[:, pl.ds(pl.multiple_of((a * SIDE + plane) * depth, depth), depth)] for a in range(SIDE)], axis=1
        )

    def dot(a, b):
        return jnp.dot(a, b, preferred_element_type=F32)

    tile = 256

    def early(h, other):
        for n in range(half // tile):
            cols = slice(n * tile, (n + 1) * tile)
            total = sum(dot(columns_of(h, p), up_plane(h, p, other)[:, cols]) for p in (0, 1, 2))
            at = (2 * other + h) * half + n * tile
            pre[:, at:at + tile] = total

    def late(h, other):
        for n in range(half // tile):
            cols = slice(n * tile, (n + 1) * tile)
            at = (2 * other + h) * half + n * tile
            total = pre[:, at:at + tile] + dot(columns_of(h, 3), up_plane(h, 3, other)[:, cols])
            hid[:, at:at + tile] = jnp.square(jnp.maximum(total, 0.0)).astype(BF)

    for h in (0, 1):
        early(h, 0)
    for p in (0, 1, 2):
        up_shared(p)
    for j in (0, 1):
        up.far_second(j)
        up_share(j, 3)
    for h in (0, 1):
        early(h, 1)
    for j in (2, 3):
        up.far_second(j)
        up_share(j, 3)
    for h in (0, 1):
        late(h, 0)
    def near_own():
        dn.relay(0, 0)
        dn_share(1, 1, 2)
        dn_share(0, 3, 4)

    def farthest():
        dn.far_second(3)
        for h in (0, 1):
            dn_share(h, 15)

    pl.when(core == 1)(near_own)
    up_shared(3)
    for h in (0, 1):
        late(h, 1)

    def part_at(b, slot, q=0, n=2):
        row = (b * 3 + slot) * rows + q * (rows // 2)
        return part.at[row:row + n * (rows // 2), :]

    def project(group):
        g = GROUPS.index(group)

        def product(depth_from, depth_to):
            pieces = []
            for b in group:
                block = near(z, ORDER[b][0]) * SIDE + near(y, ORDER[b][1])
                row = pl.multiple_of(block * 4 * half + depth_from, half)
                pieces.append(dnw[pl.ds(row, depth_to - depth_from), :])
            weights = jnp.concatenate(pieces, axis=1) if len(pieces) > 1 else pieces[0]
            parts = [dot(hid[at:at + 2 * rows, depth_from:depth_to], weights) for at in (0, 2 * rows)]
            return jnp.concatenate(parts, axis=0)

        last_group = g == len(GROUPS) - 1
        if last_group:
            pre[:, :rows] = product(0, 2 * half)
        ref = dnw.at[0:len(group) * 2 * half, :]
        copy(ref, ref, dn_pair_send, dn_pair.at[g], partner).wait_recv()
        both = pre[:, :rows] + product(2 * half, 4 * half) if last_group else product(0, 4 * half)
        terms = [both[:, i * rows:(i + 1) * rows] for i in range(len(group))]
        for side, by in ((0, 1), (1, -1)):
            row = 3 * rows + side * (rows // 2)
            out, there = first_at(first_out, side, g), first_at(first, side, g)
            out[...] = code(jnp.concatenate([t[row:row + rows // 2] for t in terms], axis=0))
            copy(out, there, rs_send, first_recv.at[g], device(dx=by)).start()
        for b, t in zip(group, terms):
            part[b * 3 * rows:(b + 1) * 3 * rows, :] = t[:3 * rows]

    def first_at(ref, side, g):
        return ref.at[side, g, 0:coded_rows(len(GROUPS[g]) * rows // 2), :]

    def last_at(ref, side, g):
        return ref.at[side, g, 0:coded_rows(len(GROUPS[g]) * rows), :]

    def pass_on(g):
        came = dnw.at[0:2 * coded_rows(len(GROUPS[g]) * rows // 2), :]
        copy(came, came, rs_send, first_recv.at[g], partner).wait_recv()
        for side, by in ((0, 1), (1, -1)):
            slot = 2 - side
            got = decode(first_at(first, side, g)[...])
            ordered = []
            for i, b in enumerate(GROUPS[g]):
                summed = part_at(b, slot, side, 1)[...] + got[i * (rows // 2):(i + 1) * (rows // 2)]
                other = part_at(b, slot, 1 - side, 1)[...]
                ordered += [summed, other] if side == 0 else [other, summed]
            out, there = last_at(last_out, side, g), last_at(last, side, g)
            out[...] = code(jnp.concatenate(ordered, axis=0))
            copy(out, there, rs_send, last_recv.at[g], device(dx=by)).start()

    def finish(g):
        came = dnw.at[0:2 * coded_rows(len(GROUPS[g]) * rows), :]
        copy(came, came, rs_send, last_recv.at[g], partner).wait_recv()
        got = decode(last_at(last, 0, g)[...]) + decode(last_at(last, 1, g)[...])
        for i, b in enumerate(GROUPS[g]):
            block = near(z, ORDER[b][0]) * SIDE + near(y, ORDER[b][1])
            total = part_at(b, 0)[...] + got[i * rows:(i + 1) * rows]
            out_ref[:, pl.ds(pl.multiple_of(block * rows, rows), rows)] = total.astype(BF)

    project(GROUPS[0])
    pl.when(core == 0)(near_own)
    project(GROUPS[1])
    dn.far_first()
    dn_share(0, 10)
    dn_share(1, 9)
    project(GROUPS[2])
    pass_on(0)
    dn.relay(1, 2)
    for h in (0, 1):
        dn_share(h, 5, 6)
    pass_on(1)
    project(GROUPS[3])
    dn.relay(2, 1)
    for h in (0, 1):
        dn_share(h, 7, 8)
    pass_on(2)
    dn.far_second(0)
    dn_share(0, 9)
    dn_share(1, 10)
    project(GROUPS[4])
    finish(0)
    project(GROUPS[5])
    dn.relay(3, 3)
    dn_share(0, 11, 13)
    dn_share(1, 12, 14)
    pass_on(3)
    finish(1)
    dn.far_second(1)
    dn_share(1, 11)
    dn_share(0, 12)
    pass_on(4)
    dn.far_second(2)
    dn_share(1, 13)
    dn_share(0, 14)
    project(GROUPS[6])
    pl.when(core == 1)(farthest)
    project(GROUPS[7])
    pass_on(5)
    pl.when(core == 0)(farthest)
    finish(2)
    finish(3)
    project(GROUPS[8])
    pass_on(6)
    finish(4)
    pass_on(7)
    pass_on(8)
    for g in (5, 6, 7, 8):
        finish(g)

    def drained(ref, sem):
        pltpu.make_async_copy(ref, ref, sem).wait()

    drained(upw.at[pl.ds(0, 15 * 4 * depth // 2), :], up_send)
    drained(dnw.at[pl.ds(0, 15 * 4 * half // 2), :], dn_send)
    drained(upw.at[pl.ds(0, 2 * blocks * depth), :], up_pair_send)
    drained(dnw.at[pl.ds(0, blocks * 2 * half), :], dn_pair_send)
    drained(tok.at[pl.ds(0, 3 * rows), :], tok_send)
    sent = sum(coded_rows(len(g) * rows // 2) + coded_rows(len(g) * rows) for g in GROUPS)
    drained(dnw.at[0:2 * sent, :], rs_send)


def shards(tokens, norm_gain, up_weight, down_weight):
    rows, width = tokens.shape
    depth, inner = up_weight.shape
    blocks = SIDE * SIDE
    vmem = pl.BlockSpec(memory_space=pltpu.VMEM)
    anywhere = pl.BlockSpec(memory_space=pl.ANY)
    dma = pltpu.SemaphoreType.DMA
    return pl.pallas_call(
        kernel,
        out_shape=jax.ShapeDtypeStruct((rows, width), BF),
        in_specs=[anywhere, vmem, anywhere, anywhere],
        out_specs=vmem,
        scratch_shapes=[
            pltpu.VMEM(tokens.shape, BF),
            pltpu.VMEM(up_weight.shape, F32),
            pltpu.VMEM(down_weight.shape, F32),
            pltpu.VMEM((SIDE * rows, width), BF),
            pltpu.VMEM((4 * blocks * depth, inner // 2), BF),
            pltpu.VMEM((blocks * 2 * inner, rows), BF),
            pltpu.VMEM((SIDE * rows, 2 * inner), F32),
            pltpu.VMEM((SIDE * rows, 2 * inner), BF),
            pltpu.VMEM((blocks * 3 * rows, rows), F32),
            pltpu.VMEM((2, len(GROUPS), coded_rows(rows), rows), BF),
            pltpu.VMEM((2, len(GROUPS), coded_rows(2 * rows), rows), BF),
            pltpu.VMEM((2, len(GROUPS), coded_rows(rows), rows), BF),
            pltpu.VMEM((2, len(GROUPS), coded_rows(2 * rows), rows), BF),
            dma((10,)), dma((10,)), dma((4,)), dma((len(GROUPS),)), dma((2,)), dma((len(GROUPS),)), dma((len(GROUPS),)),
            dma, dma, dma, dma, dma, dma, dma((3,)),
        ],
        compiler_params=pltpu.CompilerParams(
            collective_id=0, has_side_effects=True, vmem_limit_bytes=56_000_000
        ),
    )(tokens, norm_gain.reshape(1, width), up_weight, down_weight)


def solution(mesh):
    placed = (P(("fs", "tp"), None), P(), P("fs", "tp"), P("tp", "fs"))
    return jax.shard_map(
        shards, mesh=mesh, in_specs=placed, out_specs=P(("fs", "tp"), None), check_vma=False
    )
```

```python
import jax
import jax.numpy as jnp
from jax import lax
from jax.experimental import pallas as pl
from jax.experimental.pallas import tpu as pltpu
from jax.sharding import PartitionSpec as P

epsilon = 1e-06
MESH = pl.DeviceIdType.MESH
SIDE = 4
OFFSETS = (0, -1, 1, 2)
BF = jnp.bfloat16
F32 = jnp.float32

ORDER = (
    (0, 0),
    (0, -1), (0, 1), (-1, 0), (1, 0),
    (-1, -1), (1, 1), (-1, 1), (1, -1),
    (2, 0), (0, 2),
    (-1, 2), (2, -1), (1, 2), (2, 1),
    (2, 2),
)


GROUPS = ((0,), (1, 2), (3, 4), (5, 6), (7, 8), (9, 10), (11, 12), (13, 14), (15,))


LEVELS = 248 * 128 - 1
LOWEST = 123.0


def coded_rows(rows):
    return rows + 8


def code(values):
    groups = values.reshape(-1, 8, values.shape[1])
    top = jnp.maximum(jnp.max(jnp.abs(groups), axis=0), 1e-20)
    exponent = jnp.ceil(jnp.log2(top * (1.0 / LEVELS)) + 0.001)
    scaled = groups * jnp.exp2(-exponent)
    level = jnp.round(jnp.abs(scaled))
    e = jnp.floor(level * (1.0 / 128.0))
    word = jnp.exp2(e - LOWEST) * (level * (1.0 / 128.0) + (1.0 - e))
    word = jnp.where(scaled < 0.0, -word, word)
    both = jnp.concatenate([word, exponent[None]], axis=0)
    return both.reshape(-1, values.shape[1]).astype(BF)


def decode(coded):
    groups = coded.astype(F32).reshape(-1, 8, coded.shape[1])
    words, unit = groups[:-1], jnp.exp2(groups[-1])
    size = jnp.abs(words)
    e = jnp.floor(jnp.log2(size) + 0.001)
    level = (e + size * jnp.exp2(-e)) * 128.0 + (LOWEST - 1.0) * 128.0
    return (jnp.where(words < 0.0, -level, level) * unit).reshape(-1, coded.shape[1])


def kernel(
    tokens_hbm, gain_ref, up_hbm, down_hbm, out_ref,
    tokens_ref, up_ref, down_ref, tok, upw, dnw, pre, hid, part, first, last, first_out, last_out,
    up_recv, dn_recv, up_pair, dn_pair, tok_recv, first_recv, last_recv,
    up_send, dn_send, up_pair_send, dn_pair_send, tok_send, rs_send, load,
):
    rows, width = tokens_ref.shape
    half = up_ref.shape[1] // 2
    depth = up_ref.shape[0]
    blocks = SIDE * SIDE
    fs = lax.axis_index("fs")
    tp = lax.axis_index("tp")
    z, y, x, core = fs // SIDE, fs % SIDE, tp // 2, tp % 2

    def near(at, by):
        return (at + (by + SIDE)) % SIDE

    def device(dz=0, dy=0, dx=0):
        return {"fs": near(z, dz) * SIDE + near(y, dy), "tp": near(x, dx) * 2 + core}

    partner = {"fs": fs, "tp": x * 2 + (1 - core)}

    def copy(src, dst, send_sem, recv_sem, to):
        return pltpu.make_async_remote_copy(
            src_ref=src, dst_ref=dst, send_sem=send_sem, recv_sem=recv_sem,
            device_id=to, device_id_type=MESH,
        )

    barrier = pltpu.get_barrier_semaphore()
    peers = [device(dz=1), device(dz=-1), device(dy=1), device(dy=-1), device(dx=1), device(dx=-1), partner]
    for peer in peers:
        pl.semaphore_signal(barrier, inc=1, device_id=peer, device_id_type=MESH)

    loads = [
        pltpu.make_async_copy(src, dst, load.at[i])
        for i, (src, dst) in enumerate(((up_hbm, up_ref), (tokens_hbm, tokens_ref), (down_hbm, down_ref)))
    ]
    loads[0].start()

    def up_at(h, dz, dy, q, n):
        zs, ys = near(z, dz), near(y, dy)
        block = zs * SIDE + ys if h == 0 else ys * SIDE + zs
        row = h * blocks * depth + block * depth + q * (depth // 2)
        return upw.at[pl.ds(pl.multiple_of(row, depth // 2), n * (depth // 2)), :]

    def dn_at(h, dz, dy, q, n):
        block = near(z, dz) * SIDE + near(y, dy)
        row = block * 4 * half + h * half + q * (half // 2)
        return dnw.at[pl.ds(pl.multiple_of(row, half // 2), n * (half // 2)), :]

    class Gather:
        def __init__(self, at, span, recv, send):
            self.at, self.span, self.recv, self.send = at, span, recv, send

        def piece(self, h, df, ds, q=0, n=2):
            return self.at(h, ds, df, q, n) if h == 0 else self.at(h, df, ds, q, n)

        def post(self, h, axis, sem, by, df, ds, q=0, n=2):
            ref = self.piece(h, df, ds, q, n)
            to = device(dy=by) if (h == 0) == (axis == 0) else device(dz=by)
            copy(ref, ref, self.send, self.recv.at[sem], to).start()

        def wait(self, sem, quarters):
            ref = self.span(quarters)
            copy(ref, ref, self.send, self.recv.at[sem], partner).wait_recv()

        def start_first(self):
            for h in (0, 1):
                for by in (1, -1):
                    self.post(h, 0, 0, by, 0, 0)

        def start_second(self):
            for h in (0, 1):
                for by in (1, -1):
                    self.post(h, 1, 2, by, 0, 0)

        def first_axis(self):
            self.wait(0, 8)
            for h in (0, 1):
                for q, by in ((0, 1), (1, -1)):
                    self.post(h, 0, 1, by, -by, 0, q, 1)
            for turn in (0, 1):
                for h in (0, 1):
                    for by in (1, -1):
                        self.post(h, 1, 3 + turn, by, -by if turn == 0 else by, 0)

        def far_first(self):
            self.wait(1, 4)
            for h in (0, 1):
                for by in (1, -1):
                    self.post(h, 1, 5, by, 2, 0)

        def relay(self, minus, plus):
            self.wait(2 + minus, 8)
            for h in (0, 1):
                for q, by, j in ((0, 1, minus), (1, -1, plus)):
                    self.post(h, 1, 6 + j, by, OFFSETS[j], -by, q, 1)

        def far_second(self, j):
            self.wait(6 + j, 4)

    up = Gather(up_at, lambda n: upw.at[0:n * (depth // 2), :], up_recv, up_send)
    dn = Gather(dn_at, lambda n: dnw.at[0:n * (half // 2), :], dn_recv, dn_send)

    loads[0].wait()
    loads[1].start()
    loads[2].start()
    for h in (0, 1):
        block = fs if h == 0 else y * SIDE + z
        row = pl.multiple_of(h * blocks * depth + block * depth, depth)
        upw[pl.ds(row, depth), :] = up_ref[:, h * half:(h + 1) * half].astype(BF)
    pl.semaphore_wait(barrier, len(peers))
    up.start_first()

    loads[1].wait()
    values = tokens_ref[...].astype(F32)
    scale = lax.rsqrt(jnp.mean(values * values, axis=-1, keepdims=True) + epsilon)
    tok[0:rows, :] = (values * scale * gain_ref[...]).astype(BF)

    def tok_at(slot, q):
        row = slot * rows + q * (rows // 2)
        return tok.at[row:row + rows // 2, :]

    def tok_post(sem, slot, there, q, by):
        copy(tok_at(slot, q), tok_at(there, q), tok_send, tok_recv.at[sem], device(dx=by)).start()

    def tok_wait(sem, halves):
        ref = tok.at[0:halves * (rows // 2), :]
        copy(ref, ref, tok_send, tok_recv.at[sem], partner).wait_recv()

    tok_post(0, 0, 1, 0, 1)
    tok_post(0, 0, 2, 1, -1)
    tok_post(1, 0, 1, 1, 1)
    tok_post(1, 0, 2, 0, -1)
    up.start_second()
    loads[2].wait()

    own = pl.multiple_of(fs * 4 * half, 4 * half)
    dnw[pl.ds(own, 2 * half), :] = down_ref[...].astype(BF)

    def dn_block(b, to_partner):
        block = near(z, ORDER[b][0]) * SIDE + near(y, ORDER[b][1])
        row = block * 4 * half + (2 * half if to_partner else 0)
        return dnw.at[pl.ds(pl.multiple_of(row, 2 * half), 2 * half), :]

    def dn_share(h, *bs):
        for b in bs:
            block = near(z, ORDER[b][0]) * SIDE + near(y, ORDER[b][1])
            mine, theirs = (
                dnw.at[pl.ds(pl.multiple_of(block * 4 * half + (2 * side + h) * half, half), half), :] for side in (0, 1)
            )
            copy(mine, theirs, dn_pair_send, dn_pair.at[(b + 1) // 2], partner).start()

    def up_plane(h, p, to_partner):
        plane = near(z if h == 0 else y, OFFSETS[p])
        row = (h + (2 if to_partner else 0)) * blocks * depth + plane * SIDE * depth
        return upw.at[pl.ds(pl.multiple_of(row, SIDE * depth), SIDE * depth), :]

    def up_share(j, p):
        for h in (0, 1):
            plane = near(z if h == 0 else y, OFFSETS[p])
            row = (plane * SIDE + near(y if h == 0 else z, OFFSETS[j])) * depth
            mine, theirs = (
                upw.at[pl.ds(pl.multiple_of((h + 2 * side) * blocks * depth + row, depth), depth), :] for side in (0, 1)
            )
            copy(mine, theirs, up_pair_send, up_pair.at[p], partner).start()

    def up_shared(p):
        ref = upw.at[0:2 * SIDE * depth, :]
        copy(ref, ref, up_pair_send, up_pair.at[p], partner).wait_recv()

    dn.start_first()
    up_share(0, 0)
    for h in (0, 1):
        dn_share(h, 0)

    up.first_axis()
    up_share(1, 0)
    up_share(2, 0)
    up.relay(0, 0)
    up_share(0, 1)
    up_share(0, 2)
    up.far_first()
    up_share(3, 0)
    tok_wait(0, 2)
    tok_post(1, 1, 3, 0, 1)
    tok_post(1, 2, 3, 1, -1)
    for minus, plus in ((1, 2), (2, 1), (3, 3)):
        up.relay(minus, plus)
        up_share(minus, 1)
        up_share(plus, 2)
    dn.start_second()
    dn.first_axis()
    dn_share(0, 1, 2)
    dn_share(1, 3, 4)
    tok_wait(1, 4)

    def columns_of(h, p):
        plane = near(z if h == 0 else y, OFFSETS[p])
        if h == 0:
            return tok[:, pl.ds(pl.multiple_of(plane * SIDE * depth, SIDE * depth), SIDE * depth)]
        return jnp.concatenate(
            [tok[:, pl.ds(pl.multiple_of((a * SIDE + plane) * depth, depth), depth)] for a in range(SIDE)], axis=1
        )

    def dot(a, b):
        return jnp.dot(a, b, preferred_element_type=F32)

    tile = 256

    def early(h, other):
        for n in range(half // tile):
            cols = slice(n * tile, (n + 1) * tile)
            total = sum(dot(columns_of(h, p), up_plane(h, p, other)[:, cols]) for p in (0, 1, 2))
            at = (2 * other + h) * half + n * tile
            pre[:, at:at + tile] = total

    def late(h, other):
        for n in range(half // tile):
            cols = slice(n * tile, (n + 1) * tile)
            at = (2 * other + h) * half + n * tile
            total = pre[:, at:at + tile] + dot(columns_of(h, 3), up_plane(h, 3, other)[:, cols])
            hid[:, at:at + tile] = jnp.square(jnp.maximum(total, 0.0)).astype(BF)

    for h in (0, 1):
        early(h, 0)
    for p in (0, 1, 2):
        up_shared(p)
    for j in (0, 1):
        up.far_second(j)
        up_share(j, 3)
    for h in (0, 1):
        early(h, 1)
    for j in (2, 3):
        up.far_second(j)
        up_share(j, 3)
    for h in (0, 1):
        late(h, 0)
    def near_own():
        dn.relay(0, 0)
        dn_share(1, 1, 2)
        dn_share(0, 3, 4)

    def farthest():
        dn.far_second(3)
        for h in (0, 1):
            dn_share(h, 15)

    pl.when(core == 1)(near_own)
    up_shared(3)
    for h in (0, 1):
        late(h, 1)

    def part_at(b, slot, q=0, n=2):
        row = (b * 3 + slot) * rows + q * (rows // 2)
        return part.at[row:row + n * (rows // 2), :]

    def project(group):
        g = GROUPS.index(group)

        def product(depth_from, depth_to):
            pieces = []
            for b in group:
                block = near(z, ORDER[b][0]) * SIDE + near(y, ORDER[b][1])
                row = pl.multiple_of(block * 4 * half + depth_from, half)
                pieces.append(dnw[pl.ds(row, depth_to - depth_from), :])
            weights = jnp.concatenate(pieces, axis=1) if len(pieces) > 1 else pieces[0]
            parts = [dot(hid[at:at + 2 * rows, depth_from:depth_to], weights) for at in (0, 2 * rows)]
            return jnp.concatenate(parts, axis=0)

        last_group = g in (1, len(GROUPS) - 1)
        if last_group:
            pre[:, :len(group) * rows] = product(0, 2 * half)
        ref = dnw.at[0:len(group) * 2 * half, :]
        copy(ref, ref, dn_pair_send, dn_pair.at[g], partner).wait_recv()
        both = pre[:, :len(group) * rows] + product(2 * half, 4 * half) if last_group else product(0, 4 * half)
        terms = [both[:, i * rows:(i + 1) * rows] for i in range(len(group))]
        for side, by in ((0, 1), (1, -1)):
            row = 3 * rows + side * (rows // 2)
            out, there = first_at(first_out, side, g), first_at(first, side, g)
            out[...] = code(jnp.concatenate([t[row:row + rows // 2] for t in terms], axis=0))
            copy(out, there, rs_send, first_recv.at[g], device(dx=by)).start()
        for b, t in zip(group, terms):
            part[b * 3 * rows:(b + 1) * 3 * rows, :] = t[:3 * rows]

    def first_at(ref, side, g):
        return ref.at[side, g, 0:coded_rows(len(GROUPS[g]) * rows // 2), :]

    def last_at(ref, side, g):
        return ref.at[side, g, 0:coded_rows(len(GROUPS[g]) * rows), :]

    def pass_on(g):
        came = dnw.at[0:2 * coded_rows(len(GROUPS[g]) * rows // 2), :]
        copy(came, came, rs_send, first_recv.at[g], partner).wait_recv()
        for side, by in ((0, 1), (1, -1)):
            slot = 2 - side
            got = decode(first_at(first, side, g)[...])
            ordered = []
            for i, b in enumerate(GROUPS[g]):
                summed = part_at(b, slot, side, 1)[...] + got[i * (rows // 2):(i + 1) * (rows // 2)]
                other = part_at(b, slot, 1 - side, 1)[...]
                ordered += [summed, other] if side == 0 else [other, summed]
            out, there = last_at(last_out, side, g), last_at(last, side, g)
            out[...] = code(jnp.concatenate(ordered, axis=0))
            copy(out, there, rs_send, last_recv.at[g], device(dx=by)).start()

    def finish(g):
        came = dnw.at[0:2 * coded_rows(len(GROUPS[g]) * rows), :]
        copy(came, came, rs_send, last_recv.at[g], partner).wait_recv()
        got = decode(last_at(last, 0, g)[...]) + decode(last_at(last, 1, g)[...])
        for i, b in enumerate(GROUPS[g]):
            block = near(z, ORDER[b][0]) * SIDE + near(y, ORDER[b][1])
            total = part_at(b, 0)[...] + got[i * rows:(i + 1) * rows]
            out_ref[:, pl.ds(pl.multiple_of(block * rows, rows), rows)] = total.astype(BF)

    project(GROUPS[0])
    pl.when(core == 0)(near_own)
    project(GROUPS[1])
    dn.far_first()
    dn_share(0, 10)
    dn_share(1, 9)
    project(GROUPS[2])
    pass_on(0)
    dn.relay(1, 2)
    for h in (0, 1):
        dn_share(h, 5, 6)
    pass_on(1)
    project(GROUPS[3])
    dn.relay(2, 1)
    for h in (0, 1):
        dn_share(h, 7, 8)
    pass_on(2)
    dn.far_second(0)
    dn_share(0, 9)
    dn_share(1, 10)
    project(GROUPS[4])
    finish(0)
    project(GROUPS[5])
    dn.relay(3, 3)
    dn_share(0, 11, 13)
    dn_share(1, 12, 14)
    pass_on(3)
    finish(1)
    dn.far_second(1)
    dn_share(1, 11)
    dn_share(0, 12)
    pass_on(4)
    dn.far_second(2)
    dn_share(1, 13)
    dn_share(0, 14)
    project(GROUPS[6])
    pl.when(core == 1)(farthest)
    project(GROUPS[7])
    pass_on(5)
    pl.when(core == 0)(farthest)
    project(GROUPS[8])
    finish(2)
    finish(3)
    pass_on(6)
    finish(4)
    pass_on(7)
    pass_on(8)
    for g in (5, 6, 7, 8):
        finish(g)

    def drained(ref, sem):
        pltpu.make_async_copy(ref, ref, sem).wait()

    drained(upw.at[pl.ds(0, 15 * 4 * depth // 2), :], up_send)
    drained(dnw.at[pl.ds(0, 15 * 4 * half // 2), :], dn_send)
    drained(upw.at[pl.ds(0, 2 * blocks * depth), :], up_pair_send)
    drained(dnw.at[pl.ds(0, blocks * 2 * half), :], dn_pair_send)
    drained(tok.at[pl.ds(0, 3 * rows), :], tok_send)
    sent = sum(coded_rows(len(g) * rows // 2) + coded_rows(len(g) * rows) for g in GROUPS)
    drained(dnw.at[0:2 * sent, :], rs_send)


def shards(tokens, norm_gain, up_weight, down_weight):
    rows, width = tokens.shape
    depth, inner = up_weight.shape
    blocks = SIDE * SIDE
    vmem = pl.BlockSpec(memory_space=pltpu.VMEM)
    anywhere = pl.BlockSpec(memory_space=pl.ANY)
    dma = pltpu.SemaphoreType.DMA
    return pl.pallas_call(
        kernel,
        out_shape=jax.ShapeDtypeStruct((rows, width), BF),
        in_specs=[anywhere, vmem, anywhere, anywhere],
        out_specs=vmem,
        scratch_shapes=[
            pltpu.VMEM(tokens.shape, BF),
            pltpu.VMEM(up_weight.shape, F32),
            pltpu.VMEM(down_weight.shape, F32),
            pltpu.VMEM((SIDE * rows, width), BF),
            pltpu.VMEM((4 * blocks * depth, inner // 2), BF),
            pltpu.VMEM((blocks * 2 * inner, rows), BF),
            pltpu.VMEM((SIDE * rows, 2 * inner), F32),
            pltpu.VMEM((SIDE * rows, 2 * inner), BF),
            pltpu.VMEM((blocks * 3 * rows, rows), F32),
            pltpu.VMEM((2, len(GROUPS), rows + 16, rows), BF),
            pltpu.VMEM((2, len(GROUPS), 2 * rows + 16, rows), BF),
            pltpu.VMEM((2, len(GROUPS), rows + 16, rows), BF),
            pltpu.VMEM((2, len(GROUPS), 2 * rows + 16, rows), BF),
            dma((10,)), dma((10,)), dma((4,)), dma((len(GROUPS),)), dma((2,)), dma((len(GROUPS),)), dma((len(GROUPS),)),
            dma, dma, dma, dma, dma, dma, dma((3,)),
        ],
        compiler_params=pltpu.CompilerParams(
            collective_id=0, has_side_effects=True, vmem_limit_bytes=56_000_000
        ),
    )(tokens, norm_gain.reshape(1, width), up_weight, down_weight)


def solution(mesh):
    placed = (P(("fs", "tp"), None), P(), P("fs", "tp"), P("tp", "fs"))
    return jax.shard_map(
        shards, mesh=mesh, in_specs=placed, out_specs=P(("fs", "tp"), None), check_vma=False
    )
```

```python
import jax
import jax.numpy as jnp
from jax import lax
from jax.experimental import pallas as pl
from jax.experimental.pallas import tpu as pltpu
from jax.sharding import PartitionSpec as P

epsilon = 1e-06
MESH = pl.DeviceIdType.MESH
SIDE = 4
OFFSETS = (0, -1, 1, 2)
BF = jnp.bfloat16
F32 = jnp.float32

ORDER = (
    (0, 0),
    (0, -1), (0, 1), (-1, 0), (1, 0),
    (-1, -1), (1, 1), (-1, 1), (1, -1),
    (2, 0), (0, 2),
    (-1, 2), (2, -1), (1, 2), (2, 1),
    (2, 2),
)


GROUPS = ((0,), (1, 2), (3, 4), (5, 6), (7, 8), (9, 10), (11, 12), (13, 14), (15,))


LEVELS = 248 * 128 - 1
LOWEST = 123.0


def coded_rows(rows):
    return rows + 8


def code(values):
    groups = values.reshape(-1, 8, values.shape[1])
    top = jnp.maximum(jnp.max(jnp.abs(groups), axis=0), 1e-20)
    exponent = jnp.ceil(jnp.log2(top * (1.0 / LEVELS)) + 0.001)
    scaled = groups * jnp.exp2(-exponent)
    level = jnp.round(jnp.abs(scaled))
    e = jnp.floor(level * (1.0 / 128.0))
    word = jnp.exp2(e - LOWEST) * (level * (1.0 / 128.0) + (1.0 - e))
    word = jnp.where(scaled < 0.0, -word, word)
    both = jnp.concatenate([word, exponent[None]], axis=0)
    return both.reshape(-1, values.shape[1]).astype(BF)


def decode(coded):
    groups = coded.astype(F32).reshape(-1, 8, coded.shape[1])
    words, unit = groups[:-1], jnp.exp2(groups[-1])
    size = jnp.abs(words)
    e = jnp.floor(jnp.log2(size) + 0.001)
    level = (e + size * jnp.exp2(-e)) * 128.0 + (LOWEST - 1.0) * 128.0
    return (jnp.where(words < 0.0, -level, level) * unit).reshape(-1, coded.shape[1])


def kernel(
    tokens_hbm, gain_ref, up_hbm, down_hbm, out_ref,
    tokens_ref, up_ref, down_ref, tok, upw, dnw, pre, hid, part, first, last, first_out, last_out,
    up_recv, dn_recv, up_pair, dn_pair, tok_recv, first_recv, last_recv,
    up_send, dn_send, up_pair_send, dn_pair_send, tok_send, rs_send, load,
):
    rows, width = tokens_ref.shape
    half = up_ref.shape[1] // 2
    depth = up_ref.shape[0]
    blocks = SIDE * SIDE
    fs = lax.axis_index("fs")
    tp = lax.axis_index("tp")
    z, y, x, core = fs // SIDE, fs % SIDE, tp // 2, tp % 2

    def near(at, by):
        return (at + (by + SIDE)) % SIDE

    def device(dz=0, dy=0, dx=0):
        return {"fs": near(z, dz) * SIDE + near(y, dy), "tp": near(x, dx) * 2 + core}

    partner = {"fs": fs, "tp": x * 2 + (1 - core)}

    def copy(src, dst, send_sem, recv_sem, to):
        return pltpu.make_async_remote_copy(
            src_ref=src, dst_ref=dst, send_sem=send_sem, recv_sem=recv_sem,
            device_id=to, device_id_type=MESH,
        )

    barrier = pltpu.get_barrier_semaphore()
    peers = [device(dz=1), device(dz=-1), device(dy=1), device(dy=-1), device(dx=1), device(dx=-1), partner]
    for peer in peers:
        pl.semaphore_signal(barrier, inc=1, device_id=peer, device_id_type=MESH)

    loads = [
        pltpu.make_async_copy(src, dst, load.at[i])
        for i, (src, dst) in enumerate((
            (up_hbm.at[:, 0:up_hbm.shape[1] // 2], up_ref.at[:, 0:up_hbm.shape[1] // 2]),
            (tokens_hbm, tokens_ref),
            (down_hbm, down_ref),
            (up_hbm.at[:, up_hbm.shape[1] // 2:], up_ref.at[:, up_hbm.shape[1] // 2:]),
        ))
    ]
    loads[0].start()
    loads[3].start()

    def up_at(h, dz, dy, q, n):
        zs, ys = near(z, dz), near(y, dy)
        block = zs * SIDE + ys if h == 0 else ys * SIDE + zs
        row = h * blocks * depth + block * depth + q * (depth // 2)
        return upw.at[pl.ds(pl.multiple_of(row, depth // 2), n * (depth // 2)), :]

    def dn_at(h, dz, dy, q, n):
        block = near(z, dz) * SIDE + near(y, dy)
        row = block * 4 * half + h * half + q * (half // 2)
        return dnw.at[pl.ds(pl.multiple_of(row, half // 2), n * (half // 2)), :]

    class Gather:
        def __init__(self, at, span, recv, send):
            self.at, self.span, self.recv, self.send = at, span, recv, send

        def piece(self, h, df, ds, q=0, n=2):
            return self.at(h, ds, df, q, n) if h == 0 else self.at(h, df, ds, q, n)

        def post(self, h, axis, sem, by, df, ds, q=0, n=2):
            ref = self.piece(h, df, ds, q, n)
            to = device(dy=by) if (h == 0) == (axis == 0) else device(dz=by)
            copy(ref, ref, self.send, self.recv.at[sem], to).start()

        def wait(self, sem, quarters):
            ref = self.span(quarters)
            copy(ref, ref, self.send, self.recv.at[sem], partner).wait_recv()

        def start_first(self, *halves):
            for h in halves:
                for by in (1, -1):
                    self.post(h, 0, 0, by, 0, 0)

        def start_second(self):
            for h in (0, 1):
                for by in (1, -1):
                    self.post(h, 1, 2, by, 0, 0)

        def first_axis(self):
            self.wait(0, 8)
            for h in (0, 1):
                for q, by in ((0, 1), (1, -1)):
                    self.post(h, 0, 1, by, -by, 0, q, 1)
            for turn in (0, 1):
                for h in (0, 1):
                    for by in (1, -1):
                        self.post(h, 1, 3 + turn, by, -by if turn == 0 else by, 0)

        def far_first(self):
            self.wait(1, 4)
            for h in (0, 1):
                for by in (1, -1):
                    self.post(h, 1, 5, by, 2, 0)

        def relay(self, minus, plus):
            self.wait(2 + minus, 8)
            for h in (0, 1):
                for q, by, j in ((0, 1, minus), (1, -1, plus)):
                    self.post(h, 1, 6 + j, by, OFFSETS[j], -by, q, 1)

        def far_second(self, j):
            self.wait(6 + j, 4)

    up = Gather(up_at, lambda n: upw.at[0:n * (depth // 2), :], up_recv, up_send)
    dn = Gather(dn_at, lambda n: dnw.at[0:n * (half // 2), :], dn_recv, dn_send)

    for h in (0, 1):
        loads[3 * h].wait()
        block = fs if h == 0 else y * SIDE + z
        row = pl.multiple_of(h * blocks * depth + block * depth, depth)
        upw[pl.ds(row, depth), :] = up_ref[:, h * half:(h + 1) * half].astype(BF)
        if h == 0:
            pl.semaphore_wait(barrier, len(peers))
        up.start_first(h)
    loads[1].start()
    loads[2].start()

    loads[1].wait()
    values = tokens_ref[...].astype(F32)
    scale = lax.rsqrt(jnp.mean(values * values, axis=-1, keepdims=True) + epsilon)
    tok[0:rows, :] = (values * scale * gain_ref[...]).astype(BF)

    def tok_at(slot, q):
        row = slot * rows + q * (rows // 2)
        return tok.at[row:row + rows // 2, :]

    def tok_post(sem, slot, there, q, by):
        copy(tok_at(slot, q), tok_at(there, q), tok_send, tok_recv.at[sem], device(dx=by)).start()

    def tok_wait(sem, halves):
        ref = tok.at[0:halves * (rows // 2), :]
        copy(ref, ref, tok_send, tok_recv.at[sem], partner).wait_recv()

    tok_post(0, 0, 1, 0, 1)
    tok_post(0, 0, 2, 1, -1)
    tok_post(1, 0, 1, 1, 1)
    tok_post(1, 0, 2, 0, -1)
    up.start_second()
    loads[2].wait()

    own = pl.multiple_of(fs * 4 * half, 4 * half)
    dnw[pl.ds(own, 2 * half), :] = down_ref[...].astype(BF)

    def dn_block(b, to_partner):
        block = near(z, ORDER[b][0]) * SIDE + near(y, ORDER[b][1])
        row = block * 4 * half + (2 * half if to_partner else 0)
        return dnw.at[pl.ds(pl.multiple_of(row, 2 * half), 2 * half), :]

    def dn_share(h, *bs):
        for b in bs:
            block = near(z, ORDER[b][0]) * SIDE + near(y, ORDER[b][1])
            mine, theirs = (
                dnw.at[pl.ds(pl.multiple_of(block * 4 * half + (2 * side + h) * half, half), half), :] for side in (0, 1)
            )
            copy(mine, theirs, dn_pair_send, dn_pair.at[(b + 1) // 2], partner).start()

    def up_plane(h, p, to_partner):
        plane = near(z if h == 0 else y, OFFSETS[p])
        row = (h + (2 if to_partner else 0)) * blocks * depth + plane * SIDE * depth
        return upw.at[pl.ds(pl.multiple_of(row, SIDE * depth), SIDE * depth), :]

    def up_share(j, p):
        for h in (0, 1):
            plane = near(z if h == 0 else y, OFFSETS[p])
            row = (plane * SIDE + near(y if h == 0 else z, OFFSETS[j])) * depth
            mine, theirs = (
                upw.at[pl.ds(pl.multiple_of((h + 2 * side) * blocks * depth + row, depth), depth), :] for side in (0, 1)
            )
            copy(mine, theirs, up_pair_send, up_pair.at[p], partner).start()

    def up_shared(p):
        ref = upw.at[0:2 * SIDE * depth, :]
        copy(ref, ref, up_pair_send, up_pair.at[p], partner).wait_recv()

    dn.start_first(0, 1)
    up_share(0, 0)
    for h in (0, 1):
        dn_share(h, 0)

    up.first_axis()
    up_share(1, 0)
    up_share(2, 0)
    up.relay(0, 0)
    up_share(0, 1)
    up_share(0, 2)
    up.far_first()
    up_share(3, 0)
    tok_wait(0, 2)
    tok_post(1, 1, 3, 0, 1)
    tok_post(1, 2, 3, 1, -1)
    for minus, plus in ((1, 2), (2, 1), (3, 3)):
        up.relay(minus, plus)
        up_share(minus, 1)
        up_share(plus, 2)
    dn.start_second()
    dn.first_axis()
    dn_share(0, 1, 2)
    dn_share(1, 3, 4)
    tok_wait(1, 4)

    def columns_of(h, p):
        plane = near(z if h == 0 else y, OFFSETS[p])
        if h == 0:
            return tok[:, pl.ds(pl.multiple_of(plane * SIDE * depth, SIDE * depth), SIDE * depth)]
        return jnp.concatenate(
            [tok[:, pl.ds(pl.multiple_of((a * SIDE + plane) * depth, depth), depth)] for a in range(SIDE)], axis=1
        )

    def dot(a, b):
        return jnp.dot(a, b, preferred_element_type=F32)

    tile = 256

    def early(h, other):
        for n in range(half // tile):
            cols = slice(n * tile, (n + 1) * tile)
            total = sum(dot(columns_of(h, p), up_plane(h, p, other)[:, cols]) for p in (0, 1, 2))
            at = (2 * other + h) * half + n * tile
            pre[:, at:at + tile] = total

    def late(h, other):
        for n in range(half // tile):
            cols = slice(n * tile, (n + 1) * tile)
            at = (2 * other + h) * half + n * tile
            total = pre[:, at:at + tile] + dot(columns_of(h, 3), up_plane(h, 3, other)[:, cols])
            hid[:, at:at + tile] = jnp.square(jnp.maximum(total, 0.0)).astype(BF)

    for h in (0, 1):
        early(h, 0)
    for p in (0, 1, 2):
        up_shared(p)
    for j in (0, 1):
        up.far_second(j)
        up_share(j, 3)
    for h in (0, 1):
        early(h, 1)
    for j in (2, 3):
        up.far_second(j)
        up_share(j, 3)
    for h in (0, 1):
        late(h, 0)
    def near_own():
        dn.relay(0, 0)
        dn_share(1, 1, 2)
        dn_share(0, 3, 4)

    def farthest():
        dn.far_second(3)
        for h in (0, 1):
            dn_share(h, 15)

    pl.when(core == 1)(near_own)
    up_shared(3)
    for h in (0, 1):
        late(h, 1)

    def part_at(b, slot, q=0, n=2):
        row = (b * 3 + slot) * rows + q * (rows // 2)
        return part.at[row:row + n * (rows // 2), :]

    def project(group):
        g = GROUPS.index(group)

        def product(depth_from, depth_to):
            pieces = []
            for b in group:
                block = near(z, ORDER[b][0]) * SIDE + near(y, ORDER[b][1])
                row = pl.multiple_of(block * 4 * half + depth_from, half)
                pieces.append(dnw[pl.ds(row, depth_to - depth_from), :])
            weights = jnp.concatenate(pieces, axis=1) if len(pieces) > 1 else pieces[0]
            parts = [dot(hid[at:at + 2 * rows, depth_from:depth_to], weights) for at in (0, 2 * rows)]
            return jnp.concatenate(parts, axis=0)

        last_group = g == len(GROUPS) - 1
        if last_group:
            pre[:, :rows] = product(0, 2 * half)
        ref = dnw.at[0:len(group) * 2 * half, :]
        copy(ref, ref, dn_pair_send, dn_pair.at[g], partner).wait_recv()
        both = pre[:, :rows] + product(2 * half, 4 * half) if last_group else product(0, 4 * half)
        terms = [both[:, i * rows:(i + 1) * rows] for i in range(len(group))]
        for side, by in ((0, 1), (1, -1)):
            row = 3 * rows + side * (rows // 2)
            out, there = first_at(first_out, side, g), first_at(first, side, g)
            out[...] = code(jnp.concatenate([t[row:row + rows // 2] for t in terms], axis=0))
            copy(out, there, rs_send, first_recv.at[g], device(dx=by)).start()
        for b, t in zip(group, terms):
            part[b * 3 * rows:(b + 1) * 3 * rows, :] = t[:3 * rows]

    def first_at(ref, side, g):
        return ref.at[side, g, 0:coded_rows(len(GROUPS[g]) * rows // 2), :]

    def last_at(ref, side, g):
        return ref.at[side, g, 0:coded_rows(len(GROUPS[g]) * rows), :]

    def pass_on(g):
        came = dnw.at[0:2 * coded_rows(len(GROUPS[g]) * rows // 2), :]
        copy(came, came, rs_send, first_recv.at[g], partner).wait_recv()
        for side, by in ((0, 1), (1, -1)):
            slot = 2 - side
            got = decode(first_at(first, side, g)[...])
            ordered = []
            for i, b in enumerate(GROUPS[g]):
                summed = part_at(b, slot, side, 1)[...] + got[i * (rows // 2):(i + 1) * (rows // 2)]
                other = part_at(b, slot, 1 - side, 1)[...]
                ordered += [summed, other] if side == 0 else [other, summed]
            out, there = last_at(last_out, side, g), last_at(last, side, g)
            out[...] = code(jnp.concatenate(ordered, axis=0))
            copy(out, there, rs_send, last_recv.at[g], device(dx=by)).start()

    def finish(g):
        came = dnw.at[0:2 * coded_rows(len(GROUPS[g]) * rows), :]
        copy(came, came, rs_send, last_recv.at[g], partner).wait_recv()
        got = decode(last_at(last, 0, g)[...]) + decode(last_at(last, 1, g)[...])
        for i, b in enumerate(GROUPS[g]):
            block = near(z, ORDER[b][0]) * SIDE + near(y, ORDER[b][1])
            total = part_at(b, 0)[...] + got[i * rows:(i + 1) * rows]
            out_ref[:, pl.ds(pl.multiple_of(block * rows, rows), rows)] = total.astype(BF)

    project(GROUPS[0])
    pl.when(core == 0)(near_own)
    project(GROUPS[1])
    dn.far_first()
    dn_share(0, 10)
    dn_share(1, 9)
    project(GROUPS[2])
    pass_on(0)
    dn.relay(1, 2)
    for h in (0, 1):
        dn_share(h, 5, 6)
    pass_on(1)
    project(GROUPS[3])
    dn.relay(2, 1)
    for h in (0, 1):
        dn_share(h, 7, 8)
    pass_on(2)
    dn.far_second(0)
    dn_share(0, 9)
    dn_share(1, 10)
    project(GROUPS[4])
    finish(0)
    project(GROUPS[5])
    dn.relay(3, 3)
    dn_share(0, 11, 13)
    dn_share(1, 12, 14)
    pass_on(3)
    finish(1)
    dn.far_second(1)
    dn_share(1, 11)
    dn_share(0, 12)
    pass_on(4)
    dn.far_second(2)
    dn_share(1, 13)
    dn_share(0, 14)
    project(GROUPS[6])
    pl.when(core == 1)(farthest)
    project(GROUPS[7])
    pass_on(5)
    pl.when(core == 0)(farthest)
    project(GROUPS[8])
    finish(2)
    finish(3)
    pass_on(6)
    finish(4)
    pass_on(7)
    pass_on(8)
    for g in (5, 6, 7, 8):
        finish(g)

    def drained(ref, sem):
        pltpu.make_async_copy(ref, ref, sem).wait()

    drained(upw.at[pl.ds(0, 15 * 4 * depth // 2), :], up_send)
    drained(dnw.at[pl.ds(0, 15 * 4 * half // 2), :], dn_send)
    drained(upw.at[pl.ds(0, 2 * blocks * depth), :], up_pair_send)
    drained(dnw.at[pl.ds(0, blocks * 2 * half), :], dn_pair_send)
    drained(tok.at[pl.ds(0, 3 * rows), :], tok_send)
    sent = sum(coded_rows(len(g) * rows // 2) + coded_rows(len(g) * rows) for g in GROUPS)
    drained(dnw.at[0:2 * sent, :], rs_send)


def shards(tokens, norm_gain, up_weight, down_weight):
    rows, width = tokens.shape
    depth, inner = up_weight.shape
    blocks = SIDE * SIDE
    vmem = pl.BlockSpec(memory_space=pltpu.VMEM)
    anywhere = pl.BlockSpec(memory_space=pl.ANY)
    dma = pltpu.SemaphoreType.DMA
    return pl.pallas_call(
        kernel,
        out_shape=jax.ShapeDtypeStruct((rows, width), BF),
        in_specs=[anywhere, vmem, anywhere, anywhere],
        out_specs=vmem,
        scratch_shapes=[
            pltpu.VMEM(tokens.shape, BF),
            pltpu.VMEM(up_weight.shape, F32),
            pltpu.VMEM(down_weight.shape, F32),
            pltpu.VMEM((SIDE * rows, width), BF),
            pltpu.VMEM((4 * blocks * depth, inner // 2), BF),
            pltpu.VMEM((blocks * 2 * inner, rows), BF),
            pltpu.VMEM((SIDE * rows, 2 * inner), F32),
            pltpu.VMEM((SIDE * rows, 2 * inner), BF),
            pltpu.VMEM((blocks * 3 * rows, rows), F32),
            pltpu.VMEM((2, len(GROUPS), rows + 16, rows), BF),
            pltpu.VMEM((2, len(GROUPS), 2 * rows + 16, rows), BF),
            pltpu.VMEM((2, len(GROUPS), rows + 16, rows), BF),
            pltpu.VMEM((2, len(GROUPS), 2 * rows + 16, rows), BF),
            dma((10,)), dma((10,)), dma((4,)), dma((len(GROUPS),)), dma((2,)), dma((len(GROUPS),)), dma((len(GROUPS),)),
            dma, dma, dma, dma, dma, dma, dma((4,)),
        ],
        compiler_params=pltpu.CompilerParams(
            collective_id=0, has_side_effects=True, vmem_limit_bytes=56_000_000
        ),
    )(tokens, norm_gain.reshape(1, width), up_weight, down_weight)


def solution(mesh):
    placed = (P(("fs", "tp"), None), P(), P("fs", "tp"), P("tp", "fs"))
    return jax.shard_map(
        shards, mesh=mesh, in_specs=placed, out_specs=P(("fs", "tp"), None), check_vma=False
    )
```
